256 devices in a mesh: sp: 64 (over z, y, core), tp: 4 (over x).
Axes of the slice: x: 4, y: 4, z: 8, core: 2. Of those that a mesh axis runs over, the one named last changes fastest.
Arguments:
- conv_outer: bfloat16 [49152, 2048], P('sp', 'tp'), may hold values from -6 to 6
- conv_inner: bfloat16 [49152, 2048], P('sp', 'tp'), may hold values from -6 to 6
- conv_input: bfloat16 [49152, 2048], P('sp', 'tp'), may hold values from -6 to 6
- conv_taps: float32 [3, 2048], P(None, 'tp'), may hold values from -3.5 to 3.5
- out_weight: bfloat16 [2048, 2048], P('tp'), may hold values from -0.125 to 0.125
- mix_gate: bfloat16 [49152, 2048], P(('sp', 'tp')), may hold values from -8 to 8
- residual: bfloat16 [49152, 2048], P(('sp', 'tp')), may hold values from -6 to 6
- mix_gain: float32 [2048], replicated, may hold values from 0.1 to 1.9
- expert_gain: float32 [2048], replicated, may hold values from 0.1 to 1.9
- expert_ids: int32 [49152, 2], P(('sp', 'tp')), may hold values from 0 to 63, all different within a row; in each aligned block of 192 rows (0 to 191, 192 to 383, ...) at most 12 rows name the same one
- group_share: float32 [49152], P(('sp', 'tp')), may hold values from 0.25 to 1
- pair_scores: float32 [49152, 2], P(('sp', 'tp')), may hold values from -8 to 8
- gate_experts: bfloat16 [64, 2048, 512], P('sp'), may hold values from -0.125 to 0.125
- up_experts: bfloat16 [64, 2048, 512], P('sp'), may hold values from -0.125 to 0.125
- down_experts: bfloat16 [64, 512, 2048], P('sp'), may hold values from -0.25 to 0.25
Outputs:
- layer_out: bfloat16 [49152, 2048], P(('sp', 'tp'))
The draws below stay inside these ranges and needn't reach their ends.
Inputs may be any that keep to these rules, and one draw needn't show every extreme that they name: `expert_ids`: within the rows of one device (aligned blocks of 192 rows), no expert is named by more than 12 rows, a bound that some block reaches; the 2 experts of a row differ.
All inputs are finite; a program needn't handle non-finite values.
Results may differ from the reference program's by a relative error of at most 0.0069.
Values may be sent and summed in bfloat16 or wider, within the bound.
A program may use at most 128 MiB of HBM per device.

```python
import math
import jax
import jax.numpy as jnp
import numpy as np
from jax import lax

D = 2048
CW = 2048
FF = 512
KSIZE = 3
TOP = 2
TOK_DEV = 192
EXPERTS = 64
CAP = 12
TOKENS = 49152


def block_scale(stream_key, dims, cuts, smallest, largest):
    loudness, own = 1.0, jax.random.fold_in(stream_key, 6)
    for axis_at, blocks in cuts:
        steps = jnp.exp(jax.random.uniform(jax.random.fold_in(own, axis_at), (blocks,), jnp.float32, smallest / len(cuts), largest / len(cuts)))
        loudness = loudness * jnp.repeat(steps, dims[axis_at] // blocks).reshape([-1 if axis == axis_at else 1 for axis in range(len(dims))])
    return loudness


def routed_block(own_key, own, number, rows, amount, top, limit, skew):
    order = jax.random.permutation(own_key, amount)
    packed, ordinary = load_shares(amount, rows * top, limit, skew, True), load_shares(amount, rows * top, limit, skew, False)
    places = jnp.arange(amount)

    def named(sizes, rotation):
        used = int((sizes > 0).sum())
        fixed = max(1, used // 4)
        moved = fixed + (places - fixed + rotation * (used - fixed)) % max(1, amount - fixed)
        return jnp.zeros((amount,), jnp.int32).at[order[jnp.where(places < fixed, places, moved)]].set(jnp.asarray(sizes, jnp.int32))

    sizes = jnp.where(number % 4 == 0, named(packed, number // 4), named(ordinary, number - number // 4 - 1))
    mixed = jax.random.permutation(jax.random.fold_in(own, 3), amount)
    donor, sink = mixed[0:amount // 2 * 2:2], mixed[1:amount // 2 * 2:2]
    margin = jnp.minimum(sizes[donor] - 1, limit - sizes[sink]) // 2
    margin = jnp.where((donor == order[0]) | (sink == order[0]) | (sizes[sink] == 0), 0, jnp.maximum(margin, 0))
    moved = jax.random.randint(jax.random.fold_in(own, 4), (amount // 2,), 0, 1 << 20) % (margin + 1)
    sizes = sizes.at[donor].add(-moved).at[sink].add(moved)
    members = jnp.searchsorted(jnp.cumsum(sizes), jnp.arange(rows * top), side="right").astype(jnp.int32)
    table = members.reshape(top, rows).T
    table = table[jax.random.permutation(jax.random.fold_in(own, 1), rows)]
    rotation = jax.random.randint(jax.random.fold_in(own, 2), (rows, 1), 0, top)
    return jnp.take_along_axis(table, (jnp.arange(top)[None, :] + rotation) % top, axis=1)


def load_shares(number_of, total, reach, slope, full):
    portions = [(1 << 20) // math.isqrt(standing ** slope) + 1 for standing in range(1, number_of + 1)]
    largest = reach if full else min(reach, max(-(-total // number_of), total * portions[0] // sum(portions)))
    least = 1 if total - largest >= number_of - 1 else 0
    given, spare = [largest] + [least] * (number_of - 1), total - largest - least * (number_of - 1)
    while spare > 0:
        candidates = [i for i in range(1, number_of) if given[i] < largest] or [i for i in range(1, number_of) if given[i] < reach]
        mass, budget = sum([portions[i] for i in candidates]), spare
        for i in candidates:
            extra = min(reach - given[i], max(1, budget * portions[i] // mass), spare)
            given[i] = given[i] + extra
            spare = spare - extra
    return np.array(given)


def bell_draw(rng, extent, spread, limit, pieces=(), kind=jnp.bfloat16):
    level = block_scale(rng, extent, pieces, -0.22, 0.18) if pieces else 1.0
    values = jax.random.normal(rng, extent, jnp.float32) * spread * level
    return jnp.minimum(jnp.maximum(values, -limit), limit).astype(kind)


def setup_inputs(seed: int = 0) -> dict:
    key_list = jax.random.split(jax.random.key(seed), 16)
    conv_outer = bell_draw(key_list[0], (TOKENS, CW), 1.0, 6.0, ((0, 64), (1, 4)))
    conv_inner = bell_draw(key_list[1], (TOKENS, CW), 1.0, 6.0, ((0, 64), (1, 4)))
    conv_input = bell_draw(key_list[2], (TOKENS, CW), 1.0, 6.0, ((0, 64), (1, 4)))
    conv_taps = bell_draw(key_list[3], (KSIZE, CW), KSIZE ** -0.5, 3.5, ((1, 4),), jnp.float32)
    out_weight = bell_draw(key_list[4], (CW, D), CW ** -0.5, 0.125, ((0, 4),))
    mix_gate = bell_draw(key_list[5], (TOKENS, D), 1.5, 8.0, ((0, 256),))
    residual = bell_draw(key_list[6], (TOKENS, D), 1.0, 6.0, ((0, 256),))
    mix_gain = jnp.clip(1.0 + 0.18 * jax.random.normal(key_list[7], (D,), jnp.float32), 0.1, 1.9)
    expert_gain = jnp.clip(1.0 + 0.18 * jax.random.normal(key_list[8], (D,), jnp.float32), 0.1, 1.9)
    expert_ids_keys = jax.random.split(jax.random.fold_in(key_list[9], 1), TOKENS // TOK_DEV)
    expert_ids_turns = jax.random.permutation(jax.random.fold_in(key_list[9], 3), TOKENS // TOK_DEV)
    expert_ids = jax.vmap(lambda own, number: routed_block(jax.random.fold_in(key_list[9], 2), own, number, TOK_DEV, EXPERTS, TOP, CAP, 1))(expert_ids_keys, expert_ids_turns).reshape((TOKENS, TOP))
    group_share = jnp.clip(0.25 + 0.75 * jax.random.uniform(key_list[10], (TOKENS,), jnp.float32) ** block_scale(key_list[10], (TOKENS,), ((0, 256),), -0.2, 0.2), 0.25, 1.0)
    pair_scores = bell_draw(key_list[11], (TOKENS, TOP), 1.5, 8.0, ((0, 256),), jnp.float32)
    gate_experts = bell_draw(key_list[12], (EXPERTS, D, FF), D ** -0.5, 0.125, ((0, 64),))
    up_experts = bell_draw(key_list[13], (EXPERTS, D, FF), D ** -0.5, 0.125, ((0, 64),))
    down_experts = bell_draw(key_list[14], (EXPERTS, FF, D), FF ** -0.5, 0.25, ((0, 64),))
    return {"conv_outer": conv_outer, "conv_inner": conv_inner, "conv_input": conv_input, "conv_taps": conv_taps, "out_weight": out_weight, "mix_gate": mix_gate, "residual": residual, "mix_gain": mix_gain, "expert_gain": expert_gain, "expert_ids": expert_ids, "group_share": group_share, "pair_scores": pair_scores, "gate_experts": gate_experts, "up_experts": up_experts, "down_experts": down_experts}


epsilon = 1e-06

def rms_scale(values, gain):
    return values * lax.rsqrt(lax.optimization_barrier(jnp.mean(values * values, axis=-1, keepdims=True)) + epsilon) * gain

def reference(conv_outer, conv_inner, conv_input, conv_taps, out_weight, mix_gate, residual, mix_gain, expert_gain, expert_ids, group_share, pair_scores, gate_experts, up_experts, down_experts):
    inner = conv_inner.astype(jnp.float32) * conv_input.astype(jnp.float32)
    length = inner.shape[0]
    padded = jnp.pad(inner, ((KSIZE - 1, 0), (0, 0)))
    conv = conv_taps[0] * padded[0:length]
    for offset in range(1, KSIZE):
        conv = conv + conv_taps[offset] * padded[offset:offset + length]
    mixed_rows = (conv_outer.astype(jnp.float32) * conv).astype(jnp.bfloat16)
    projected = jnp.dot(mixed_rows, out_weight, preferred_element_type=jnp.float32)
    mixed = jax.nn.sigmoid(mix_gate.astype(jnp.float32)) * projected
    hidden_state = (residual.astype(jnp.float32) + rms_scale(mixed, mix_gain)).astype(jnp.bfloat16)
    normed = rms_scale(hidden_state.astype(jnp.float32), expert_gain).astype(jnp.bfloat16)
    flat_ids = expert_ids.reshape(-1).astype(jnp.int32)
    total = flat_ids.shape[0]
    bound = TOKENS // TOK_DEV * CAP

    def one_expert(carried, expert):
        chosen = jnp.nonzero(flat_ids == expert, size=bound, fill_value=total)[0].astype(jnp.int32)
        rows = normed[jnp.minimum(chosen, total - 1) // TOP]
        first = jnp.dot(rows, gate_experts[expert], preferred_element_type=jnp.float32)
        second = jnp.dot(rows, up_experts[expert], preferred_element_type=jnp.float32)
        inner_hidden = (jax.nn.silu(first) * second).astype(jnp.bfloat16)
        result = jnp.dot(inner_hidden, down_experts[expert], preferred_element_type=jnp.float32).astype(jnp.bfloat16)
        return (carried.at[chosen].set(result, mode='drop'), None)
    start = jnp.zeros((total, D), jnp.bfloat16)
    assigned, unused = lax.scan(one_expert, start, jnp.arange(EXPERTS, dtype=jnp.int32))
    assigned = assigned.reshape(TOKENS, TOP, D)
    weights = group_share[:, None] * jax.nn.softmax(pair_scores, axis=-1)
    result = hidden_state.astype(jnp.float32)
    for slot in range(TOP):
        result = result + weights[:, slot:slot + 1] * assigned[:, slot].astype(jnp.float32)
    return result.astype(jnp.bfloat16)
```

```python
import functools

import jax
import jax.numpy as jnp
from jax import lax
from jax.experimental import pallas as pl
from jax.experimental.pallas import tpu as pltpu
from jax.sharding import Mesh
from jax.sharding import PartitionSpec as P

Z, Y, CORE, X = "sp_0", "sp_1", "sp_2", "tp"
SP = (Z, Y, CORE)
SP_TP = (Z, Y, CORE, X)
MESH = pl.DeviceIdType.MESH

epsilon = 1e-06
WIDTH = 256


def passed_along(value, axis, steps):
    count = lax.axis_size(axis)
    leading, last = (max(0, -steps), min(count, count - steps))
    return lax.ppermute(value, axis, [(source, source + steps) for source in range(leading, last)])


def split_up(value, dim, peers):
    before, after = (value.shape[:dim], value.shape[dim + 1 :])
    return jnp.moveaxis(value.reshape(*before, peers, -1, *after), dim, 0)


def sent_and_summed(value, axis, dim):
    peers = lax.axis_size(axis)
    parts = lax.all_to_all(split_up(value, dim, peers), axis, 0, 0, tiled=True)
    return jnp.sum(parts.astype(jnp.float32), axis=0)


def rms_scale(values, gain):
    return values * lax.rsqrt(jnp.mean(values * values, axis=-1, keepdims=True) + epsilon) * gain


def dot32(a, b):
    return jnp.dot(a, b, preferred_element_type=jnp.float32)


def expert_kernel(
    zs, ys, cs, cap, slots,
    normed_ref, hidden_ref, pick_ref, meta_ref, whi_ref, wlo_ref, gate_hbm, up_hbm, down_hbm,
    out_ref,
    s1, r1, s2, r2, o2, b2, o1, b1, metar, onehot_t, onehot, acc, act, gate_v, up_v, down_v,
    z_send, z_recv, g_send, g_recv, bg_send, bg_recv, bz_send, bz_recv, m_send, m_recv, w_sem,
):
    z, y, c = lax.axis_index(Z), lax.axis_index(Y), lax.axis_index(CORE)
    groups = ys * cs
    g_me = y * cs + c
    chunks = s1.shape[0]
    width = s1.shape[3]
    bf = jnp.bfloat16

    weights = [
        pltpu.make_async_copy(src, dst, w_sem.at[i])
        for i, (src, dst) in enumerate(((gate_hbm, gate_v), (up_hbm, up_v), (down_hbm, down_v)))
    ]
    for copy in weights:
        copy.start()

    def z_peer(o):
        return lax.rem(z + o, zs)

    def g_peer(o):
        return lax.rem(g_me + o, groups)

    def g_device(g):
        return {Y: lax.div(g, cs), CORE: lax.rem(g, cs)}

    barrier = pltpu.get_barrier_semaphore()
    for o in range(1, zs):
        pl.semaphore_signal(barrier, inc=1, device_id={Z: z_peer(o)}, device_id_type=MESH)
    for o in range(1, groups):
        pl.semaphore_signal(barrier, inc=1, device_id=g_device(g_peer(o)), device_id_type=MESH)
    pl.semaphore_wait(barrier, zs + groups - 2)

    def z_copy(src, dst, send, recv, k, o):
        return pltpu.make_async_remote_copy(
            src_ref=src.at[k, z_peer(o)], dst_ref=dst.at[k, z],
            send_sem=send.at[k, o - 1], recv_sem=recv.at[k, o - 1],
            device_id={Z: z_peer(o)}, device_id_type=MESH,
        )

    def g_copy(src, dst, send, recv, k, o):
        return pltpu.make_async_remote_copy(
            src_ref=src.at[k, g_peer(o)], dst_ref=dst.at[k, g_me],
            send_sem=send.at[k, o - 1], recv_sem=recv.at[k, o - 1],
            device_id=g_device(g_peer(o)), device_id_type=MESH,
        )

    def m_copy(o):
        return pltpu.make_async_remote_copy(
            src_ref=meta_ref.at[z_peer(o)], dst_ref=metar.at[z],
            send_sem=m_send.at[o - 1], recv_sem=m_recv.at[o - 1],
            device_id={Z: z_peer(o)}, device_id_type=MESH,
        )

    z_sends = functools.partial(z_copy, s1, r1, z_send, z_recv)
    g_sends = functools.partial(g_copy, s2, r2, g_send, g_recv)
    g_backs = functools.partial(g_copy, o2, b2, bg_send, bg_recv)
    z_backs = functools.partial(z_copy, o1, b1, bz_send, bz_recv)

    def start_all(copies, k, count):
        for o in range(1, count):
            copies(k, o).start()

    def wait_recv_all(copies, k, count):
        for o in range(1, count):
            copies(k, o).wait_recv()

    for o in range(1, zs):
        m_copy(o).start()

    def columns(k):
        return pl.ds(pl.multiple_of(k * width, width), width)

    @pl.loop(0, chunks)
    def _(k):
        values = normed_ref[:, columns(k)]
        for j in range(zs):
            s1[k, j] = dot32(pick_ref[j * cap : (j + 1) * cap, :], values).astype(bf)
        start_all(z_sends, k, zs)
        r1[k, z] = s1[k, z]

    metar[z] = meta_ref[z]
    for o in range(1, zs):
        m_copy(o).wait_recv()
    total = groups * slots
    places = lax.broadcasted_iota(jnp.int32, (cap, total), 1).astype(jnp.float32)

    @pl.loop(0, zs)
    def _(j):
        where = jnp.transpose(metar[j])[:cap, 0:1]
        onehot_t[pl.ds(pl.multiple_of(j * cap, 16), cap), :] = jnp.where(
            where == places, jnp.ones((), jnp.float32), jnp.zeros((), jnp.float32)
        ).astype(bf)

    @pl.loop(0, zs * cap // 128)
    def _(j):
        rows = pl.ds(pl.multiple_of(j * 128, 128), 128)
        onehot[:, rows] = jnp.transpose(onehot_t[rows, :].astype(jnp.float32)).astype(bf)

    weights[0].wait()
    weights[1].wait()
    acc[...] = jnp.zeros_like(acc)
    hidden_units = gate_v.shape[1]

    @pl.loop(0, chunks + 1)
    def _(k):
        @pl.when(k < chunks)
        def _():
            wait_recv_all(z_sends, k, zs)
            rows = r1[k].reshape(zs * cap, width)
            for g in range(groups):
                s2[k, g] = dot32(onehot[g * slots : (g + 1) * slots, :], rows).astype(bf)
            start_all(g_sends, k, groups)
            r2[k, g_me] = s2[k, g_me]

        @pl.when(k >= 1)
        def _():
            b = k - 1
            wait_recv_all(g_sends, b, groups)
            ks = pl.ds(pl.multiple_of(b * width, width), width)
            for half in range(2):
                rows = r2[b, half * groups // 2 : (half + 1) * groups // 2].reshape(total // 2, width)
                at = slice(half * total // 2, (half + 1) * total // 2)
                acc[at, :hidden_units] += dot32(rows, gate_v[ks, :])
                acc[at, hidden_units:] += dot32(rows, up_v[ks, :])

    @pl.loop(0, groups)
    def _(g):
        at = pl.ds(pl.multiple_of(g * slots, slots), slots)
        first = acc[at, :hidden_units]
        second = acc[at, hidden_units:]
        act[at, :] = (first / (1.0 + jnp.exp(-first)) * second).astype(bf)

    weights[2].wait()

    @pl.loop(0, chunks)
    def _(k):
        down = down_v[:, columns(k)]
        for g in range(groups):
            o2[k, g] = dot32(act[g * slots : (g + 1) * slots, :], down).astype(bf)
        start_all(g_backs, k, groups)
        b2[k, g_me] = o2[k, g_me]

    @pl.loop(0, chunks)
    def _(k):
        wait_recv_all(g_backs, k, groups)
        rows = b2[k].reshape(total, width)
        for j in range(zs):
            o1[k, j] = dot32(onehot_t[j * cap : (j + 1) * cap, :], rows).astype(bf)
        start_all(z_backs, k, zs)
        b1[k, z] = o1[k, z]

    @pl.loop(0, chunks)
    def _(k):
        wait_recv_all(z_backs, k, zs)
        rows = b1[k].reshape(zs * cap, width)
        value = hidden_ref[:, columns(k)].astype(jnp.float32)
        value = value + (dot32(whi_ref[...], rows) + dot32(wlo_ref[...], rows))
        out_ref[:, columns(k)] = value.astype(bf)

    for o in range(1, zs):
        m_copy(o).wait_send()

    @pl.loop(0, chunks)
    def _(k):
        for o in range(1, zs):
            z_sends(k, o).wait_send()
            z_backs(k, o).wait_send()
        for o in range(1, groups):
            g_sends(k, o).wait_send()
            g_backs(k, o).wait_send()


def routed_experts(normed, hidden, expert_ids, weights, gate, up, down, cap):
    zs, ys, cs = lax.axis_size(Z), lax.axis_size(Y), lax.axis_size(CORE)
    groups = ys * cs
    tokens, model = normed.shape
    per_token = expert_ids.shape[1]
    experts = zs * groups
    limit = 2 * per_token * tokens // experts
    slots = zs * limit
    entries = tokens * per_token
    expert_of = expert_ids.reshape(-1)
    z_of = expert_of // groups
    order = jnp.arange(entries, dtype=jnp.int32)
    before = (order[None, :] < order[:, None]).astype(jnp.bfloat16)

    def rank(labels, count):
        onehot = labels[:, None] == jnp.arange(count, dtype=jnp.int32)[None, :]
        seen = dot32(before, onehot.astype(jnp.bfloat16))
        return jnp.sum(jnp.where(onehot, seen, 0.0), axis=1).astype(jnp.int32)

    slot_of = (expert_of % groups) * slots + lax.axis_index(Z) * limit + rank(expert_of, experts)
    row_of = z_of * cap + rank(z_of, zs)
    rows = zs * cap
    matched = row_of[None, :] == jnp.arange(rows, dtype=jnp.int32)[:, None]
    meta = jnp.sum(jnp.where(matched, (slot_of + 1)[None, :], 0), axis=1) - 1
    meta = jnp.pad(meta.reshape(zs, 1, cap), ((0, 0), (0, 7), (0, 128 - cap)), constant_values=-1)
    meta = meta.astype(jnp.float32)
    row_pair = row_of.reshape(tokens, per_token)
    row_ids = jnp.arange(rows, dtype=jnp.int32)
    pick = jnp.zeros((rows, tokens), bool)
    weigh = jnp.zeros((tokens, rows), jnp.float32)
    for k in range(per_token):
        pick = pick | (row_ids[:, None] == row_pair[None, :, k])
        weigh = weigh + jnp.where(row_ids[None, :] == row_pair[:, k : k + 1], weights[:, k : k + 1], 0.0)
    pick = pick.astype(jnp.bfloat16)
    whi = weigh.astype(jnp.bfloat16)
    wlo = (weigh - whi.astype(jnp.float32)).astype(jnp.bfloat16)
    chunks = model // WIDTH
    units = gate.shape[1]
    bf = jnp.bfloat16
    vmem, anywhere = pl.BlockSpec(memory_space=pltpu.VMEM), pl.BlockSpec(memory_space=pl.ANY)
    z_block, g_block = (chunks, zs, cap, WIDTH), (chunks, groups, slots, WIDTH)
    z_sem, g_sem = pltpu.SemaphoreType.DMA((chunks, zs - 1)), pltpu.SemaphoreType.DMA((chunks, groups - 1))
    m_sem = pltpu.SemaphoreType.DMA((zs - 1,))
    total = groups * slots
    return pl.pallas_call(
        functools.partial(expert_kernel, zs, ys, cs, cap, slots),
        out_shape=jax.ShapeDtypeStruct((tokens, model), bf),
        in_specs=[vmem] * 6 + [anywhere] * 3,
        out_specs=vmem,
        scratch_shapes=[
            pltpu.VMEM(z_block, bf), pltpu.VMEM(z_block, bf),
            pltpu.VMEM(g_block, bf), pltpu.VMEM(g_block, bf),
            pltpu.VMEM(g_block, bf), pltpu.VMEM(g_block, bf),
            pltpu.VMEM(z_block, bf), pltpu.VMEM(z_block, bf),
            pltpu.VMEM((zs, 8, 128), jnp.float32),
            pltpu.VMEM((rows, total), bf),
            pltpu.VMEM((total, rows), bf),
            pltpu.VMEM((total, 2 * units), jnp.float32),
            pltpu.VMEM((total, units), bf),
            pltpu.VMEM(gate.shape, bf), pltpu.VMEM(up.shape, bf), pltpu.VMEM(down.shape, bf),
            z_sem, z_sem, g_sem, g_sem, g_sem, g_sem, z_sem, z_sem, m_sem, m_sem,
            pltpu.SemaphoreType.DMA((3,)),
        ],
        compiler_params=pltpu.CompilerParams(
            collective_id=1, has_side_effects=True, vmem_limit_bytes=60 * 1024 * 1024
        ),
        name="routed_experts",
    )(normed, hidden, pick, meta, whi, wlo, gate, up, down)


def per_device(
    conv_outer,
    conv_inner,
    conv_input,
    conv_taps,
    out_weight,
    mix_gate,
    residual,
    mix_gain,
    expert_gain,
    expert_ids,
    group_share,
    pair_scores,
    gate_experts,
    up_experts,
    down_experts,
):
    kept = conv_taps.shape[0] - 1
    earlier = passed_along((conv_inner[-kept:], conv_input[-kept:]), SP, 1)
    inner = jnp.concatenate(
        [
            earlier[0].astype(jnp.float32) * earlier[1].astype(jnp.float32),
            conv_inner.astype(jnp.float32) * conv_input.astype(jnp.float32),
        ],
        0,
    )
    length = conv_inner.shape[0]
    conv = conv_taps[0] * inner[0:length]
    for offset in range(1, kept + 1):
        conv = conv + conv_taps[offset] * inner[offset : offset + length]
    mixed_rows = (conv_outer.astype(jnp.float32) * conv).astype(jnp.bfloat16)
    projected = sent_and_summed(
        jnp.dot(mixed_rows, out_weight, preferred_element_type=jnp.float32).astype(jnp.bfloat16),
        X,
        0,
    )
    mixed = jax.nn.sigmoid(mix_gate.astype(jnp.float32)) * projected
    hidden_state = (residual.astype(jnp.float32) + rms_scale(mixed, mix_gain)).astype(jnp.bfloat16)
    normed = rms_scale(hidden_state.astype(jnp.float32), expert_gain).astype(jnp.bfloat16)
    weights = group_share[:, None] * jax.nn.softmax(pair_scores, axis=-1)
    limit = 2 * expert_ids.shape[1] * residual.shape[0] // (lax.axis_size(SP) * gate_experts.shape[0])
    cap = limit * lax.axis_size(Y) * lax.axis_size(CORE)
    return routed_experts(
        normed, hidden_state, expert_ids, weights, gate_experts[0], up_experts[0], down_experts[0], cap
    )


def solution(mesh):
    torus = Mesh(mesh.devices.reshape(8, 4, 2, mesh.shape["tp"]), SP_TP)
    return jax.shard_map(
        per_device,
        mesh=torus,
        in_specs=(
            P(SP, X),
            P(SP, X),
            P(SP, X),
            P(None, X),
            P(X, None),
            P(SP_TP, None),
            P(SP_TP, None),
            P(),
            P(),
            P(SP_TP, None),
            P(SP_TP),
            P(SP_TP, None),
            P(SP, None, None),
            P(SP, None, None),
            P(SP, None, None),
        ),
        out_specs=P(SP_TP, None),
        check_vma=False,
    )
```

```python
import functools

import jax
import jax.numpy as jnp
from jax import lax
from jax.experimental import pallas as pl
from jax.experimental.pallas import tpu as pltpu
from jax.sharding import Mesh
from jax.sharding import PartitionSpec as P

Z, Y, CORE, X = "sp_0", "sp_1", "sp_2", "tp"
SP = (Z, Y, CORE)
SP_TP = (Z, Y, CORE, X)
MESH = pl.DeviceIdType.MESH

epsilon = 1e-06
WIDTH = 256
USUAL = 80


def rms_scale(values, gain):
    return values * lax.rsqrt(jnp.mean(values * values, axis=-1, keepdims=True) + epsilon) * gain


def dot32(a, b):
    return jnp.dot(a, b, preferred_element_type=jnp.float32)


def mixer_kernel(
    sizes, limit, parts,
    taps_ref, mix_gain_ref, expert_gain_ref, ids_ref, share_ref, scores_ref,
    outer_hbm, inner_hbm, input_hbm, weight_hbm, gate_hbm, residual_hbm,
    hidden_ref, normed_ref, columns_ref, lanes_ref, most_ref,
    outer_v, inner_v, input_v, weight_v, gate_v, residual_v,
    products, mixed, own, far, far_in, near, near_in, tails, tail_in, table,
    mine, x_in, g_in, z_in, sent_x, sent_g,
    l_sem, t_send, t_recv, f_send, f_recv, n_send, n_recv, mx_send, mx_recv, mg_send, mg_recv, mz_send, mz_recv,
):
    zs, ys, cs, xs = sizes
    z, y, c, x = (lax.axis_index(a) for a in SP_TP)
    groups = ys * cs
    g_me = y * cs + c
    devices = zs * groups
    me = z * groups + g_me
    bf, f32 = jnp.bfloat16, jnp.float32
    length, lanes = inner_v.shape
    rows = length // xs
    half = own.shape[1] // 2
    piece = rows // parts

    loads = [
        pltpu.make_async_copy(src, dst, l_sem.at[i])
        for i, (src, dst) in enumerate(
            (
                (inner_hbm, inner_v), (input_hbm, input_v), (outer_hbm, outer_v),
                (weight_hbm, weight_v), (gate_hbm, gate_v), (residual_hbm, residual_v),
            )
        )
    ]
    for load in loads:
        load.start()

    def sp_device(index):
        return {Z: lax.div(index, groups), Y: lax.div(lax.rem(index, groups), cs), CORE: lax.rem(index, cs)}

    following, preceding = lax.rem(me + 1, devices), lax.rem(me + devices - 1, devices)
    x_peers = [{X: lax.rem(x + o, xs)} for o in range(1, xs)]
    z_peers = [{Z: lax.rem(z + o, zs)} for o in range(1, zs)]
    g_peers = []
    for o in range(1, groups):
        g = lax.rem(g_me + o, groups)
        g_peers.append({Y: lax.div(g, cs), CORE: lax.rem(g, cs)})
    everyone = x_peers + z_peers + g_peers + [sp_device(following), sp_device(preceding)]
    barrier = pltpu.get_barrier_semaphore()
    for peer in everyone:
        pl.semaphore_signal(barrier, inc=1, device_id=peer, device_id_type=MESH)

    loads[0].wait()
    loads[1].wait()
    last = tails.shape[1]
    tails[0] = inner_v[length - last :, :]
    tails[1] = input_v[length - last :, :]
    pl.semaphore_wait(barrier, len(everyone))
    tail_copy = pltpu.make_async_remote_copy(
        src_ref=tails, dst_ref=tail_in, send_sem=t_send, recv_sem=t_recv,
        device_id=sp_device(following), device_id_type=MESH,
    )
    tail_copy.start()

    pad = 8
    for b in range(xs):
        at = slice(b * rows, (b + 1) * rows)
        products[pad + b * rows : pad + (b + 1) * rows, :] = inner_v[at, :].astype(f32) * input_v[at, :].astype(f32)
    loads[2].wait()
    for b in reversed(range(xs)):
        if b == 0:
            tail_copy.wait_recv()
            earlier = tail_in[0].astype(f32) * tail_in[1].astype(f32)
            earlier = jnp.where(me == 0, jnp.zeros_like(earlier), earlier)
            products[0:pad, :] = earlier[last - pad :, :]
        start = b * rows
        conv = taps_ref[0:1, :] * products[start + pad - 2 : start + pad - 2 + rows, :]
        conv = conv + taps_ref[1:2, :] * products[start + pad - 1 : start + pad - 1 + rows, :]
        conv = conv + taps_ref[2:3, :] * products[start + pad : start + pad + rows, :]
        mixed[start : start + rows, :] = (outer_v[start : start + rows, :].astype(f32) * conv).astype(bf)
    loads[3].wait()

    right, left = lax.rem(x + 1, xs), lax.rem(x + xs - 1, xs)
    ways = (right, left)

    def partial_of(owner, h):
        block = mixed[pl.ds(pl.multiple_of(owner * rows, 16), rows), :]
        return dot32(block, weight_v[:, h * half : (h + 1) * half])

    def far_copy(h, t):
        at = pl.ds(t * piece, piece)
        return pltpu.make_async_remote_copy(
            src_ref=far.at[h, at], dst_ref=far_in.at[h, at],
            send_sem=f_send.at[h, t], recv_sem=f_recv.at[h, t],
            device_id={X: ways[h]}, device_id_type=MESH,
        )

    def near_copy(d, h, t):
        at = pl.ds(t * piece, piece)
        return pltpu.make_async_remote_copy(
            src_ref=near.at[d, h, at], dst_ref=near_in.at[d, h, at],
            send_sem=n_send.at[d, h, t], recv_sem=n_recv.at[d, h, t],
            device_id={X: ways[d]}, device_id_type=MESH,
        )

    opposite = lax.rem(x + 2, xs)
    for h in range(2):
        far[h] = partial_of(opposite, h).astype(bf)
        for t in range(parts):
            far_copy(h, t).start()
    for d in range(2):
        near[d, 1 - d] = partial_of(ways[d], 1 - d).astype(bf)
        for t in range(parts):
            near_copy(d, 1 - d, t).start()
    for d in range(2):
        own[:, d * half : (d + 1) * half] = partial_of(ways[d], d)

    tokens = ids_ref.shape[0]
    expert = [ids_ref[:, k : k + 1].astype(f32) for k in range(2)]
    z_of = [jnp.floor((e + 0.5) / groups) for e in expert]
    lane = lax.broadcasted_iota(jnp.int32, (tokens, 128), 1).astype(f32)
    marks = [
        jnp.where((e == lane) | (zz + devices == lane), jnp.ones((), f32), jnp.zeros((), f32))
        for e, zz in zip(expert, z_of)
    ]
    before = jnp.where(
        lax.broadcasted_iota(jnp.int32, (tokens, tokens), 1) < lax.broadcasted_iota(jnp.int32, (tokens, tokens), 0),
        jnp.ones((), f32), jnp.zeros((), f32),
    ).astype(bf)
    first_sum = jnp.sum(marks[0], axis=0, keepdims=True)
    most = first_sum + jnp.sum(marks[1], axis=0, keepdims=True)
    most = jnp.where(lane[0:1, :] >= devices, most, jnp.zeros_like(most))
    most = jnp.broadcast_to(jnp.max(most, axis=1, keepdims=True), (8, 128))
    mine[...] = most

    def flag_copy(src, dst, send, recv, i, peer):
        return pltpu.make_async_remote_copy(
            src_ref=src, dst_ref=dst.at[i], send_sem=send.at[i], recv_sem=recv.at[i],
            device_id=peer, device_id_type=MESH,
        )

    x_flags = [flag_copy(mine, x_in, mx_send, mx_recv, i, p) for i, p in enumerate(x_peers)]
    g_flags = [flag_copy(sent_x, g_in, mg_send, mg_recv, i, p) for i, p in enumerate(g_peers)]
    z_flags = [flag_copy(sent_g, z_in, mz_send, mz_recv, i, p) for i, p in enumerate(z_peers)]
    for flag in x_flags:
        flag.start()

    seen = [dot32(before, marks[0].astype(bf)), dot32(before, marks[1].astype(bf)) + first_sum]
    info = []
    scores = [scores_ref[:, k : k + 1] for k in range(2)]
    top = jnp.maximum(scores[0], scores[1])
    powers = [jnp.exp(v - top) for v in scores]
    for k in range(2):
        hit = marks[k] * seen[k]
        rank = jnp.sum(jnp.where(lane < devices, hit, 0.0), axis=1, keepdims=True)
        place = jnp.sum(jnp.where(lane >= devices, hit, 0.0), axis=1, keepdims=True)
        slot = (expert[k] - groups * z_of[k]) * (zs * limit) + (z * limit).astype(f32) + rank
        info.append((z_of[k], place, slot, share_ref[...] * (powers[k] / (powers[0] + powers[1]))))
    column = jnp.zeros((tokens, 128), f32)
    for i in range(4):
        for k in range(2):
            column = column + jnp.where(lane == 2 * i + k, info[k][i], 0.0)
    columns_ref[...] = column
    table[...] = jnp.zeros_like(table)
    table[0:tokens, :] = column
    lanes_ref[...] = jnp.transpose(table[...])[0:8, :]

    for flag in x_flags:
        flag.wait_recv()
    for i in range(xs - 1):
        most = jnp.maximum(most, x_in[i])
    sent_x[...] = most
    for flag in g_flags:
        flag.start()

    for t in range(parts):
        at = slice(t * piece, (t + 1) * piece)
        for d in range(2):
            far_copy(d, t).wait_recv()
            near[d, d, at, :] = (own[at, d * half : (d + 1) * half] + far_in[d, at, :].astype(f32)).astype(bf)
            near_copy(d, d, t).start()
    for h in range(2):
        own[:, h * half : (h + 1) * half] = partial_of(x, h)

    for flag in g_flags:
        flag.wait_recv()
    for i in range(groups - 1):
        most = jnp.maximum(most, g_in[i])
    sent_g[...] = most
    for flag in z_flags:
        flag.start()

    loads[4].wait()
    loads[5].wait()
    for t in range(parts):
        at = slice(t * piece, (t + 1) * piece)
        for d in range(2):
            for h in range(2):
                near_copy(d, h, t).wait_recv()
        sums = []
        for h in range(2):
            part = own[at, h * half : (h + 1) * half]
            sums.append(part + near_in[0, h, at, :].astype(f32) + near_in[1, h, at, :].astype(f32))
        projected = jnp.concatenate(sums, axis=1)
        value = jax.nn.sigmoid(gate_v[at, :].astype(f32)) * projected
        hidden = (residual_v[at, :].astype(f32) + rms_scale(value, mix_gain_ref[...])).astype(bf)
        hidden_ref[at, :] = hidden
        normed_ref[at, :] = rms_scale(hidden.astype(f32), expert_gain_ref[...]).astype(bf)

    for flag in z_flags:
        flag.wait_recv()
    for i in range(zs - 1):
        most = jnp.maximum(most, z_in[i])
    most_ref[...] = most

    tail_copy.wait_send()
    for h in range(2):
        for t in range(parts):
            far_copy(h, t).wait_send()
            for d in range(2):
                near_copy(d, h, t).wait_send()
    for flag in x_flags + g_flags + z_flags:
        flag.wait_send()


def mixer(outer, inner, values, taps, weight, gate, residual, mix_gain, expert_gain, ids, share, scores, limit):
    sizes = tuple(lax.axis_size(a) for a in SP_TP)
    zs, ys, cs, xs = sizes
    groups = ys * cs
    length, lanes = inner.shape
    rows, model = residual.shape
    half, parts, last = model // 2, 4, 16
    bf, f32 = jnp.bfloat16, jnp.float32
    vmem, anywhere = pl.BlockSpec(memory_space=pltpu.VMEM), pl.BlockSpec(memory_space=pl.ANY)
    dma = pltpu.SemaphoreType.DMA
    flag = (8, 128)
    return pl.pallas_call(
        functools.partial(mixer_kernel, sizes, limit, parts),
        out_shape=(
            jax.ShapeDtypeStruct((rows, model), bf),
            jax.ShapeDtypeStruct((rows, model), bf),
            jax.ShapeDtypeStruct((rows, 128), f32),
            jax.ShapeDtypeStruct((8, 256), f32),
            jax.ShapeDtypeStruct(flag, f32),
        ),
        in_specs=[vmem] * 6 + [anywhere] * 6,
        out_specs=(vmem,) * 5,
        scratch_shapes=[
            pltpu.VMEM(outer.shape, bf), pltpu.VMEM(inner.shape, bf), pltpu.VMEM(values.shape, bf),
            pltpu.VMEM(weight.shape, bf), pltpu.VMEM(gate.shape, bf), pltpu.VMEM(residual.shape, bf),
            pltpu.VMEM((length + 8, lanes), f32),
            pltpu.VMEM((length, lanes), bf),
            pltpu.VMEM((rows, model), f32),
            pltpu.VMEM((2, rows, half), bf), pltpu.VMEM((2, rows, half), bf),
            pltpu.VMEM((2, 2, rows, half), bf), pltpu.VMEM((2, 2, rows, half), bf),
            pltpu.VMEM((2, last, lanes), bf), pltpu.VMEM((2, last, lanes), bf),
            pltpu.VMEM((256, 128), f32),
            pltpu.VMEM(flag, f32), pltpu.VMEM((xs - 1, *flag), f32),
            pltpu.VMEM((groups - 1, *flag), f32), pltpu.VMEM((zs - 1, *flag), f32),
            pltpu.VMEM(flag, f32), pltpu.VMEM(flag, f32),
            dma((6,)), dma, dma,
            dma((2, parts)), dma((2, parts)), dma((2, 2, parts)), dma((2, 2, parts)),
            dma((xs - 1,)), dma((xs - 1,)), dma((groups - 1,)), dma((groups - 1,)), dma((zs - 1,)), dma((zs - 1,)),
        ],
        compiler_params=pltpu.CompilerParams(
            collective_id=1, has_side_effects=True, vmem_limit_bytes=48 * 1024 * 1024
        ),
        name="mixer",
    )(
        taps, mix_gain[None, :], expert_gain[None, :], ids, share[:, None], scores,
        outer, inner, values, weight, gate, residual,
    )


def expert_kernel(
    zs, ys, cs, cap, slots,
    normed_ref, hidden_ref, columns_ref, lanes_ref, gate_hbm, up_hbm, down_hbm,
    out_ref,
    pick_ref, meta_ref, whi_ref, wlo_ref, s1, r1, s2, r2, o2, b2, o1, b1, metar, onehot_t, onehot, acc, act, gate_v, up_v, down_v,
    z_send, z_recv, g_send, g_recv, bg_send, bg_recv, bz_send, bz_recv, m_send, m_recv, w_sem,
):
    z, y, c = lax.axis_index(Z), lax.axis_index(Y), lax.axis_index(CORE)
    groups = ys * cs
    g_me = y * cs + c
    chunks = s1.shape[0]
    width = s1.shape[3]
    bf = jnp.bfloat16

    weights = [
        pltpu.make_async_copy(src, dst, w_sem.at[i])
        for i, (src, dst) in enumerate(((gate_hbm, gate_v), (up_hbm, up_v), (down_hbm, down_v)))
    ]
    for copy in weights:
        copy.start()

    def z_peer(o):
        return lax.rem(z + o, zs)

    def g_peer(o):
        return lax.rem(g_me + o, groups)

    def g_device(g):
        return {Y: lax.div(g, cs), CORE: lax.rem(g, cs)}

    barrier = pltpu.get_barrier_semaphore()
    for o in range(1, zs):
        pl.semaphore_signal(barrier, inc=1, device_id={Z: z_peer(o)}, device_id_type=MESH)
    for o in range(1, groups):
        pl.semaphore_signal(barrier, inc=1, device_id=g_device(g_peer(o)), device_id_type=MESH)
    pl.semaphore_wait(barrier, zs + groups - 2)

    def z_copy(src, dst, send, recv, k, o):
        return pltpu.make_async_remote_copy(
            src_ref=src.at[k, z_peer(o)], dst_ref=dst.at[k, z],
            send_sem=send.at[k, o - 1], recv_sem=recv.at[k, o - 1],
            device_id={Z: z_peer(o)}, device_id_type=MESH,
        )

    def g_copy(src, dst, send, recv, k, o):
        return pltpu.make_async_remote_copy(
            src_ref=src.at[k, g_peer(o)], dst_ref=dst.at[k, g_me],
            send_sem=send.at[k, o - 1], recv_sem=recv.at[k, o - 1],
            device_id=g_device(g_peer(o)), device_id_type=MESH,
        )

    def m_copy(o):
        return pltpu.make_async_remote_copy(
            src_ref=meta_ref.at[z_peer(o)], dst_ref=metar.at[z],
            send_sem=m_send.at[o - 1], recv_sem=m_recv.at[o - 1],
            device_id={Z: z_peer(o)}, device_id_type=MESH,
        )

    z_sends = functools.partial(z_copy, s1, r1, z_send, z_recv)
    g_sends = functools.partial(g_copy, s2, r2, g_send, g_recv)
    g_backs = functools.partial(g_copy, o2, b2, bg_send, bg_recv)
    z_backs = functools.partial(z_copy, o1, b1, bz_send, bz_recv)

    def start_all(copies, k, count):
        for o in range(1, count):
            copies(k, o).start()

    def wait_recv_all(copies, k, count):
        for o in range(1, count):
            copies(k, o).wait_recv()

    def columns(k):
        return pl.ds(pl.multiple_of(k * width, width), width)

    f32 = jnp.float32
    tokens = normed_ref.shape[0]
    row_of = [lanes_ref[k : k + 1, 0:tokens] * cap + lanes_ref[2 + k : 3 + k, 0:tokens] for k in range(2)]
    slot_of = [lanes_ref[4 + k : 5 + k, 0:tokens] + 1.0 for k in range(2)]
    place = lax.broadcasted_iota(jnp.int32, (cap, tokens), 0).astype(f32)
    for j in range(zs):
        hit = [place + float(j * cap) == r for r in row_of]
        pick_ref[j * cap : (j + 1) * cap, :] = jnp.where(hit[0] | hit[1], jnp.ones((), f32), jnp.zeros((), f32)).astype(bf)

    @pl.loop(0, chunks)
    def _(k):
        values = normed_ref[:, columns(k)]
        for j in range(zs):
            s1[k, j] = dot32(pick_ref[j * cap : (j + 1) * cap, :], values).astype(bf)
        start_all(z_sends, k, zs)
        r1[k, z] = s1[k, z]

    for j in range(zs):
        hit = [place + float(j * cap) == r for r in row_of]
        found = jnp.where(hit[0], slot_of[0], 0.0) + jnp.where(hit[1], slot_of[1], 0.0)
        found = jnp.broadcast_to(jnp.sum(found, axis=1, keepdims=True) - 1.0, (cap, 128))
        found = jnp.concatenate([found, jnp.full((128 - cap, 128), -1.0, f32)], axis=0)
        meta_ref[j] = jnp.transpose(found)[0:8, :]
    for o in range(1, zs):
        m_copy(o).start()
    row_lane = lax.broadcasted_iota(jnp.int32, (tokens, zs * cap), 1).astype(f32)
    weigh = jnp.zeros((tokens, zs * cap), f32)
    for k in range(2):
        row = columns_ref[:, k : k + 1] * cap + columns_ref[:, 2 + k : 3 + k]
        weigh = weigh + jnp.where(row == row_lane, columns_ref[:, 6 + k : 7 + k], 0.0)
    whi_ref[...] = weigh.astype(bf)
    wlo_ref[...] = (weigh - whi_ref[...].astype(f32)).astype(bf)
    metar[z] = meta_ref[z]
    for o in range(1, zs):
        m_copy(o).wait_recv()
    total = groups * slots
    places = lax.broadcasted_iota(jnp.int32, (cap, total), 1).astype(jnp.float32)

    @pl.loop(0, zs)
    def _(j):
        where = jnp.transpose(metar[j])[:cap, 0:1]
        onehot_t[pl.ds(pl.multiple_of(j * cap, 16), cap), :] = jnp.where(
            where == places, jnp.ones((), jnp.float32), jnp.zeros((), jnp.float32)
        ).astype(bf)

    @pl.loop(0, zs * cap // 128)
    def _(j):
        rows = pl.ds(pl.multiple_of(j * 128, 128), 128)
        onehot[:, rows] = jnp.transpose(onehot_t[rows, :].astype(jnp.float32)).astype(bf)

    weights[0].wait()
    weights[1].wait()
    acc[...] = jnp.zeros_like(acc)
    hidden_units = gate_v.shape[1]

    @pl.loop(0, chunks + 1)
    def _(k):
        @pl.when(k < chunks)
        def _():
            wait_recv_all(z_sends, k, zs)
            rows = r1[k].reshape(zs * cap, width)
            for g in range(groups):
                s2[k, g] = dot32(onehot[g * slots : (g + 1) * slots, :], rows).astype(bf)
            start_all(g_sends, k, groups)
            r2[k, g_me] = s2[k, g_me]

        @pl.when(k >= 1)
        def _():
            b = k - 1
            wait_recv_all(g_sends, b, groups)
            ks = pl.ds(pl.multiple_of(b * width, width), width)
            for half in range(2):
                rows = r2[b, half * groups // 2 : (half + 1) * groups // 2].reshape(total // 2, width)
                at = slice(half * total // 2, (half + 1) * total // 2)
                acc[at, :hidden_units] += dot32(rows, gate_v[ks, :])
                acc[at, hidden_units:] += dot32(rows, up_v[ks, :])

    @pl.loop(0, groups)
    def _(g):
        at = pl.ds(pl.multiple_of(g * slots, slots), slots)
        first = acc[at, :hidden_units]
        second = acc[at, hidden_units:]
        act[at, :] = (first / (1.0 + jnp.exp(-first)) * second).astype(bf)

    weights[2].wait()

    @pl.loop(0, chunks)
    def _(k):
        down = down_v[:, columns(k)]
        for g in range(groups):
            o2[k, g] = dot32(act[g * slots : (g + 1) * slots, :], down).astype(bf)
        start_all(g_backs, k, groups)
        b2[k, g_me] = o2[k, g_me]

    @pl.loop(0, chunks)
    def _(k):
        wait_recv_all(g_backs, k, groups)
        rows = b2[k].reshape(total, width)
        for j in range(zs):
            o1[k, j] = dot32(onehot_t[j * cap : (j + 1) * cap, :], rows).astype(bf)
        start_all(z_backs, k, zs)
        b1[k, z] = o1[k, z]

    @pl.loop(0, chunks)
    def _(k):
        wait_recv_all(z_backs, k, zs)
        rows = b1[k].reshape(zs * cap, width)
        value = hidden_ref[:, columns(k)].astype(jnp.float32)
        value = value + (dot32(whi_ref[...], rows) + dot32(wlo_ref[...], rows))
        out_ref[:, columns(k)] = value.astype(bf)

    for o in range(1, zs):
        m_copy(o).wait_send()

    @pl.loop(0, chunks)
    def _(k):
        for o in range(1, zs):
            z_sends(k, o).wait_send()
            z_backs(k, o).wait_send()
        for o in range(1, groups):
            g_sends(k, o).wait_send()
            g_backs(k, o).wait_send()


def routed_experts(cap, limit, collective, normed, hidden, columns, lanes, gate, up, down):
    zs, ys, cs = lax.axis_size(Z), lax.axis_size(Y), lax.axis_size(CORE)
    groups = ys * cs
    tokens, model = normed.shape
    slots = zs * limit
    rows = zs * cap
    chunks = model // WIDTH
    units = gate.shape[1]
    bf = jnp.bfloat16
    vmem, anywhere = pl.BlockSpec(memory_space=pltpu.VMEM), pl.BlockSpec(memory_space=pl.ANY)
    z_block, g_block = (chunks, zs, cap, WIDTH), (chunks, groups, slots, WIDTH)
    z_sem, g_sem = pltpu.SemaphoreType.DMA((chunks, zs - 1)), pltpu.SemaphoreType.DMA((chunks, groups - 1))
    m_sem = pltpu.SemaphoreType.DMA((zs - 1,))
    total = groups * slots
    return pl.pallas_call(
        functools.partial(expert_kernel, zs, ys, cs, cap, slots),
        out_shape=jax.ShapeDtypeStruct((tokens, model), bf),
        in_specs=[vmem] * 4 + [anywhere] * 3,
        out_specs=vmem,
        scratch_shapes=[
            pltpu.VMEM((rows, tokens), bf), pltpu.VMEM((zs, 8, 128), jnp.float32),
            pltpu.VMEM((tokens, rows), bf), pltpu.VMEM((tokens, rows), bf),
            pltpu.VMEM(z_block, bf), pltpu.VMEM(z_block, bf),
            pltpu.VMEM(g_block, bf), pltpu.VMEM(g_block, bf),
            pltpu.VMEM(g_block, bf), pltpu.VMEM(g_block, bf),
            pltpu.VMEM(z_block, bf), pltpu.VMEM(z_block, bf),
            pltpu.VMEM((zs, 8, 128), jnp.float32),
            pltpu.VMEM((rows, total), bf),
            pltpu.VMEM((total, rows), bf),
            pltpu.VMEM((total, 2 * units), jnp.float32),
            pltpu.VMEM((total, units), bf),
            pltpu.VMEM(gate.shape, bf), pltpu.VMEM(up.shape, bf), pltpu.VMEM(down.shape, bf),
            z_sem, z_sem, g_sem, g_sem, g_sem, g_sem, z_sem, z_sem, m_sem, m_sem,
            pltpu.SemaphoreType.DMA((3,)),
        ],
        compiler_params=pltpu.CompilerParams(
            collective_id=collective, has_side_effects=True, vmem_limit_bytes=60 * 1024 * 1024
        ),
        name="routed_experts",
    )(normed, hidden, columns, lanes, gate, up, down)


def per_device(
    conv_outer,
    conv_inner,
    conv_input,
    conv_taps,
    out_weight,
    mix_gate,
    residual,
    mix_gain,
    expert_gain,
    expert_ids,
    group_share,
    pair_scores,
    gate_experts,
    up_experts,
    down_experts,
):
    limit = 2 * expert_ids.shape[1] * residual.shape[0] // (lax.axis_size(SP) * gate_experts.shape[0])
    worst = limit * lax.axis_size(Y) * lax.axis_size(CORE)
    hidden, normed, columns, lanes, most = mixer(
        conv_outer, conv_inner, conv_input, conv_taps, out_weight, mix_gate, residual, mix_gain, expert_gain,
        expert_ids, group_share, pair_scores, limit,
    )
    arguments = (normed, hidden, columns, lanes, gate_experts[0], up_experts[0], down_experts[0])
    usual = USUAL
    return lax.cond(
        most[0, 0] <= usual,
        functools.partial(routed_experts, usual, limit, 2),
        functools.partial(routed_experts, worst, limit, 3),
        *arguments,
    )


def solution(mesh):
    torus = Mesh(mesh.devices.reshape(8, 4, 2, mesh.shape["tp"]), SP_TP)
    return jax.shard_map(
        per_device,
        mesh=torus,
        in_specs=(
            P(SP, X),
            P(SP, X),
            P(SP, X),
            P(None, X),
            P(X, None),
            P(SP_TP, None),
            P(SP_TP, None),
            P(),
            P(),
            P(SP_TP, None),
            P(SP_TP),
            P(SP_TP, None),
            P(SP, None, None),
            P(SP, None, None),
            P(SP, None, None),
        ),
        out_specs=P(SP_TP, None),
        check_vma=False,
    )
```

```python
import functools

import jax
import jax.numpy as jnp
from jax import lax
from jax.experimental import pallas as pl
from jax.experimental.pallas import tpu as pltpu
from jax.sharding import Mesh
from jax.sharding import PartitionSpec as P

Z, Y, CORE, X = "sp_0", "sp_1", "sp_2", "tp"
SP = (Z, Y, CORE)
SP_TP = (Z, Y, CORE, X)
MESH = pl.DeviceIdType.MESH

epsilon = 1e-06
WIDTH = 256
VMEM_LIMIT = 67043328
DEPTH = 2
WINDOW = 3
USUAL = 80


def rms_scale(values, gain):
    return values * lax.rsqrt(jnp.mean(values * values, axis=-1, keepdims=True) + epsilon) * gain


def dot32(a, b):
    return jnp.dot(a, b, preferred_element_type=jnp.float32)


def mixer_kernel(
    sizes, limit, parts,
    taps_hbm, mix_gain_hbm, expert_gain_hbm, ids_hbm, share_hbm, scores_hbm,
    outer_hbm, inner_hbm, input_hbm, weight_hbm, gate_hbm, residual_hbm,
    hidden_ref, normed_ref, columns_ref, lanes_ref, most_ref,
    taps_ref, mix_gain_ref, expert_gain_ref, ids_v, share_v, scores_v,
    outer_v, inner_v, input_v, weight_v, gate_v, residual_v,
    products, mixed, own, far, far_in, near, near_in, tails, tail_in, table,
    mine, x_in, g_in, z_in, sent_x, sent_g,
    l_sem, t_send, t_recv, f_send, f_recv, n_send, n_recv, mx_send, mx_recv, mg_send, mg_recv, mz_send, mz_recv,
):
    zs, ys, cs, xs = sizes
    z, y, c, x = (lax.axis_index(a) for a in SP_TP)
    groups = ys * cs
    g_me = y * cs + c
    devices = zs * groups
    me = z * groups + g_me
    bf, f32 = jnp.bfloat16, jnp.float32
    length, lanes = inner_v.shape
    rows = length // xs
    half = own.shape[1] // 2
    piece = rows // parts

    loads = [
        pltpu.make_async_copy(src, dst, l_sem.at[i])
        for i, (src, dst) in enumerate(
            (
                (inner_hbm, inner_v), (input_hbm, input_v), (outer_hbm, outer_v),
                (taps_hbm, taps_ref), (weight_hbm, weight_v), (ids_hbm, ids_v), (share_hbm, share_v),
                (scores_hbm, scores_v), (gate_hbm, gate_v), (residual_hbm, residual_v),
                (mix_gain_hbm, mix_gain_ref), (expert_gain_hbm, expert_gain_ref),
            )
        )
    ]
    for load in loads:
        load.start()

    def sp_device(index):
        return {Z: lax.div(index, groups), Y: lax.div(lax.rem(index, groups), cs), CORE: lax.rem(index, cs)}

    following, preceding = lax.rem(me + 1, devices), lax.rem(me + devices - 1, devices)
    x_peers = [{X: lax.rem(x + o, xs)} for o in range(1, xs)]
    z_peers = [{Z: lax.rem(z + o, zs)} for o in range(1, zs)]
    g_peers = []
    for o in range(1, groups):
        g = lax.rem(g_me + o, groups)
        g_peers.append({Y: lax.div(g, cs), CORE: lax.rem(g, cs)})
    everyone = x_peers + z_peers + g_peers + [sp_device(following), sp_device(preceding)]
    barrier = pltpu.get_barrier_semaphore()
    for peer in everyone:
        pl.semaphore_signal(barrier, inc=1, device_id=peer, device_id_type=MESH)

    loads[0].wait()
    loads[1].wait()
    last = tails.shape[1]
    tails[0] = inner_v[length - last :, :]
    tails[1] = input_v[length - last :, :]
    pl.semaphore_wait(barrier, len(everyone))
    tail_copy = pltpu.make_async_remote_copy(
        src_ref=tails, dst_ref=tail_in, send_sem=t_send, recv_sem=t_recv,
        device_id=sp_device(following), device_id_type=MESH,
    )
    tail_copy.start()

    pad = 8
    for b in range(xs):
        at = slice(b * rows, (b + 1) * rows)
        products[pad + b * rows : pad + (b + 1) * rows, :] = inner_v[at, :].astype(f32) * input_v[at, :].astype(f32)
    loads[2].wait()
    loads[3].wait()
    for b in reversed(range(xs)):
        if b == 0:
            tail_copy.wait_recv()
            earlier = tail_in[0].astype(f32) * tail_in[1].astype(f32)
            earlier = jnp.where(me == 0, jnp.zeros_like(earlier), earlier)
            products[0:pad, :] = earlier[last - pad :, :]
        start = b * rows
        conv = taps_ref[0:1, :] * products[start + pad - 2 : start + pad - 2 + rows, :]
        conv = conv + taps_ref[1:2, :] * products[start + pad - 1 : start + pad - 1 + rows, :]
        conv = conv + taps_ref[2:3, :] * products[start + pad : start + pad + rows, :]
        mixed[start : start + rows, :] = (outer_v[start : start + rows, :].astype(f32) * conv).astype(bf)
    loads[4].wait()

    right, left = lax.rem(x + 1, xs), lax.rem(x + xs - 1, xs)
    ways = (right, left)

    def partial_of(owner, h):
        block = mixed[pl.ds(pl.multiple_of(owner * rows, 16), rows), :]
        return dot32(block, weight_v[:, h * half : (h + 1) * half])

    def far_copy(h, t):
        at = pl.ds(t * piece, piece)
        return pltpu.make_async_remote_copy(
            src_ref=far.at[h, at], dst_ref=far_in.at[h, at],
            send_sem=f_send.at[h, t], recv_sem=f_recv.at[h, t],
            device_id={X: ways[h]}, device_id_type=MESH,
        )

    def near_copy(d, h, t):
        at = pl.ds(t * piece, piece)
        return pltpu.make_async_remote_copy(
            src_ref=near.at[d, h, at], dst_ref=near_in.at[d, h, at],
            send_sem=n_send.at[d, h, t], recv_sem=n_recv.at[d, h, t],
            device_id={X: ways[d]}, device_id_type=MESH,
        )

    steps = [functools.partial(far_copy, t=t) for t in range(parts)]
    steps += [lambda d, t=t: near_copy(d, 1 - d, t) for t in range(parts)]
    steps += [lambda d, t=t: near_copy(d, d, t) for t in range(parts)]

    opposite = lax.rem(x + 2, xs)
    for h in range(2):
        far[h] = partial_of(opposite, h).astype(bf)
        for t in range(WINDOW):
            steps[t](h).start()
    for d in range(2):
        near[d, 1 - d] = partial_of(ways[d], 1 - d).astype(bf)
    for d in range(2):
        own[:, d * half : (d + 1) * half] = partial_of(ways[d], d)

    def step(i):
        for d in range(2):
            steps[i](d).wait_recv()
            if i < parts:
                at = slice(i * piece, (i + 1) * piece)
                near[d, d, at, :] = (own[at, d * half : (d + 1) * half] + far_in[d, at, :].astype(f32)).astype(bf)
            if i + WINDOW < len(steps):
                steps[i + WINDOW](d).start()

    step(0)
    tokens = ids_v.shape[1]
    for load in loads[5:8]:
        load.wait()
    table[...] = jnp.zeros_like(table)
    table[0:2, 0:tokens] = ids_v[...].astype(f32)
    table[2:4, 0:tokens] = scores_v[...]
    table[4:5, 0:tokens] = share_v[...]
    given = jnp.transpose(table[...])[0:tokens, :]
    expert = [given[:, k : k + 1] for k in range(2)]
    z_of = [jnp.floor((e + 0.5) / groups) for e in expert]
    lane = lax.broadcasted_iota(jnp.int32, (tokens, 128), 1).astype(f32)
    marks = [
        jnp.where((e == lane) | (zz + devices == lane), jnp.ones((), f32), jnp.zeros((), f32))
        for e, zz in zip(expert, z_of)
    ]
    before = jnp.where(
        lax.broadcasted_iota(jnp.int32, (tokens, tokens), 1) < lax.broadcasted_iota(jnp.int32, (tokens, tokens), 0),
        jnp.ones((), f32), jnp.zeros((), f32),
    ).astype(bf)
    first_sum = jnp.sum(marks[0], axis=0, keepdims=True)
    most = first_sum + jnp.sum(marks[1], axis=0, keepdims=True)
    most = jnp.where(lane[0:1, :] >= devices, most, jnp.zeros_like(most))
    most = jnp.broadcast_to(jnp.max(most, axis=1, keepdims=True), (8, 128))
    mine[...] = most

    def flag_copy(src, dst, send, recv, i, peer):
        return pltpu.make_async_remote_copy(
            src_ref=src, dst_ref=dst.at[i], send_sem=send.at[i], recv_sem=recv.at[i],
            device_id=peer, device_id_type=MESH,
        )

    x_flags = [flag_copy(mine, x_in, mx_send, mx_recv, i, p) for i, p in enumerate(x_peers)]
    g_flags = [flag_copy(sent_x, g_in, mg_send, mg_recv, i, p) for i, p in enumerate(g_peers)]
    z_flags = [flag_copy(sent_g, z_in, mz_send, mz_recv, i, p) for i, p in enumerate(z_peers)]
    for flag in x_flags:
        flag.start()

    seen = [dot32(before, marks[0].astype(bf)), dot32(before, marks[1].astype(bf)) + first_sum]
    info = []
    step(1)
    scores = [given[:, 2 + k : 3 + k] for k in range(2)]
    top = jnp.maximum(scores[0], scores[1])
    powers = [jnp.exp(v - top) for v in scores]
    for k in range(2):
        hit = marks[k] * seen[k]
        rank = jnp.sum(jnp.where(lane < devices, hit, 0.0), axis=1, keepdims=True)
        place = jnp.sum(jnp.where(lane >= devices, hit, 0.0), axis=1, keepdims=True)
        slot = (expert[k] - groups * z_of[k]) * (zs * limit) + (z * limit).astype(f32) + rank
        info.append((z_of[k], place, slot, given[:, 4:5] * (powers[k] / (powers[0] + powers[1]))))
    column = jnp.zeros((tokens, 128), f32)
    for i in range(4):
        for k in range(2):
            column = column + jnp.where(lane == 2 * i + k, info[k][i], 0.0)
    columns_ref[...] = column
    spare = jnp.zeros((table.shape[1] - tokens, 128), f32)
    lanes_ref[...] = jnp.transpose(jnp.concatenate([column, spare], axis=0))[0:8, :]
    step(2)

    for flag in x_flags:
        flag.wait_recv()
    for i in range(xs - 1):
        most = jnp.maximum(most, x_in[i])
    sent_x[...] = most
    for flag in g_flags:
        flag.start()

    for i in range(3, parts):
        step(i)
    for h in range(2):
        own[:, h * half : (h + 1) * half] = partial_of(x, h)

    for flag in g_flags:
        flag.wait_recv()
    for i in range(groups - 1):
        most = jnp.maximum(most, g_in[i])
    sent_g[...] = most
    for flag in z_flags:
        flag.start()

    for load in loads[8:]:
        load.wait()
    for i in range(parts, 2 * parts):
        step(i)
    for t in range(parts):
        at = slice(t * piece, (t + 1) * piece)
        step(2 * parts + t)
        sums = []
        for h in range(2):
            part = own[at, h * half : (h + 1) * half]
            sums.append(part + near_in[0, h, at, :].astype(f32) + near_in[1, h, at, :].astype(f32))
        projected = jnp.concatenate(sums, axis=1)
        value = jax.nn.sigmoid(gate_v[at, :].astype(f32)) * projected
        hidden = (residual_v[at, :].astype(f32) + rms_scale(value, mix_gain_ref[...])).astype(bf)
        hidden_ref[at, :] = hidden
        normed_ref[at, :] = rms_scale(hidden.astype(f32), expert_gain_ref[...]).astype(bf)

    for flag in z_flags:
        flag.wait_recv()
    for i in range(zs - 1):
        most = jnp.maximum(most, z_in[i])
    most_ref[...] = most

    tail_copy.wait_send()
    for h in range(2):
        for t in range(parts):
            far_copy(h, t).wait_send()
            for d in range(2):
                near_copy(d, h, t).wait_send()
    for flag in x_flags + g_flags + z_flags:
        flag.wait_send()


def mixer(outer, inner, values, taps, weight, gate, residual, mix_gain, expert_gain, ids, share, scores, limit):
    sizes = tuple(lax.axis_size(a) for a in SP_TP)
    zs, ys, cs, xs = sizes
    groups = ys * cs
    length, lanes = inner.shape
    rows, model = residual.shape
    half, parts, last = model // 2, 4, 16
    bf, f32 = jnp.bfloat16, jnp.float32
    vmem, anywhere = pl.BlockSpec(memory_space=pltpu.VMEM), pl.BlockSpec(memory_space=pltpu.HBM)
    dma = pltpu.SemaphoreType.DMA
    flag = (8, 128)
    return pl.pallas_call(
        functools.partial(mixer_kernel, sizes, limit, parts),
        out_shape=(
            jax.ShapeDtypeStruct((rows, model), bf),
            jax.ShapeDtypeStruct((rows, model), bf),
            jax.ShapeDtypeStruct((rows, 128), f32),
            jax.ShapeDtypeStruct((8, 256), f32),
            jax.ShapeDtypeStruct(flag, f32),
        ),
        in_specs=[anywhere] * 12,
        out_specs=(vmem,) * 5,
        scratch_shapes=[
            pltpu.VMEM(taps.shape, f32), pltpu.VMEM((1, model), f32), pltpu.VMEM((1, model), f32),
            pltpu.VMEM((2, rows), jnp.int32), pltpu.VMEM((1, rows), f32), pltpu.VMEM((2, rows), f32),
            pltpu.VMEM(outer.shape, bf), pltpu.VMEM(inner.shape, bf), pltpu.VMEM(values.shape, bf),
            pltpu.VMEM(weight.shape, bf), pltpu.VMEM(gate.shape, bf), pltpu.VMEM(residual.shape, bf),
            pltpu.VMEM((length + 8, lanes), f32),
            pltpu.VMEM((length, lanes), bf),
            pltpu.VMEM((rows, model), f32),
            pltpu.VMEM((2, rows, half), bf), pltpu.VMEM((2, rows, half), bf),
            pltpu.VMEM((2, 2, rows, half), bf), pltpu.VMEM((2, 2, rows, half), bf),
            pltpu.VMEM((2, last, lanes), bf), pltpu.VMEM((2, last, lanes), bf),
            pltpu.VMEM((128, 256), f32),
            pltpu.VMEM(flag, f32), pltpu.VMEM((xs - 1, *flag), f32),
            pltpu.VMEM((groups - 1, *flag), f32), pltpu.VMEM((zs - 1, *flag), f32),
            pltpu.VMEM(flag, f32), pltpu.VMEM(flag, f32),
            dma((12,)), dma, dma,
            dma((2, parts)), dma((2, parts)), dma((2, 2, parts)), dma((2, 2, parts)),
            dma((xs - 1,)), dma((xs - 1,)), dma((groups - 1,)), dma((groups - 1,)), dma((zs - 1,)), dma((zs - 1,)),
        ],
        compiler_params=pltpu.CompilerParams(
            collective_id=1, has_side_effects=True, vmem_limit_bytes=VMEM_LIMIT
        ),
        name="mixer",
    )(
        taps, mix_gain[None, :], expert_gain[None, :], ids.T, share[None, :], scores.T,
        outer, inner, values, weight, gate, residual,
    )


def expert_kernel(
    zs, ys, cs, cap, slots,
    normed_ref, hidden_ref, columns_ref, lanes_ref, gate_hbm, up_hbm, down_hbm,
    out_ref,
    pick_ref, meta_ref, whi_ref, wlo_ref, s1, r1, s2, r2, o2, b2, o1, b1, metar, onehot_t, onehot, acc, act, gate_v, up_v, down_v,
    z_send, z_recv, g_send, g_recv, bg_send, bg_recv, bz_send, bz_recv, m_send, m_recv, w_sem,
):
    z, y, c = lax.axis_index(Z), lax.axis_index(Y), lax.axis_index(CORE)
    groups = ys * cs
    g_me = y * cs + c
    chunks = s1.shape[0]
    width = s1.shape[3]
    bf = jnp.bfloat16

    weights = [
        pltpu.make_async_copy(src, dst, w_sem.at[i])
        for i, (src, dst) in enumerate(((gate_hbm, gate_v), (up_hbm, up_v), (down_hbm, down_v)))
    ]
    for copy in weights:
        copy.start()

    def z_peer(o):
        return lax.rem(z + o, zs)

    def g_peer(o):
        return lax.rem(g_me + o, groups)

    def g_device(g):
        return {Y: lax.div(g, cs), CORE: lax.rem(g, cs)}

    barrier = pltpu.get_barrier_semaphore()
    for o in range(1, zs):
        pl.semaphore_signal(barrier, inc=1, device_id={Z: z_peer(o)}, device_id_type=MESH)
    for o in range(1, groups):
        pl.semaphore_signal(barrier, inc=1, device_id=g_device(g_peer(o)), device_id_type=MESH)
    pl.semaphore_wait(barrier, zs + groups - 2)

    def z_copy(src, dst, send, recv, k, o):
        return pltpu.make_async_remote_copy(
            src_ref=src.at[k, z_peer(o)], dst_ref=dst.at[k, z],
            send_sem=send.at[k, o - 1], recv_sem=recv.at[k, o - 1],
            device_id={Z: z_peer(o)}, device_id_type=MESH,
        )

    def g_copy(src, dst, send, recv, k, o):
        return pltpu.make_async_remote_copy(
            src_ref=src.at[k, g_peer(o)], dst_ref=dst.at[k, g_me],
            send_sem=send.at[k, o - 1], recv_sem=recv.at[k, o - 1],
            device_id=g_device(g_peer(o)), device_id_type=MESH,
        )

    def m_copy(o):
        return pltpu.make_async_remote_copy(
            src_ref=meta_ref.at[z_peer(o)], dst_ref=metar.at[z],
            send_sem=m_send.at[o - 1], recv_sem=m_recv.at[o - 1],
            device_id={Z: z_peer(o)}, device_id_type=MESH,
        )

    z_sends = functools.partial(z_copy, s1, r1, z_send, z_recv)
    g_sends = functools.partial(g_copy, s2, r2, g_send, g_recv)
    g_backs = functools.partial(g_copy, o2, b2, bg_send, bg_recv)
    z_backs = functools.partial(z_copy, o1, b1, bz_send, bz_recv)

    def start_all(copies, k, count):
        for o in range(1, count):
            copies(k, o).start()

    def wait_recv_all(copies, k, count):
        for o in range(1, count):
            copies(k, o).wait_recv()

    def columns(k):
        return pl.ds(pl.multiple_of(k * width, width), width)

    f32 = jnp.float32
    tokens = normed_ref.shape[0]
    row_of = [lanes_ref[k : k + 1, 0:tokens] * cap + lanes_ref[2 + k : 3 + k, 0:tokens] for k in range(2)]
    slot_of = [lanes_ref[4 + k : 5 + k, 0:tokens] + 1.0 for k in range(2)]
    place = lax.broadcasted_iota(jnp.int32, (cap, tokens), 0).astype(f32)
    for j in range(zs):
        hit = [place + float(j * cap) == r for r in row_of]
        pick_ref[j * cap : (j + 1) * cap, :] = jnp.where(hit[0] | hit[1], jnp.ones((), f32), jnp.zeros((), f32)).astype(bf)

    def pick_rows(k):
        values = normed_ref[:, columns(k)]
        s1[k] = dot32(pick_ref[...], values).astype(bf).reshape(zs, cap, width)
        r1[k, z] = s1[k, z]

    for k in range(DEPTH):
        pick_rows(k)
        start_all(z_sends, k, zs)

    for j in range(zs):
        hit = [place + float(j * cap) == r for r in row_of]
        found = jnp.where(hit[0], slot_of[0], 0.0) + jnp.where(hit[1], slot_of[1], 0.0)
        found = jnp.broadcast_to(jnp.sum(found, axis=1, keepdims=True) - 1.0, (cap, 128))
        found = jnp.concatenate([found, jnp.full((128 - cap, 128), -1.0, f32)], axis=0)
        meta_ref[j] = jnp.transpose(found)[0:8, :]
    for o in range(1, zs):
        m_copy(o).start()
    row_lane = lax.broadcasted_iota(jnp.int32, (tokens, zs * cap), 1).astype(f32)
    weigh = jnp.zeros((tokens, zs * cap), f32)
    for k in range(2):
        row = columns_ref[:, k : k + 1] * cap + columns_ref[:, 2 + k : 3 + k]
        weigh = weigh + jnp.where(row == row_lane, columns_ref[:, 6 + k : 7 + k], 0.0)
    whi_ref[...] = weigh.astype(bf)
    wlo_ref[...] = (weigh - whi_ref[...].astype(f32)).astype(bf)
    metar[z] = meta_ref[z]

    @pl.loop(DEPTH, chunks)
    def _(k):
        pick_rows(k)

    for o in range(1, zs):
        m_copy(o).wait_recv()
    total = groups * slots
    places = lax.broadcasted_iota(jnp.int32, (cap, total), 1).astype(jnp.float32)

    @pl.loop(0, zs)
    def _(j):
        where = jnp.transpose(metar[j])[:cap, 0:1]
        onehot_t[pl.ds(pl.multiple_of(j * cap, 16), cap), :] = jnp.where(
            where == places, jnp.ones((), jnp.float32), jnp.zeros((), jnp.float32)
        ).astype(bf)

    @pl.loop(0, zs * cap // 128)
    def _(j):
        rows = pl.ds(pl.multiple_of(j * 128, 128), 128)
        onehot[:, rows] = jnp.transpose(onehot_t[rows, :].astype(jnp.float32)).astype(bf)

    weights[0].wait()
    weights[1].wait()
    acc[...] = jnp.zeros_like(acc)
    hidden_units = gate_v.shape[1]

    @pl.loop(0, chunks + 1)
    def _(k):
        @pl.when(k < chunks)
        def _():
            wait_recv_all(z_sends, k, zs)

            @pl.when(k + DEPTH < chunks)
            def _():
                start_all(z_sends, k + DEPTH, zs)

            rows = r1[k].reshape(zs * cap, width)
            for half in range(2):
                at = slice(half * total // 2, (half + 1) * total // 2)
                s2[k, half * groups // 2 : (half + 1) * groups // 2] = (
                    dot32(onehot[at, :], rows).astype(bf).reshape(groups // 2, slots, width)
                )
            start_all(g_sends, k, groups)
            r2[k, g_me] = s2[k, g_me]

        @pl.when(k >= 1)
        def _():
            b = k - 1
            wait_recv_all(g_sends, b, groups)
            ks = pl.ds(pl.multiple_of(b * width, width), width)
            for half in range(2):
                rows = r2[b, half * groups // 2 : (half + 1) * groups // 2].reshape(total // 2, width)
                at = slice(half * total // 2, (half + 1) * total // 2)
                acc[at, :hidden_units] += dot32(rows, gate_v[ks, :])
                acc[at, hidden_units:] += dot32(rows, up_v[ks, :])

    @pl.loop(0, groups)
    def _(g):
        at = pl.ds(pl.multiple_of(g * slots, slots), slots)
        first = acc[at, :hidden_units]
        second = acc[at, hidden_units:]
        act[at, :] = (first / (1.0 + jnp.exp(-first)) * second).astype(bf)

    weights[2].wait()

    def outputs_of(k):
        down = down_v[:, columns(k)]
        for half in range(2):
            at = slice(half * total // 2, (half + 1) * total // 2)
            o2[k, half * groups // 2 : (half + 1) * groups // 2] = (
                dot32(act[at, :], down).astype(bf).reshape(groups // 2, slots, width)
            )
        b2[k, g_me] = o2[k, g_me]

    for k in range(DEPTH):
        outputs_of(k)
        start_all(g_backs, k, groups)

    @pl.loop(DEPTH, chunks)
    def _(k):
        outputs_of(k)

    @pl.loop(0, chunks + DEPTH)
    def _(k):
        @pl.when(k < chunks)
        def _():
            wait_recv_all(g_backs, k, groups)

            @pl.when(k + DEPTH < chunks)
            def _():
                start_all(g_backs, k + DEPTH, groups)

            rows = b2[k].reshape(total, width)
            o1[k] = dot32(onehot_t[...], rows).astype(bf).reshape(zs, cap, width)
            b1[k, z] = o1[k, z]

        @pl.when(k >= DEPTH)
        def _():
            wait_recv_all(z_backs, k - DEPTH, zs)

        @pl.when(k < chunks)
        def _():
            start_all(z_backs, k, zs)

        @pl.when(k >= DEPTH)
        def _():
            b = k - DEPTH
            rows = b1[b].reshape(zs * cap, width)
            value = hidden_ref[:, columns(b)].astype(jnp.float32)
            value = value + (dot32(whi_ref[...], rows) + dot32(wlo_ref[...], rows))
            out_ref[:, columns(b)] = value.astype(bf)

    for o in range(1, zs):
        m_copy(o).wait_send()

    @pl.loop(0, chunks)
    def _(k):
        for o in range(1, zs):
            z_sends(k, o).wait_send()
            z_backs(k, o).wait_send()
        for o in range(1, groups):
            g_sends(k, o).wait_send()
            g_backs(k, o).wait_send()


def routed_experts(cap, limit, collective, normed, hidden, columns, lanes, gate, up, down):
    zs, ys, cs = lax.axis_size(Z), lax.axis_size(Y), lax.axis_size(CORE)
    groups = ys * cs
    tokens, model = normed.shape
    slots = zs * limit
    rows = zs * cap
    chunks = model // WIDTH
    units = gate.shape[1]
    bf = jnp.bfloat16
    vmem, anywhere = pl.BlockSpec(memory_space=pltpu.VMEM), pl.BlockSpec(memory_space=pltpu.HBM)
    z_block, g_block = (chunks, zs, cap, WIDTH), (chunks, groups, slots, WIDTH)
    z_sem, g_sem = pltpu.SemaphoreType.DMA((chunks, zs - 1)), pltpu.SemaphoreType.DMA((chunks, groups - 1))
    m_sem = pltpu.SemaphoreType.DMA((zs - 1,))
    total = groups * slots
    return pl.pallas_call(
        functools.partial(expert_kernel, zs, ys, cs, cap, slots),
        out_shape=jax.ShapeDtypeStruct((tokens, model), bf),
        in_specs=[vmem] * 4 + [anywhere] * 3,
        out_specs=vmem,
        scratch_shapes=[
            pltpu.VMEM((rows, tokens), bf), pltpu.VMEM((zs, 8, 128), jnp.float32),
            pltpu.VMEM((tokens, rows), bf), pltpu.VMEM((tokens, rows), bf),
            pltpu.VMEM(z_block, bf), pltpu.VMEM(z_block, bf),
            pltpu.VMEM(g_block, bf), pltpu.VMEM(g_block, bf),
            pltpu.VMEM(g_block, bf), pltpu.VMEM(g_block, bf),
            pltpu.VMEM(z_block, bf), pltpu.VMEM(z_block, bf),
            pltpu.VMEM((zs, 8, 128), jnp.float32),
            pltpu.VMEM((rows, total), bf),
            pltpu.VMEM((total, rows), bf),
            pltpu.VMEM((total, 2 * units), jnp.float32),
            pltpu.VMEM((total, units), bf),
            pltpu.VMEM(gate.shape, bf), pltpu.VMEM(up.shape, bf), pltpu.VMEM(down.shape, bf),
            z_sem, z_sem, g_sem, g_sem, g_sem, g_sem, z_sem, z_sem, m_sem, m_sem,
            pltpu.SemaphoreType.DMA((3,)),
        ],
        compiler_params=pltpu.CompilerParams(
            collective_id=collective, has_side_effects=True, vmem_limit_bytes=VMEM_LIMIT
        ),
        name="routed_experts",
    )(normed, hidden, columns, lanes, gate, up, down)


def per_device(
    conv_outer,
    conv_inner,
    conv_input,
    conv_taps,
    out_weight,
    mix_gate,
    residual,
    mix_gain,
    expert_gain,
    expert_ids,
    group_share,
    pair_scores,
    gate_experts,
    up_experts,
    down_experts,
):
    limit = 2 * expert_ids.shape[1] * residual.shape[0] // (lax.axis_size(SP) * gate_experts.shape[0])
    worst = limit * lax.axis_size(Y) * lax.axis_size(CORE)
    hidden, normed, columns, lanes, most = mixer(
        conv_outer, conv_inner, conv_input, conv_taps, out_weight, mix_gate, residual, mix_gain, expert_gain,
        expert_ids, group_share, pair_scores, limit,
    )
    arguments = (normed, hidden, columns, lanes, gate_experts[0], up_experts[0], down_experts[0])
    usual = USUAL
    return lax.cond(
        most[0, 0] <= usual,
        functools.partial(routed_experts, usual, limit, 2),
        functools.partial(routed_experts, worst, limit, 3),
        *arguments,
    )


def solution(mesh):
    torus = Mesh(mesh.devices.reshape(8, 4, 2, mesh.shape["tp"]), SP_TP)
    return jax.shard_map(
        per_device,
        mesh=torus,
        in_specs=(
            P(SP, X),
            P(SP, X),
            P(SP, X),
            P(None, X),
            P(X, None),
            P(SP_TP, None),
            P(SP_TP, None),
            P(),
            P(),
            P(SP_TP, None),
            P(SP_TP),
            P(SP_TP, None),
            P(SP, None, None),
            P(SP, None, None),
            P(SP, None, None),
        ),
        out_specs=P(SP_TP, None),
        check_vma=False,
    )
```

```python
import functools

import jax
import jax.numpy as jnp
from jax import lax
from jax.experimental import pallas as pl
from jax.experimental.pallas import tpu as pltpu
from jax.sharding import Mesh
from jax.sharding import PartitionSpec as P

Z, Y, CORE, X = "sp_0", "sp_1", "sp_2", "tp"
SP = (Z, Y, CORE)
SP_TP = (Z, Y, CORE, X)
MESH = pl.DeviceIdType.MESH

epsilon = 1e-06
WIDTH = 512
VMEM_LIMIT = 67043328
DEPTH = 2
WINDOW = 3
USUAL = 40


def rms_scale(values, gain):
    return values * lax.rsqrt(jnp.mean(values * values, axis=-1, keepdims=True) + epsilon) * gain


def dot32(a, b):
    return jnp.dot(a, b, preferred_element_type=jnp.float32)


def mixer_kernel(
    sizes, limit, parts,
    taps_hbm, mix_gain_hbm, expert_gain_hbm, ids_hbm, share_hbm, scores_hbm,
    outer_hbm, inner_hbm, input_hbm, weight_hbm, gate_hbm, residual_hbm,
    hidden_ref, normed_ref, columns_ref, lanes_ref, most_ref,
    taps_ref, mix_gain_ref, expert_gain_ref, ids_v, share_v, scores_v,
    outer_v, inner_v, input_v, weight_v, gate_v, residual_v,
    products, mixed, own, far, far_in, near, near_in, tails, tail_in, table,
    mine, x_in, g_in, z_in, sent_x, sent_g,
    l_sem, t_send, t_recv, f_send, f_recv, n_send, n_recv, mx_send, mx_recv, mg_send, mg_recv, mz_send, mz_recv,
):
    zs, ys, cs, xs = sizes
    z, y, c, x = (lax.axis_index(a) for a in SP_TP)
    groups = ys * cs
    g_me = y * cs + c
    devices = zs * groups
    me = z * groups + g_me
    bf, f32 = jnp.bfloat16, jnp.float32
    length, lanes = inner_v.shape
    rows = length // xs
    half = own.shape[1] // 2
    piece = rows // parts

    loads = [
        pltpu.make_async_copy(src, dst, l_sem.at[i])
        for i, (src, dst) in enumerate(
            (
                (inner_hbm, inner_v), (input_hbm, input_v), (outer_hbm, outer_v),
                (taps_hbm, taps_ref), (weight_hbm, weight_v), (ids_hbm, ids_v), (share_hbm, share_v),
                (scores_hbm, scores_v), (gate_hbm, gate_v), (residual_hbm, residual_v),
                (mix_gain_hbm, mix_gain_ref), (expert_gain_hbm, expert_gain_ref),
            )
        )
    ]
    for load in loads:
        load.start()

    def sp_device(index):
        return {Z: lax.div(index, groups), Y: lax.div(lax.rem(index, groups), cs), CORE: lax.rem(index, cs)}

    following, preceding = lax.rem(me + 1, devices), lax.rem(me + devices - 1, devices)
    x_peers = [{X: lax.rem(x + o, xs)} for o in range(1, xs)]
    z_peers = [{Z: lax.rem(z + o, zs)} for o in range(1, zs)]
    g_peers = []
    for o in range(1, groups):
        g = lax.rem(g_me + o, groups)
        g_peers.append({Y: lax.div(g, cs), CORE: lax.rem(g, cs)})
    everyone = x_peers + z_peers + g_peers + [sp_device(following), sp_device(preceding)]
    barrier = pltpu.get_barrier_semaphore()
    for peer in everyone:
        pl.semaphore_signal(barrier, inc=1, device_id=peer, device_id_type=MESH)

    loads[0].wait()
    loads[1].wait()
    last = tails.shape[1]
    tails[0] = inner_v[length - last :, :]
    tails[1] = input_v[length - last :, :]
    pl.semaphore_wait(barrier, len(everyone))
    tail_copy = pltpu.make_async_remote_copy(
        src_ref=tails, dst_ref=tail_in, send_sem=t_send, recv_sem=t_recv,
        device_id=sp_device(following), device_id_type=MESH,
    )
    tail_copy.start()

    pad = 8
    for b in range(xs):
        at = slice(b * rows, (b + 1) * rows)
        products[pad + b * rows : pad + (b + 1) * rows, :] = inner_v[at, :].astype(f32) * input_v[at, :].astype(f32)
    loads[2].wait()
    loads[3].wait()
    for b in reversed(range(xs)):
        if b == 0:
            tail_copy.wait_recv()
            earlier = tail_in[0].astype(f32) * tail_in[1].astype(f32)
            earlier = jnp.where(me == 0, jnp.zeros_like(earlier), earlier)
            products[0:pad, :] = earlier[last - pad :, :]
        start = b * rows
        conv = taps_ref[0:1, :] * products[start + pad - 2 : start + pad - 2 + rows, :]
        conv = conv + taps_ref[1:2, :] * products[start + pad - 1 : start + pad - 1 + rows, :]
        conv = conv + taps_ref[2:3, :] * products[start + pad : start + pad + rows, :]
        mixed[start : start + rows, :] = (outer_v[start : start + rows, :].astype(f32) * conv).astype(bf)
    loads[4].wait()

    right, left = lax.rem(x + 1, xs), lax.rem(x + xs - 1, xs)
    ways = (right, left)

    def partial_of(owner, h):
        block = mixed[pl.ds(pl.multiple_of(owner * rows, 16), rows), :]
        return dot32(block, weight_v[:, h * half : (h + 1) * half])

    def far_copy(h, t):
        at = pl.ds(t * piece, piece)
        return pltpu.make_async_remote_copy(
            src_ref=far.at[h, at], dst_ref=far_in.at[h, at],
            send_sem=f_send.at[h, t], recv_sem=f_recv.at[h, t],
            device_id={X: ways[h]}, device_id_type=MESH,
        )

    def near_copy(d, h, t):
        at = pl.ds(t * piece, piece)
        return pltpu.make_async_remote_copy(
            src_ref=near.at[d, h, at], dst_ref=near_in.at[d, h, at],
            send_sem=n_send.at[d, h, t], recv_sem=n_recv.at[d, h, t],
            device_id={X: ways[d]}, device_id_type=MESH,
        )

    steps = [functools.partial(far_copy, t=t) for t in range(parts)]
    steps += [lambda d, t=t: near_copy(d, 1 - d, t) for t in range(parts)]
    steps += [lambda d, t=t: near_copy(d, d, t) for t in range(parts)]

    opposite = lax.rem(x + 2, xs)
    for h in range(2):
        far[h] = partial_of(opposite, h).astype(bf)
        for t in range(WINDOW):
            steps[t](h).start()
    for d in range(2):
        near[d, 1 - d] = partial_of(ways[d], 1 - d).astype(bf)
    for d in range(2):
        own[:, d * half : (d + 1) * half] = partial_of(ways[d], d)

    def step(i):
        for d in range(2):
            steps[i](d).wait_recv()
            if i < parts:
                at = slice(i * piece, (i + 1) * piece)
                near[d, d, at, :] = (own[at, d * half : (d + 1) * half] + far_in[d, at, :].astype(f32)).astype(bf)
            if i + WINDOW < len(steps):
                steps[i + WINDOW](d).start()

    step(0)
    tokens = ids_v.shape[1]
    for load in loads[5:8]:
        load.wait()
    table[...] = jnp.zeros_like(table)
    table[0:2, 0:tokens] = ids_v[...].astype(f32)
    table[2:4, 0:tokens] = scores_v[...]
    table[4:5, 0:tokens] = share_v[...]
    given = jnp.transpose(table[...])[0:tokens, :]
    expert = [given[:, k : k + 1] for k in range(2)]
    z_of = [jnp.floor((e + 0.5) / groups) for e in expert]
    lane = lax.broadcasted_iota(jnp.int32, (tokens, 128), 1).astype(f32)
    before = jnp.where(
        lax.broadcasted_iota(jnp.int32, (tokens, tokens), 1) < lax.broadcasted_iota(jnp.int32, (tokens, tokens), 0),
        jnp.ones((), f32), jnp.zeros((), f32),
    ).astype(bf)

    def ranks(labels):
        marks = [jnp.where(label == lane, jnp.ones((), f32), jnp.zeros((), f32)) for label in labels]
        firsts = jnp.sum(marks[0], axis=0, keepdims=True)
        seen = [dot32(before, marks[0].astype(bf)), dot32(before, marks[1].astype(bf)) + firsts]
        found = [jnp.sum(mark * s, axis=1, keepdims=True) for mark, s in zip(marks, seen)]
        return found, jnp.max(firsts + jnp.sum(marks[1], axis=0, keepdims=True), axis=1, keepdims=True)

    rank, _ = ranks(expert)
    lower = [jnp.floor(r * 0.5) for r in rank]
    parity = [r + e - 2.0 * jnp.floor((r + e) * 0.5) for r, e in zip(rank, expert)]
    block = [h * zs + zz for h, zz in zip(parity, z_of)]
    place, most = ranks(block)
    most = jnp.broadcast_to(most, (8, 128))
    mine[...] = most

    def flag_copy(src, dst, send, recv, i, peer):
        return pltpu.make_async_remote_copy(
            src_ref=src, dst_ref=dst.at[i], send_sem=send.at[i], recv_sem=recv.at[i],
            device_id=peer, device_id_type=MESH,
        )

    x_flags = [flag_copy(mine, x_in, mx_send, mx_recv, i, p) for i, p in enumerate(x_peers)]
    g_flags = [flag_copy(sent_x, g_in, mg_send, mg_recv, i, p) for i, p in enumerate(g_peers)]
    z_flags = [flag_copy(sent_g, z_in, mz_send, mz_recv, i, p) for i, p in enumerate(z_peers)]
    for flag in x_flags:
        flag.start()

    info = []
    step(1)
    scores = [given[:, 2 + k : 3 + k] for k in range(2)]
    top = jnp.maximum(scores[0], scores[1])
    powers = [jnp.exp(v - top) for v in scores]
    for k in range(2):
        slot = (expert[k] - groups * z_of[k]) * (zs * limit / 2) + (z * limit).astype(f32) * 0.5 + lower[k]
        info.append((block[k], place[k], slot, given[:, 4:5] * (powers[k] / (powers[0] + powers[1]))))
    column = jnp.zeros((tokens, 128), f32)
    for i in range(4):
        for k in range(2):
            column = column + jnp.where(lane == 2 * i + k, info[k][i], 0.0)
    columns_ref[...] = column
    spare = jnp.zeros((table.shape[1] - tokens, 128), f32)
    lanes_ref[...] = jnp.transpose(jnp.concatenate([column, spare], axis=0))[0:8, :]
    step(2)

    for flag in x_flags:
        flag.wait_recv()
    for i in range(xs - 1):
        most = jnp.maximum(most, x_in[i])
    sent_x[...] = most
    for flag in g_flags:
        flag.start()

    for i in range(3, parts):
        step(i)
    for h in range(2):
        own[:, h * half : (h + 1) * half] = partial_of(x, h)

    for flag in g_flags:
        flag.wait_recv()
    for i in range(groups - 1):
        most = jnp.maximum(most, g_in[i])
    sent_g[...] = most
    for flag in z_flags:
        flag.start()

    for load in loads[8:]:
        load.wait()
    for i in range(parts, 2 * parts):
        step(i)
    for t in range(parts):
        at = slice(t * piece, (t + 1) * piece)
        step(2 * parts + t)
        sums = []
        for h in range(2):
            part = own[at, h * half : (h + 1) * half]
            sums.append(part + near_in[0, h, at, :].astype(f32) + near_in[1, h, at, :].astype(f32))
        projected = jnp.concatenate(sums, axis=1)
        value = jax.nn.sigmoid(gate_v[at, :].astype(f32)) * projected
        hidden = (residual_v[at, :].astype(f32) + rms_scale(value, mix_gain_ref[...])).astype(bf)
        hidden_ref[at, :] = hidden
        normed_ref[at, :] = rms_scale(hidden.astype(f32), expert_gain_ref[...]).astype(bf)

    for flag in z_flags:
        flag.wait_recv()
    for i in range(zs - 1):
        most = jnp.maximum(most, z_in[i])
    most_ref[...] = most

    tail_copy.wait_send()
    for h in range(2):
        for t in range(parts):
            far_copy(h, t).wait_send()
            for d in range(2):
                near_copy(d, h, t).wait_send()
    for flag in x_flags + g_flags + z_flags:
        flag.wait_send()


def mixer(outer, inner, values, taps, weight, gate, residual, mix_gain, expert_gain, ids, share, scores, limit):
    sizes = tuple(lax.axis_size(a) for a in SP_TP)
    zs, ys, cs, xs = sizes
    groups = ys * cs
    length, lanes = inner.shape
    rows, model = residual.shape
    half, parts, last = model // 2, 4, 16
    bf, f32 = jnp.bfloat16, jnp.float32
    vmem, anywhere = pl.BlockSpec(memory_space=pltpu.VMEM), pl.BlockSpec(memory_space=pltpu.HBM)
    dma = pltpu.SemaphoreType.DMA
    flag = (8, 128)
    return pl.pallas_call(
        functools.partial(mixer_kernel, sizes, limit, parts),
        out_shape=(
            jax.ShapeDtypeStruct((rows, model), bf),
            jax.ShapeDtypeStruct((rows, model), bf),
            jax.ShapeDtypeStruct((rows, 128), f32),
            jax.ShapeDtypeStruct((8, 256), f32),
            jax.ShapeDtypeStruct(flag, f32),
        ),
        in_specs=[anywhere] * 12,
        out_specs=(vmem,) * 5,
        scratch_shapes=[
            pltpu.VMEM(taps.shape, f32), pltpu.VMEM((1, model), f32), pltpu.VMEM((1, model), f32),
            pltpu.VMEM((2, rows), jnp.int32), pltpu.VMEM((1, rows), f32), pltpu.VMEM((2, rows), f32),
            pltpu.VMEM(outer.shape, bf), pltpu.VMEM(inner.shape, bf), pltpu.VMEM(values.shape, bf),
            pltpu.VMEM(weight.shape, bf), pltpu.VMEM(gate.shape, bf), pltpu.VMEM(residual.shape, bf),
            pltpu.VMEM((length + 8, lanes), f32),
            pltpu.VMEM((length, lanes), bf),
            pltpu.VMEM((rows, model), f32),
            pltpu.VMEM((2, rows, half), bf), pltpu.VMEM((2, rows, half), bf),
            pltpu.VMEM((2, 2, rows, half), bf), pltpu.VMEM((2, 2, rows, half), bf),
            pltpu.VMEM((2, last, lanes), bf), pltpu.VMEM((2, last, lanes), bf),
            pltpu.VMEM((128, 256), f32),
            pltpu.VMEM(flag, f32), pltpu.VMEM((xs - 1, *flag), f32),
            pltpu.VMEM((groups - 1, *flag), f32), pltpu.VMEM((zs - 1, *flag), f32),
            pltpu.VMEM(flag, f32), pltpu.VMEM(flag, f32),
            dma((12,)), dma, dma,
            dma((2, parts)), dma((2, parts)), dma((2, 2, parts)), dma((2, 2, parts)),
            dma((xs - 1,)), dma((xs - 1,)), dma((groups - 1,)), dma((groups - 1,)), dma((zs - 1,)), dma((zs - 1,)),
        ],
        compiler_params=pltpu.CompilerParams(
            collective_id=1, has_side_effects=True, vmem_limit_bytes=VMEM_LIMIT
        ),
        name="mixer",
    )(
        taps, mix_gain[None, :], expert_gain[None, :], ids.T, share[None, :], scores.T,
        outer, inner, values, weight, gate, residual,
    )


def expert_kernel(
    zs, ys, cs, cap, slots,
    normed_ref, hidden_ref, columns_ref, lanes_ref, gate_hbm, up_hbm, down_hbm,
    out_ref,
    pick, weigh, meta, s1, r1, s2, r2, o2, b2, o1, b1, metar, onehot_t, onehot, acc, act, partial,
    gate_v, up_v, down_v,
    z_send, z_recv, g_send, g_recv, bg_send, bg_recv, bz_send, bz_recv, m_send, m_recv, w_sem,
):
    z, y, c = lax.axis_index(Z), lax.axis_index(Y), lax.axis_index(CORE)
    groups = ys * cs
    g_me = y * cs + c
    chunks = s1.shape[0]
    each = chunks // 2
    side = s1.shape[3]
    width = 2 * side
    tokens = normed_ref.shape[0]
    rows = zs * cap
    padded = onehot_t.shape[1]
    total = groups * slots
    bf, f32 = jnp.bfloat16, jnp.float32
    one, zero = jnp.ones((), f32), jnp.zeros((), f32)

    weights = [
        pltpu.make_async_copy(src, dst, w_sem.at[i])
        for i, (src, dst) in enumerate(((gate_hbm, gate_v), (up_hbm, up_v), (down_hbm, down_v)))
    ]
    for copy in weights:
        copy.start()

    def z_peer(o):
        return lax.rem(z + o, zs)

    def g_peer(o):
        return lax.rem(g_me + o, groups)

    def g_device(g):
        return {Y: lax.div(g, cs), CORE: lax.rem(g, cs)}

    barrier = pltpu.get_barrier_semaphore()
    for o in range(1, zs):
        pl.semaphore_signal(barrier, inc=1, device_id={Z: z_peer(o)}, device_id_type=MESH)
    for o in range(1, groups):
        pl.semaphore_signal(barrier, inc=1, device_id=g_device(g_peer(o)), device_id_type=MESH)

    def z_copy(src, dst, send, recv, k, o):
        return pltpu.make_async_remote_copy(
            src_ref=src.at[k, z_peer(o)], dst_ref=dst.at[k, z],
            send_sem=send.at[k, o - 1], recv_sem=recv.at[k, o - 1],
            device_id={Z: z_peer(o)}, device_id_type=MESH,
        )

    def g_copy(src, dst, send, recv, k, o):
        return pltpu.make_async_remote_copy(
            src_ref=src.at[k, g_peer(o)], dst_ref=dst.at[k, g_me],
            send_sem=send.at[k, o - 1], recv_sem=recv.at[k, o - 1],
            device_id=g_device(g_peer(o)), device_id_type=MESH,
        )

    def m_copy(o):
        return pltpu.make_async_remote_copy(
            src_ref=meta.at[z_peer(o)], dst_ref=metar.at[z],
            send_sem=m_send.at[o - 1], recv_sem=m_recv.at[o - 1],
            device_id={Z: z_peer(o)}, device_id_type=MESH,
        )

    z_sends = functools.partial(z_copy, s1, r1, z_send, z_recv)
    g_sends = functools.partial(g_copy, s2, r2, g_send, g_recv)
    g_backs = functools.partial(g_copy, o2, b2, bg_send, bg_recv)
    z_backs = functools.partial(z_copy, o1, b1, bz_send, bz_recv)

    def start_all(copies, k, count):
        for o in range(1, count):
            copies(k, o).start()

    def wait_recv_all(copies, k, count):
        for o in range(1, count):
            copies(k, o).wait_recv()

    def half_of(k):
        return lax.div(k, each)

    def columns(k):
        return pl.ds(pl.multiple_of(lax.rem(k, each) * width, width), width)

    def fold(value):
        parts = []
        for j in range(zs):
            at = slice(j * cap, (j + 1) * cap)
            parts.append(jnp.concatenate([value[at, :side], value[at, side:]], axis=0)[None])
        return jnp.concatenate(parts, axis=0).astype(bf)

    def unfold(ref, k):
        value = ref[k].astype(f32).reshape(zs, 2, cap, side)
        sides = []
        for i in range(2):
            flat = value[:, i].reshape(rows, side)
            if padded > rows:
                flat = jnp.concatenate([flat, jnp.zeros((padded - rows, side), f32)], axis=0)
            sides.append(flat.astype(bf))
        return sides

    def row_of(block, place, h):
        inside = (block >= float(h * zs)) & (block < float((h + 1) * zs))
        return jnp.where(inside, (block - float(h * zs)) * cap + place, -1.0)

    lane_rows = [
        [row_of(lanes_ref[k : k + 1, 0:tokens], lanes_ref[2 + k : 3 + k, 0:tokens], h) for k in range(2)]
        for h in range(2)
    ]
    slot_of = [lanes_ref[4 + k : 5 + k, 0:tokens] + 1.0 for k in range(2)]
    numbers = lax.broadcasted_iota(jnp.int32, (padded, tokens), 0).astype(f32)
    for h in range(2):
        hit = [numbers == r for r in lane_rows[h]]
        pick[h] = jnp.where(hit[0] | hit[1], one, zero).astype(bf)

    def pick_rows(k):
        value = dot32(pick[half_of(k)], normed_ref[:, columns(k)])
        s1[k] = fold(value)
        r1[k, z] = s1[k, z]

    pl.semaphore_wait(barrier, zs + groups - 2)
    for k in range(DEPTH):
        pick_rows(k)
        start_all(z_sends, k, zs)

    place = lax.broadcasted_iota(jnp.int32, (cap, tokens), 0).astype(f32)
    blank = jnp.full((128 - cap, 128), -1.0, f32)
    spot = lax.broadcasted_iota(jnp.int32, (128, 128), 1).astype(f32)
    for j in range(zs):
        both = jnp.zeros((128, 128), f32)
        for h in range(2):
            hit = [place + float(j * cap) == r for r in lane_rows[h]]
            found = jnp.where(hit[0], slot_of[0], 0.0) + jnp.where(hit[1], slot_of[1], 0.0)
            found = jnp.broadcast_to(jnp.sum(found, axis=1, keepdims=True) - 1.0, (cap, 128))
            both = jnp.where(spot == float(h), jnp.concatenate([found, blank], axis=0), both)
        meta[j] = jnp.transpose(both)[0:8, :]
    for o in range(1, zs):
        m_copy(o).start()
    row_lane = lax.broadcasted_iota(jnp.int32, (tokens, padded), 1).astype(f32)
    for h in range(2):
        weight = jnp.zeros((tokens, padded), f32)
        for k in range(2):
            row = row_of(columns_ref[:, k : k + 1], columns_ref[:, 2 + k : 3 + k], h)
            weight = weight + jnp.where(row == row_lane, columns_ref[:, 6 + k : 7 + k], 0.0)
        high = weight.astype(bf)
        weigh[h, 0] = high
        weigh[h, 1] = (weight - high.astype(f32)).astype(bf)
    metar[z] = meta[z]

    @pl.loop(DEPTH, chunks)
    def _(k):
        pick_rows(k)

    for o in range(1, zs):
        m_copy(o).wait_recv()
    places = lax.broadcasted_iota(jnp.int32, (cap, total), 1).astype(f32)
    for h in range(2):
        blocks = []
        for j in range(zs):
            where = jnp.transpose(metar[j])[:cap, h : h + 1]
            blocks.append(jnp.where(where == places, one, zero))
        if padded > rows:
            blocks.append(jnp.zeros((padded - rows, total), f32))
        table = jnp.concatenate(blocks, axis=0)
        onehot_t[h] = table.astype(bf)
        onehot[h] = jnp.transpose(table).astype(bf)

    weights[0].wait()
    weights[1].wait()
    weights[2].wait()
    acc[...] = jnp.zeros_like(acc)
    units = gate_v.shape[1]

    @pl.loop(0, 2 * chunks)
    def _(t):
        @pl.when(t < chunks)
        def _():
            wait_recv_all(z_sends, t, zs)

        @pl.when(t >= chunks)
        def _():
            wait_recv_all(z_backs, t - chunks, zs)

        @pl.when(t + DEPTH < chunks)
        def _():
            start_all(z_sends, t + DEPTH, zs)

        @pl.when((t + DEPTH >= chunks) & (t + DEPTH < 2 * chunks))
        def _():
            start_all(z_backs, t + DEPTH - chunks, zs)

        @pl.when(t < chunks)
        def _():
            sides = unfold(r1, t)
            for i in range(2):
                value = dot32(onehot[half_of(t)], sides[i]).astype(bf)
                s2[t, :, :, i * side : (i + 1) * side] = value.reshape(groups, slots, side)
            start_all(g_sends, t, groups)
            r2[t, g_me] = s2[t, g_me]

        @pl.when((t >= 1) & (t <= chunks))
        def _():
            k = t - 1
            wait_recv_all(g_sends, k, groups)
            values = r2[k].reshape(total, width)
            h = half_of(k)
            acc[h, :, :units] += dot32(values, gate_v[columns(k), :])
            acc[h, :, units:] += dot32(values, up_v[columns(k), :])

        @pl.when((t == each) | (t == chunks))
        def _():
            h = half_of(t - 1)
            first = acc[h, :, :units]
            act[...] = (first / (1.0 + jnp.exp(-first)) * acc[h, :, units:]).astype(bf)
            for i in range(each):
                k = h * each + i
                value = dot32(act[...], down_v[:, i * width : (i + 1) * width]).astype(bf)
                o2[k] = value.reshape(groups, slots, width)
                b2[k, g_me] = o2[k, g_me]
                if i < DEPTH:
                    start_all(g_backs, k, groups)

        @pl.when((t > each) & (t <= each + chunks))
        def _():
            k = t - each - 1
            wait_recv_all(g_backs, k, groups)

            @pl.when(lax.rem(k, each) + DEPTH < each)
            def _():
                start_all(g_backs, k + DEPTH, groups)

            value = dot32(onehot_t[half_of(k)], b2[k].reshape(total, width))
            o1[k] = fold(value)
            b1[k, z] = o1[k, z]

        @pl.when(t >= chunks)
        def _():
            k = t - chunks
            h = half_of(k)
            sides = unfold(b1, k)
            for i in range(2):
                at = pl.ds(pl.multiple_of(lax.rem(k, each) * width + i * side, side), side)
                value = dot32(weigh[h, 0], sides[i]) + dot32(weigh[h, 1], sides[i])

                @pl.when(h == 0)
                def _():
                    partial[:, at] = hidden_ref[:, at].astype(f32) + value

                @pl.when(h == 1)
                def _():
                    out_ref[:, at] = (partial[:, at] + value).astype(bf)

    for o in range(1, zs):
        m_copy(o).wait_send()

    @pl.loop(0, chunks)
    def _(k):
        for o in range(1, zs):
            z_sends(k, o).wait_send()
            z_backs(k, o).wait_send()
        for o in range(1, groups):
            g_sends(k, o).wait_send()
            g_backs(k, o).wait_send()


def routed_experts(cap, limit, collective, normed, hidden, columns, lanes, gate, up, down):
    zs, ys, cs = lax.axis_size(Z), lax.axis_size(Y), lax.axis_size(CORE)
    groups = ys * cs
    tokens, model = normed.shape
    slots = zs * limit // 2
    padded = -(-zs * cap // 128) * 128
    chunks = 2 * model // WIDTH
    units = gate.shape[1]
    bf, f32 = jnp.bfloat16, jnp.float32
    vmem, anywhere = pl.BlockSpec(memory_space=pltpu.VMEM), pl.BlockSpec(memory_space=pltpu.HBM)
    z_block, g_block = (chunks, zs, 2 * cap, WIDTH // 2), (chunks, groups, slots, WIDTH)
    dma = pltpu.SemaphoreType.DMA
    z_sem, g_sem, m_sem = dma((chunks, zs - 1)), dma((chunks, groups - 1)), dma((zs - 1,))
    total = groups * slots
    return pl.pallas_call(
        functools.partial(expert_kernel, zs, ys, cs, cap, slots),
        out_shape=jax.ShapeDtypeStruct((tokens, model), bf),
        in_specs=[vmem] * 4 + [anywhere] * 3,
        out_specs=vmem,
        scratch_shapes=[
            pltpu.VMEM((2, padded, tokens), bf), pltpu.VMEM((2, 2, tokens, padded), bf),
            pltpu.VMEM((zs, 8, 128), f32),
            pltpu.VMEM(z_block, bf), pltpu.VMEM(z_block, bf),
            pltpu.VMEM(g_block, bf), pltpu.VMEM(g_block, bf),
            pltpu.VMEM(g_block, bf), pltpu.VMEM(g_block, bf),
            pltpu.VMEM(z_block, bf), pltpu.VMEM(z_block, bf),
            pltpu.VMEM((zs, 8, 128), f32),
            pltpu.VMEM((2, padded, total), bf),
            pltpu.VMEM((2, total, padded), bf),
            pltpu.VMEM((2, total, 2 * units), f32),
            pltpu.VMEM((total, units), bf),
            pltpu.VMEM((tokens, model), f32),
            pltpu.VMEM(gate.shape, bf), pltpu.VMEM(up.shape, bf), pltpu.VMEM(down.shape, bf),
            z_sem, z_sem, g_sem, g_sem, g_sem, g_sem, z_sem, z_sem, m_sem, m_sem,
            dma((3,)),
        ],
        compiler_params=pltpu.CompilerParams(
            collective_id=collective, has_side_effects=True, vmem_limit_bytes=VMEM_LIMIT
        ),
        name="routed_experts",
    )(normed, hidden, columns, lanes, gate, up, down)


def per_device(
    conv_outer,
    conv_inner,
    conv_input,
    conv_taps,
    out_weight,
    mix_gate,
    residual,
    mix_gain,
    expert_gain,
    expert_ids,
    group_share,
    pair_scores,
    gate_experts,
    up_experts,
    down_experts,
):
    limit = 2 * expert_ids.shape[1] * residual.shape[0] // (lax.axis_size(SP) * gate_experts.shape[0])
    worst = limit * lax.axis_size(Y) * lax.axis_size(CORE) // 2
    hidden, normed, columns, lanes, most = mixer(
        conv_outer, conv_inner, conv_input, conv_taps, out_weight, mix_gate, residual, mix_gain, expert_gain,
        expert_ids, group_share, pair_scores, limit,
    )
    arguments = (normed, hidden, columns, lanes, gate_experts[0], up_experts[0], down_experts[0])
    usual = USUAL
    return lax.cond(
        most[0, 0] <= usual,
        functools.partial(routed_experts, usual, limit, 2),
        functools.partial(routed_experts, worst, limit, 3),
        *arguments,
    )


def solution(mesh):
    torus = Mesh(mesh.devices.reshape(8, 4, 2, mesh.shape["tp"]), SP_TP)
    return jax.shard_map(
        per_device,
        mesh=torus,
        in_specs=(
            P(SP, X),
            P(SP, X),
            P(SP, X),
            P(None, X),
            P(X, None),
            P(SP_TP, None),
            P(SP_TP, None),
            P(),
            P(),
            P(SP_TP, None),
            P(SP_TP),
            P(SP_TP, None),
            P(SP, None, None),
            P(SP, None, None),
            P(SP, None, None),
        ),
        out_specs=P(SP_TP, None),
        check_vma=False,
    )
```

```python
import functools

import jax
import jax.numpy as jnp
from jax import lax
from jax.experimental import pallas as pl
from jax.experimental.pallas import tpu as pltpu
from jax.sharding import Mesh
from jax.sharding import PartitionSpec as P

Z, Y, CORE, X = "sp_0", "sp_1", "sp_2", "tp"
SP = (Z, Y, CORE)
SP_TP = (Z, Y, CORE, X)
MESH = pl.DeviceIdType.MESH

epsilon = 1e-06
WIDTH = 512
VMEM_LIMIT = 67043328
DEPTH = 2
WINDOW = 3
USUAL = (36, 40)


def rms_scale(values, gain):
    return values * lax.rsqrt(jnp.mean(values * values, axis=-1, keepdims=True) + epsilon) * gain


def dot32(a, b):
    return jnp.dot(a, b, preferred_element_type=jnp.float32)


def mixer_kernel(
    sizes, limit, parts,
    taps_hbm, mix_gain_hbm, expert_gain_hbm, ids_hbm, share_hbm, scores_hbm,
    outer_hbm, inner_hbm, input_hbm, weight_hbm, gate_hbm, residual_hbm,
    hidden_ref, normed_ref, columns_ref, lanes_ref, most_ref,
    taps_ref, mix_gain_ref, expert_gain_ref, ids_v, share_v, scores_v,
    outer_v, inner_v, input_v, weight_v, gate_v, residual_v,
    products, mixed, own, far, far_in, near, near_in, tails, tail_in, table,
    mine, x_in, g_in, z_in, sent_x, sent_g,
    l_sem, t_send, t_recv, f_send, f_recv, n_send, n_recv, mx_send, mx_recv, mg_send, mg_recv, mz_send, mz_recv,
):
    zs, ys, cs, xs = sizes
    z, y, c, x = (lax.axis_index(a) for a in SP_TP)
    groups = ys * cs
    g_me = y * cs + c
    devices = zs * groups
    me = z * groups + g_me
    bf, f32 = jnp.bfloat16, jnp.float32
    length, lanes = inner_v.shape
    rows = length // xs
    half = own.shape[1] // 2
    piece = rows // parts

    loads = [
        pltpu.make_async_copy(src, dst, l_sem.at[i])
        for i, (src, dst) in enumerate(
            (
                (inner_hbm, inner_v), (input_hbm, input_v), (outer_hbm, outer_v),
                (taps_hbm, taps_ref), (weight_hbm, weight_v), (ids_hbm, ids_v), (share_hbm, share_v),
                (scores_hbm, scores_v), (gate_hbm, gate_v), (residual_hbm, residual_v),
                (mix_gain_hbm, mix_gain_ref), (expert_gain_hbm, expert_gain_ref),
            )
        )
    ]
    for load in loads:
        load.start()

    def sp_device(index):
        return {Z: lax.div(index, groups), Y: lax.div(lax.rem(index, groups), cs), CORE: lax.rem(index, cs)}

    following, preceding = lax.rem(me + 1, devices), lax.rem(me + devices - 1, devices)
    x_peers = [{X: lax.rem(x + o, xs)} for o in range(1, xs)]
    z_peers = [{Z: lax.rem(z + o, zs)} for o in range(1, zs)]
    g_peers = []
    for o in range(1, groups):
        g = lax.rem(g_me + o, groups)
        g_peers.append({Y: lax.div(g, cs), CORE: lax.rem(g, cs)})
    everyone = x_peers + z_peers + g_peers + [sp_device(following), sp_device(preceding)]
    barrier = pltpu.get_barrier_semaphore()
    for peer in everyone:
        pl.semaphore_signal(barrier, inc=1, device_id=peer, device_id_type=MESH)

    loads[0].wait()
    loads[1].wait()
    last = tails.shape[1]
    tails[0] = inner_v[length - last :, :]
    tails[1] = input_v[length - last :, :]
    tail_copy = pltpu.make_async_remote_copy(
        src_ref=tails, dst_ref=tail_in, send_sem=t_send, recv_sem=t_recv,
        device_id=sp_device(following), device_id_type=MESH,
    )

    pad = 8
    products[0:pad, :] = jnp.zeros((pad, lanes), f32)
    for b in range(xs):
        at = slice(b * rows, (b + 1) * rows)
        products[pad + b * rows : pad + (b + 1) * rows, :] = inner_v[at, :].astype(f32) * input_v[at, :].astype(f32)
    loads[2].wait()
    loads[3].wait()

    def convolve(start, count):
        conv = taps_ref[0:1, :] * products[start + pad - 2 : start + pad - 2 + count, :]
        conv = conv + taps_ref[1:2, :] * products[start + pad - 1 : start + pad - 1 + count, :]
        conv = conv + taps_ref[2:3, :] * products[start + pad : start + pad + count, :]
        mixed[start : start + count, :] = (outer_v[start : start + count, :].astype(f32) * conv).astype(bf)

    for b in range(xs):
        convolve(b * rows, rows)
    loads[4].wait()

    right, left = lax.rem(x + 1, xs), lax.rem(x + xs - 1, xs)
    ways = (right, left)

    def partial_of(owner, h, start=0, count=rows):
        block = mixed[pl.ds(pl.multiple_of(owner * rows + start, 16), count), :]
        return dot32(block, weight_v[:, h * half : (h + 1) * half])

    def far_copy(h, t):
        at = pl.ds(t * piece, piece)
        return pltpu.make_async_remote_copy(
            src_ref=far.at[h, at], dst_ref=far_in.at[h, at],
            send_sem=f_send.at[h, t], recv_sem=f_recv.at[h, t],
            device_id={X: ways[h]}, device_id_type=MESH,
        )

    def near_copy(d, h, t):
        at = pl.ds(t * piece, piece)
        return pltpu.make_async_remote_copy(
            src_ref=near.at[d, h, at], dst_ref=near_in.at[d, h, at],
            send_sem=n_send.at[d, h, t], recv_sem=n_recv.at[d, h, t],
            device_id={X: ways[d]}, device_id_type=MESH,
        )

    order = [*range(1, parts), 0]
    steps = [functools.partial(far_copy, t=t) for t in order]
    steps += [lambda d, t=t: near_copy(d, 1 - d, t) for t in order]
    steps += [lambda d, t=t: near_copy(d, d, t) for t in order]

    opposite = lax.rem(x + 2, xs)
    for h in range(2):
        far[h, piece:, :] = partial_of(opposite, h, piece, rows - piece).astype(bf)
    pl.semaphore_wait(barrier, len(everyone))
    tail_copy.start()
    for i in range(WINDOW):
        for h in range(2):
            steps[i](h).start()
    tail_copy.wait_recv()
    earlier = tail_in[0].astype(f32) * tail_in[1].astype(f32)
    earlier = jnp.where(me == 0, jnp.zeros_like(earlier), earlier)
    products[0:pad, :] = earlier[last - pad :, :]
    convolve(0, last)
    for h in range(2):
        far[h, :piece, :] = partial_of(opposite, h, 0, piece).astype(bf)
    for d in range(2):
        near[d, 1 - d] = partial_of(ways[d], 1 - d).astype(bf)
    for d in range(2):
        own[:, d * half : (d + 1) * half] = partial_of(ways[d], d)

    def step(i):
        for d in range(2):
            steps[i](d).wait_recv()
            if i < parts:
                at = slice(order[i] * piece, (order[i] + 1) * piece)
                near[d, d, at, :] = (own[at, d * half : (d + 1) * half] + far_in[d, at, :].astype(f32)).astype(bf)
            if i + WINDOW < len(steps):
                steps[i + WINDOW](d).start()

    step(0)
    tokens = ids_v.shape[1]
    for load in loads[5:8]:
        load.wait()
    table[...] = jnp.zeros_like(table)
    table[0:2, 0:tokens] = ids_v[...].astype(f32)
    table[2:4, 0:tokens] = scores_v[...]
    table[4:5, 0:tokens] = share_v[...]
    given = jnp.transpose(table[...])[0:tokens, :]
    expert = [given[:, k : k + 1] for k in range(2)]
    z_of = [jnp.floor((e + 0.5) / groups) for e in expert]
    lane = lax.broadcasted_iota(jnp.int32, (tokens, 128), 1).astype(f32)
    before = jnp.where(
        lax.broadcasted_iota(jnp.int32, (tokens, tokens), 1) < lax.broadcasted_iota(jnp.int32, (tokens, tokens), 0),
        jnp.ones((), f32), jnp.zeros((), f32),
    ).astype(bf)

    def ranks(labels):
        marks = [jnp.where(label == lane, jnp.ones((), f32), jnp.zeros((), f32)) for label in labels]
        firsts = jnp.sum(marks[0], axis=0, keepdims=True)
        seen = [dot32(before, marks[0].astype(bf)), dot32(before, marks[1].astype(bf)) + firsts]
        found = [jnp.sum(mark * s, axis=1, keepdims=True) for mark, s in zip(marks, seen)]
        return found, jnp.max(firsts + jnp.sum(marks[1], axis=0, keepdims=True), axis=1, keepdims=True)

    rank, _ = ranks(expert)
    lower = [jnp.floor(r * 0.5) for r in rank]
    parity = [r + e - 2.0 * jnp.floor((r + e) * 0.5) for r, e in zip(rank, expert)]
    block = [h * zs + zz for h, zz in zip(parity, z_of)]
    place, most = ranks(block)
    most = jnp.broadcast_to(most, (8, 128))
    mine[...] = most

    def flag_copy(src, dst, send, recv, i, peer):
        return pltpu.make_async_remote_copy(
            src_ref=src, dst_ref=dst.at[i], send_sem=send.at[i], recv_sem=recv.at[i],
            device_id=peer, device_id_type=MESH,
        )

    x_flags = [flag_copy(mine, x_in, mx_send, mx_recv, i, p) for i, p in enumerate(x_peers)]
    g_flags = [flag_copy(sent_x, g_in, mg_send, mg_recv, i, p) for i, p in enumerate(g_peers)]
    z_flags = [flag_copy(sent_g, z_in, mz_send, mz_recv, i, p) for i, p in enumerate(z_peers)]
    for flag in x_flags:
        flag.start()

    info = []
    step(1)
    scores = [given[:, 2 + k : 3 + k] for k in range(2)]
    top = jnp.maximum(scores[0], scores[1])
    powers = [jnp.exp(v - top) for v in scores]
    for k in range(2):
        slot = (expert[k] - groups * z_of[k]) * (zs * limit / 2) + (z * limit).astype(f32) * 0.5 + lower[k]
        info.append((block[k], place[k], slot, given[:, 4:5] * (powers[k] / (powers[0] + powers[1]))))
    column = jnp.zeros((tokens, 128), f32)
    for i in range(4):
        for k in range(2):
            column = column + jnp.where(lane == 2 * i + k, info[k][i], 0.0)
    columns_ref[...] = column
    spare = jnp.zeros((table.shape[1] - tokens, 128), f32)
    lanes_ref[...] = jnp.transpose(jnp.concatenate([column, spare], axis=0))[0:8, :]
    step(2)

    for flag in x_flags:
        flag.wait_recv()
    for i in range(xs - 1):
        most = jnp.maximum(most, x_in[i])
    sent_x[...] = most
    for flag in g_flags:
        flag.start()

    for i in range(3, parts):
        step(i)
    for h in range(2):
        own[:, h * half : (h + 1) * half] = partial_of(x, h)

    for flag in g_flags:
        flag.wait_recv()
    for i in range(groups - 1):
        most = jnp.maximum(most, g_in[i])
    sent_g[...] = most
    for flag in z_flags:
        flag.start()

    for load in loads[8:]:
        load.wait()
    for i in range(parts, 2 * parts):
        step(i)
    for i, t in enumerate(order):
        at = slice(t * piece, (t + 1) * piece)
        step(2 * parts + i)
        sums = []
        for h in range(2):
            part = own[at, h * half : (h + 1) * half]
            sums.append(part + near_in[0, h, at, :].astype(f32) + near_in[1, h, at, :].astype(f32))
        projected = jnp.concatenate(sums, axis=1)
        value = jax.nn.sigmoid(gate_v[at, :].astype(f32)) * projected
        hidden = (residual_v[at, :].astype(f32) + rms_scale(value, mix_gain_ref[...])).astype(bf)
        hidden_ref[at, :] = hidden
        normed_ref[at, :] = rms_scale(hidden.astype(f32), expert_gain_ref[...]).astype(bf)

    for flag in z_flags:
        flag.wait_recv()
    for i in range(zs - 1):
        most = jnp.maximum(most, z_in[i])
    most_ref[...] = most

    tail_copy.wait_send()
    for h in range(2):
        for t in range(parts):
            far_copy(h, t).wait_send()
            for d in range(2):
                near_copy(d, h, t).wait_send()
    for flag in x_flags + g_flags + z_flags:
        flag.wait_send()


def mixer(outer, inner, values, taps, weight, gate, residual, mix_gain, expert_gain, ids, share, scores, limit):
    sizes = tuple(lax.axis_size(a) for a in SP_TP)
    zs, ys, cs, xs = sizes
    groups = ys * cs
    length, lanes = inner.shape
    rows, model = residual.shape
    half, parts, last = model // 2, 4, 16
    bf, f32 = jnp.bfloat16, jnp.float32
    vmem, anywhere = pl.BlockSpec(memory_space=pltpu.VMEM), pl.BlockSpec(memory_space=pltpu.HBM)
    dma = pltpu.SemaphoreType.DMA
    flag = (8, 128)
    return pl.pallas_call(
        functools.partial(mixer_kernel, sizes, limit, parts),
        out_shape=(
            jax.ShapeDtypeStruct((rows, model), bf),
            jax.ShapeDtypeStruct((rows, model), bf),
            jax.ShapeDtypeStruct((rows, 128), f32),
            jax.ShapeDtypeStruct((8, 256), f32),
            jax.ShapeDtypeStruct(flag, f32),
        ),
        in_specs=[anywhere] * 12,
        out_specs=(vmem,) * 5,
        scratch_shapes=[
            pltpu.VMEM(taps.shape, f32), pltpu.VMEM((1, model), f32), pltpu.VMEM((1, model), f32),
            pltpu.VMEM((2, rows), jnp.int32), pltpu.VMEM((1, rows), f32), pltpu.VMEM((2, rows), f32),
            pltpu.VMEM(outer.shape, bf), pltpu.VMEM(inner.shape, bf), pltpu.VMEM(values.shape, bf),
            pltpu.VMEM(weight.shape, bf), pltpu.VMEM(gate.shape, bf), pltpu.VMEM(residual.shape, bf),
            pltpu.VMEM((length + 8, lanes), f32),
            pltpu.VMEM((length, lanes), bf),
            pltpu.VMEM((rows, model), f32),
            pltpu.VMEM((2, rows, half), bf), pltpu.VMEM((2, rows, half), bf),
            pltpu.VMEM((2, 2, rows, half), bf), pltpu.VMEM((2, 2, rows, half), bf),
            pltpu.VMEM((2, last, lanes), bf), pltpu.VMEM((2, last, lanes), bf),
            pltpu.VMEM((128, 256), f32),
            pltpu.VMEM(flag, f32), pltpu.VMEM((xs - 1, *flag), f32),
            pltpu.VMEM((groups - 1, *flag), f32), pltpu.VMEM((zs - 1, *flag), f32),
            pltpu.VMEM(flag, f32), pltpu.VMEM(flag, f32),
            dma((12,)), dma, dma,
            dma((2, parts)), dma((2, parts)), dma((2, 2, parts)), dma((2, 2, parts)),
            dma((xs - 1,)), dma((xs - 1,)), dma((groups - 1,)), dma((groups - 1,)), dma((zs - 1,)), dma((zs - 1,)),
        ],
        compiler_params=pltpu.CompilerParams(
            collective_id=1, has_side_effects=True, vmem_limit_bytes=VMEM_LIMIT
        ),
        name="mixer",
    )(
        taps, mix_gain[None, :], expert_gain[None, :], ids.T, share[None, :], scores.T,
        outer, inner, values, weight, gate, residual,
    )


def expert_kernel(
    zs, ys, cs, cap, slots,
    normed_ref, hidden_ref, columns_ref, lanes_ref, gate_hbm, up_hbm, down_hbm,
    out_ref,
    pick, weigh, meta, s1, r1, s2, r2, o2, b2, o1, b1, metar, onehot_t, onehot, acc, act, partial,
    gate_v, up_v, down_v,
    z_send, z_recv, g_send, g_recv, bg_send, bg_recv, bz_send, bz_recv, m_send, m_recv, w_sem,
):
    z, y, c = lax.axis_index(Z), lax.axis_index(Y), lax.axis_index(CORE)
    groups = ys * cs
    g_me = y * cs + c
    chunks = s1.shape[0]
    each = chunks // 2
    high = -(-cap // 8) * 8
    width = s2.shape[3]
    side = width // 2
    tokens = normed_ref.shape[0]
    rows = zs * high
    padded = onehot_t.shape[1]
    total = groups * slots
    bf, f32 = jnp.bfloat16, jnp.float32
    one, zero = jnp.ones((), f32), jnp.zeros((), f32)

    weights = [
        pltpu.make_async_copy(src, dst, w_sem.at[i])
        for i, (src, dst) in enumerate(((gate_hbm, gate_v), (up_hbm, up_v), (down_hbm, down_v)))
    ]
    for copy in weights:
        copy.start()

    def z_peer(o):
        return lax.rem(z + o, zs)

    def g_peer(o):
        return lax.rem(g_me + o, groups)

    def g_device(g):
        return {Y: lax.div(g, cs), CORE: lax.rem(g, cs)}

    barrier = pltpu.get_barrier_semaphore()
    for o in range(1, zs):
        pl.semaphore_signal(barrier, inc=1, device_id={Z: z_peer(o)}, device_id_type=MESH)
    for o in range(1, groups):
        pl.semaphore_signal(barrier, inc=1, device_id=g_device(g_peer(o)), device_id_type=MESH)

    def z_copy(src, dst, send, recv, k, o):
        return pltpu.make_async_remote_copy(
            src_ref=src.at[k, z_peer(o)], dst_ref=dst.at[k, z],
            send_sem=send.at[k, o - 1], recv_sem=recv.at[k, o - 1],
            device_id={Z: z_peer(o)}, device_id_type=MESH,
        )

    def g_copy(src, dst, send, recv, k, o):
        return pltpu.make_async_remote_copy(
            src_ref=src.at[k, g_peer(o)], dst_ref=dst.at[k, g_me],
            send_sem=send.at[k, o - 1], recv_sem=recv.at[k, o - 1],
            device_id=g_device(g_peer(o)), device_id_type=MESH,
        )

    def m_copy(o):
        return pltpu.make_async_remote_copy(
            src_ref=meta.at[z_peer(o)], dst_ref=metar.at[z],
            send_sem=m_send.at[o - 1], recv_sem=m_recv.at[o - 1],
            device_id={Z: z_peer(o)}, device_id_type=MESH,
        )

    z_sends = functools.partial(z_copy, s1, r1, z_send, z_recv)
    g_sends = functools.partial(g_copy, s2, r2, g_send, g_recv)
    g_backs = functools.partial(g_copy, o2, b2, bg_send, bg_recv)
    z_backs = functools.partial(z_copy, o1, b1, bz_send, bz_recv)

    def start_all(copies, k, count):
        for o in range(1, count):
            copies(k, o).start()

    def wait_recv_all(copies, k, count):
        for o in range(1, count):
            copies(k, o).wait_recv()

    def half_of(k):
        return lax.div(k, each)

    def columns(k):
        return pl.ds(pl.multiple_of(lax.rem(k, each) * width, width), width)

    def fold(value):
        value = value.reshape(zs, high, width)
        if high == cap:
            return value.astype(bf)
        whole = high - 8
        left, right = value[:, :, :side], value[:, :, side:]
        blocks = []
        for j in range(zs):
            ends = left[j, whole:] + pltpu.roll(right[j, whole:], 4, 0)
            blocks.append(jnp.concatenate([left[j, :whole], right[j, :whole], ends], axis=0)[None])
        return jnp.concatenate(blocks, axis=0).astype(bf)

    def unfold(ref, k):
        value = ref[k].astype(f32)
        if high == cap:
            blocks = [value.reshape(rows, width)]
        else:
            whole = high - 8
            blocks = []
            for j in range(zs):
                ends = value[j, 2 * whole :]
                left = jnp.concatenate([value[j, :whole], ends], axis=0)
                right = jnp.concatenate([value[j, whole : 2 * whole], pltpu.roll(ends, 4, 0)], axis=0)
                blocks.append(jnp.concatenate([left, right], axis=1))
        if padded > rows:
            blocks.append(jnp.zeros((padded - rows, width), f32))
        return jnp.concatenate(blocks, axis=0).astype(bf)

    def row_of(block, place, h):
        inside = (block >= float(h * zs)) & (block < float((h + 1) * zs))
        return jnp.where(inside, (block - float(h * zs)) * high + place, -1.0)

    lane_rows = [
        [row_of(lanes_ref[k : k + 1, 0:tokens], lanes_ref[2 + k : 3 + k, 0:tokens], h) for k in range(2)]
        for h in range(2)
    ]
    slot_of = [lanes_ref[4 + k : 5 + k, 0:tokens] + 1.0 for k in range(2)]
    numbers = lax.broadcasted_iota(jnp.int32, (padded, tokens), 0).astype(f32)
    for h in range(2):
        hit = [numbers == r for r in lane_rows[h]]
        pick[h] = jnp.where(hit[0] | hit[1], one, zero).astype(bf)

    def pick_rows(k):
        value = dot32(pick[half_of(k)], normed_ref[:, columns(k)])
        s1[k] = fold(value[:rows])
        r1[k, z] = s1[k, z]

    pl.semaphore_wait(barrier, zs + groups - 2)
    for k in range(DEPTH):
        pick_rows(k)
        start_all(z_sends, k, zs)

    place = lax.broadcasted_iota(jnp.int32, (high, tokens), 0).astype(f32)
    blank = jnp.full((128 - high, 128), -1.0, f32)
    spot = lax.broadcasted_iota(jnp.int32, (128, 128), 1).astype(f32)
    for j in range(zs):
        both = jnp.zeros((128, 128), f32)
        for h in range(2):
            hit = [place + float(j * high) == r for r in lane_rows[h]]
            found = jnp.where(hit[0], slot_of[0], 0.0) + jnp.where(hit[1], slot_of[1], 0.0)
            found = jnp.broadcast_to(jnp.sum(found, axis=1, keepdims=True) - 1.0, (high, 128))
            both = jnp.where(spot == float(h), jnp.concatenate([found, blank], axis=0), both)
        meta[j] = jnp.transpose(both)[0:8, :]
    for o in range(1, zs):
        m_copy(o).start()
    row_lane = lax.broadcasted_iota(jnp.int32, (tokens, padded), 1).astype(f32)
    for h in range(2):
        weight = jnp.zeros((tokens, padded), f32)
        for k in range(2):
            row = row_of(columns_ref[:, k : k + 1], columns_ref[:, 2 + k : 3 + k], h)
            weight = weight + jnp.where(row == row_lane, columns_ref[:, 6 + k : 7 + k], 0.0)
        rounded = weight.astype(bf)
        weigh[h, 0] = rounded
        weigh[h, 1] = (weight - rounded.astype(f32)).astype(bf)
    metar[z] = meta[z]

    @pl.loop(DEPTH, chunks)
    def _(k):
        pick_rows(k)

    for o in range(1, zs):
        m_copy(o).wait_recv()
    places = lax.broadcasted_iota(jnp.int32, (high, total), 1).astype(f32)
    for h in range(2):
        blocks = []
        for j in range(zs):
            where = jnp.transpose(metar[j])[:high, h : h + 1]
            blocks.append(jnp.where(where == places, one, zero))
        if padded > rows:
            blocks.append(jnp.zeros((padded - rows, total), f32))
        table = jnp.concatenate(blocks, axis=0)
        onehot_t[h] = table.astype(bf)
        onehot[h] = jnp.transpose(table).astype(bf)

    weights[0].wait()
    weights[1].wait()
    weights[2].wait()
    acc[...] = jnp.zeros_like(acc)
    units = gate_v.shape[1]

    @pl.loop(0, 2 * chunks)
    def _(t):
        @pl.when(t < chunks)
        def _():
            wait_recv_all(z_sends, t, zs)

        @pl.when(t >= chunks)
        def _():
            wait_recv_all(z_backs, t - chunks, zs)

        @pl.when(t + DEPTH < chunks)
        def _():
            start_all(z_sends, t + DEPTH, zs)

        @pl.when((t + DEPTH >= chunks) & (t + DEPTH < 2 * chunks))
        def _():
            start_all(z_backs, t + DEPTH - chunks, zs)

        @pl.when(t < chunks)
        def _():
            value = dot32(onehot[half_of(t)], unfold(r1, t)).astype(bf)
            s2[t] = value.reshape(groups, slots, width)
            start_all(g_sends, t, groups)
            r2[t, g_me] = s2[t, g_me]

        @pl.when((t >= 1) & (t <= chunks))
        def _():
            k = t - 1
            wait_recv_all(g_sends, k, groups)
            values = r2[k].reshape(total, width)
            h = half_of(k)
            acc[h, :, :units] += dot32(values, gate_v[columns(k), :])
            acc[h, :, units:] += dot32(values, up_v[columns(k), :])

        @pl.when((t == each) | (t == chunks))
        def _():
            h = half_of(t - 1)
            first = acc[h, :, :units]
            act[...] = (first / (1.0 + jnp.exp(-first)) * acc[h, :, units:]).astype(bf)
            for i in range(each):
                k = h * each + i
                value = dot32(act[...], down_v[:, i * width : (i + 1) * width]).astype(bf)
                o2[k] = value.reshape(groups, slots, width)
                b2[k, g_me] = o2[k, g_me]
                if i < DEPTH:
                    start_all(g_backs, k, groups)

        @pl.when((t > each) & (t <= each + chunks))
        def _():
            k = t - each - 1
            wait_recv_all(g_backs, k, groups)

            @pl.when(lax.rem(k, each) + DEPTH < each)
            def _():
                start_all(g_backs, k + DEPTH, groups)

            value = dot32(onehot_t[half_of(k)], b2[k].reshape(total, width))
            o1[k] = fold(value[:rows])
            b1[k, z] = o1[k, z]

        @pl.when(t >= chunks)
        def _():
            k = t - chunks
            h = half_of(k)
            values = unfold(b1, k)
            at = columns(k)
            value = dot32(weigh[h, 0], values) + dot32(weigh[h, 1], values)

            @pl.when(h == 0)
            def _():
                partial[:, at] = hidden_ref[:, at].astype(f32) + value

            @pl.when(h == 1)
            def _():
                out_ref[:, at] = (partial[:, at] + value).astype(bf)

    for o in range(1, zs):
        m_copy(o).wait_send()

    @pl.loop(0, chunks)
    def _(k):
        for o in range(1, zs):
            z_sends(k, o).wait_send()
            z_backs(k, o).wait_send()
        for o in range(1, groups):
            g_sends(k, o).wait_send()
            g_backs(k, o).wait_send()


def routed_experts(cap, limit, collective, normed, hidden, columns, lanes, gate, up, down):
    zs, ys, cs = lax.axis_size(Z), lax.axis_size(Y), lax.axis_size(CORE)
    groups = ys * cs
    tokens, model = normed.shape
    slots = zs * limit // 2
    high = -(-cap // 8) * 8
    padded = -(-zs * high // 128) * 128
    chunks = 2 * model // WIDTH
    units = gate.shape[1]
    bf, f32 = jnp.bfloat16, jnp.float32
    vmem, anywhere = pl.BlockSpec(memory_space=pltpu.VMEM), pl.BlockSpec(memory_space=pltpu.HBM)
    z_block = (chunks, zs, cap, WIDTH) if high == cap else (chunks, zs, 2 * cap, WIDTH // 2)
    g_block = (chunks, groups, slots, WIDTH)
    dma = pltpu.SemaphoreType.DMA
    z_sem, g_sem, m_sem = dma((chunks, zs - 1)), dma((chunks, groups - 1)), dma((zs - 1,))
    total = groups * slots
    return pl.pallas_call(
        functools.partial(expert_kernel, zs, ys, cs, cap, slots),
        out_shape=jax.ShapeDtypeStruct((tokens, model), bf),
        in_specs=[vmem] * 4 + [anywhere] * 3,
        out_specs=vmem,
        scratch_shapes=[
            pltpu.VMEM((2, padded, tokens), bf), pltpu.VMEM((2, 2, tokens, padded), bf),
            pltpu.VMEM((zs, 8, 128), f32),
            pltpu.VMEM(z_block, bf), pltpu.VMEM(z_block, bf),
            pltpu.VMEM(g_block, bf), pltpu.VMEM(g_block, bf),
            pltpu.VMEM(g_block, bf), pltpu.VMEM(g_block, bf),
            pltpu.VMEM(z_block, bf), pltpu.VMEM(z_block, bf),
            pltpu.VMEM((zs, 8, 128), f32),
            pltpu.VMEM((2, padded, total), bf),
            pltpu.VMEM((2, total, padded), bf),
            pltpu.VMEM((2, total, 2 * units), f32),
            pltpu.VMEM((total, units), bf),
            pltpu.VMEM((tokens, model), f32),
            pltpu.VMEM(gate.shape, bf), pltpu.VMEM(up.shape, bf), pltpu.VMEM(down.shape, bf),
            z_sem, z_sem, g_sem, g_sem, g_sem, g_sem, z_sem, z_sem, m_sem, m_sem,
            dma((3,)),
        ],
        compiler_params=pltpu.CompilerParams(
            collective_id=collective, has_side_effects=True, vmem_limit_bytes=VMEM_LIMIT
        ),
        name="routed_experts",
    )(normed, hidden, columns, lanes, gate, up, down)


def per_device(
    conv_outer,
    conv_inner,
    conv_input,
    conv_taps,
    out_weight,
    mix_gate,
    residual,
    mix_gain,
    expert_gain,
    expert_ids,
    group_share,
    pair_scores,
    gate_experts,
    up_experts,
    down_experts,
):
    limit = 2 * expert_ids.shape[1] * residual.shape[0] // (lax.axis_size(SP) * gate_experts.shape[0])
    worst = limit * lax.axis_size(Y) * lax.axis_size(CORE) // 2
    hidden, normed, columns, lanes, most = mixer(
        conv_outer, conv_inner, conv_input, conv_taps, out_weight, mix_gate, residual, mix_gain, expert_gain,
        expert_ids, group_share, pair_scores, limit,
    )
    arguments = (normed, hidden, columns, lanes, gate_experts[0], up_experts[0], down_experts[0])
    caps = [cap for cap in USUAL if cap < worst]
    tier = sum((most[0, 0] > cap).astype(jnp.int32) for cap in caps)
    return lax.switch(
        tier,
        [functools.partial(routed_experts, cap, limit, 2 + i) for i, cap in enumerate(caps + [worst])],
        *arguments,
    )


def solution(mesh):
    torus = Mesh(mesh.devices.reshape(8, 4, 2, mesh.shape["tp"]), SP_TP)
    return jax.shard_map(
        per_device,
        mesh=torus,
        in_specs=(
            P(SP, X),
            P(SP, X),
            P(SP, X),
            P(None, X),
            P(X, None),
            P(SP_TP, None),
            P(SP_TP, None),
            P(),
            P(),
            P(SP_TP, None),
            P(SP_TP),
            P(SP_TP, None),
            P(SP, None, None),
            P(SP, None, None),
            P(SP, None, None),
        ),
        out_specs=P(SP_TP, None),
        check_vma=False,
    )
```

```python
import functools

import jax
import jax.numpy as jnp
from jax import lax
from jax.experimental import pallas as pl
from jax.experimental.pallas import tpu as pltpu
from jax.sharding import Mesh
from jax.sharding import PartitionSpec as P

Z, Y, CORE, X = "sp_0", "sp_1", "sp_2", "tp"
SP = (Z, Y, CORE)
SP_TP = (Z, Y, CORE, X)
MESH = pl.DeviceIdType.MESH

epsilon = 1e-06
WIDTH = 512
VMEM_LIMIT = 67043328
MIXER_ROOM = 1835008
EXPERT_ROOM = 2726297
DEPTH = 2
WINDOW = 3
USUAL = (36, 40)


def rms_scale(values, gain):
    return values * lax.rsqrt(jnp.mean(values * values, axis=-1, keepdims=True) + epsilon) * gain


def dot32(a, b):
    return jnp.dot(a, b, preferred_element_type=jnp.float32)


def mixer_kernel(
    sizes, limit, caps, parts,
    taps_hbm, mix_gain_hbm, expert_gain_hbm, ids_hbm, share_hbm, scores_hbm,
    outer_hbm, inner_hbm, input_hbm, weight_hbm, gate_hbm, residual_hbm,
    hidden_ref, normed_ref, columns_ref, lanes_ref, tier_ref,
    taps_ref, mix_gain_ref, expert_gain_ref, ids_v, share_v, scores_v,
    outer_v, inner_v, input_v, weight_v, gate_v, residual_v,
    products, mixed, own, far, far_in, near, near_in, tails, tail_in, table,
    mine, x_in, g_in, z_in, sent_x, sent_g,
    l_sem, t_send, t_recv, f_send, f_recv, n_send, n_recv, mx_send, mx_recv, mg_send, mg_recv, mz_send, mz_recv,
):
    zs, ys, cs, xs = sizes
    z, y, c, x = (lax.axis_index(a) for a in SP_TP)
    groups = ys * cs
    g_me = y * cs + c
    devices = zs * groups
    me = z * groups + g_me
    bf, f32 = jnp.bfloat16, jnp.float32
    length, lanes = inner_v.shape
    rows = length // xs
    half = own.shape[1] // 2
    piece = rows // parts

    loads = [
        pltpu.make_async_copy(src, dst, l_sem.at[i])
        for i, (src, dst) in enumerate(
            (
                (inner_hbm, inner_v), (input_hbm, input_v), (outer_hbm, outer_v),
                (taps_hbm, taps_ref), (weight_hbm, weight_v), (ids_hbm, ids_v), (share_hbm, share_v),
                (scores_hbm, scores_v), (gate_hbm, gate_v), (residual_hbm, residual_v),
                (mix_gain_hbm, mix_gain_ref), (expert_gain_hbm, expert_gain_ref),
            )
        )
    ]
    for load in loads:
        load.start()

    def sp_device(index):
        return {Z: lax.div(index, groups), Y: lax.div(lax.rem(index, groups), cs), CORE: lax.rem(index, cs)}

    following, preceding = lax.rem(me + 1, devices), lax.rem(me + devices - 1, devices)
    x_peers = [{X: lax.rem(x + o, xs)} for o in range(1, xs)]
    z_peers = [{Z: lax.rem(z + o, zs)} for o in range(1, zs)]
    g_peers = []
    for o in range(1, groups):
        g = lax.rem(g_me + o, groups)
        g_peers.append({Y: lax.div(g, cs), CORE: lax.rem(g, cs)})
    everyone = x_peers + z_peers + g_peers + [sp_device(following), sp_device(preceding)]
    barrier = pltpu.get_barrier_semaphore()
    for peer in everyone:
        pl.semaphore_signal(barrier, inc=1, device_id=peer, device_id_type=MESH)

    loads[0].wait()
    loads[1].wait()
    last = tails.shape[1]
    tails[0] = inner_v[length - last :, :]
    tails[1] = input_v[length - last :, :]
    tail_copy = pltpu.make_async_remote_copy(
        src_ref=tails, dst_ref=tail_in, send_sem=t_send, recv_sem=t_recv,
        device_id=sp_device(following), device_id_type=MESH,
    )

    pad = 8
    products[0:pad, :] = jnp.zeros((pad, lanes), f32)
    for b in range(xs):
        at = slice(b * rows, (b + 1) * rows)
        products[pad + b * rows : pad + (b + 1) * rows, :] = inner_v[at, :].astype(f32) * input_v[at, :].astype(f32)
    loads[2].wait()
    loads[3].wait()

    def convolve(start, count):
        conv = taps_ref[0:1, :] * products[start + pad - 2 : start + pad - 2 + count, :]
        conv = conv + taps_ref[1:2, :] * products[start + pad - 1 : start + pad - 1 + count, :]
        conv = conv + taps_ref[2:3, :] * products[start + pad : start + pad + count, :]
        mixed[start : start + count, :] = (outer_v[start : start + count, :].astype(f32) * conv).astype(bf)

    for b in range(xs):
        convolve(b * rows, rows)
    loads[4].wait()

    right, left = lax.rem(x + 1, xs), lax.rem(x + xs - 1, xs)
    ways = (right, left)

    def partial_of(owner, h, start=0, count=rows):
        block = mixed[pl.ds(pl.multiple_of(owner * rows + start, 16), count), :]
        return dot32(block, weight_v[:, h * half : (h + 1) * half])

    def far_copy(h, t):
        at = pl.ds(t * piece, piece)
        return pltpu.make_async_remote_copy(
            src_ref=far.at[h, at], dst_ref=far_in.at[h, at],
            send_sem=f_send.at[h, t], recv_sem=f_recv.at[h, t],
            device_id={X: ways[h]}, device_id_type=MESH,
        )

    def near_copy(d, h, t):
        at = pl.ds(t * piece, piece)
        return pltpu.make_async_remote_copy(
            src_ref=near.at[d, h, at], dst_ref=near_in.at[d, h, at],
            send_sem=n_send.at[d, h, t], recv_sem=n_recv.at[d, h, t],
            device_id={X: ways[d]}, device_id_type=MESH,
        )

    order = [*range(1, parts), 0]
    steps = [functools.partial(far_copy, t=t) for t in order]
    steps += [lambda d, t=t: near_copy(d, 1 - d, t) for t in order]
    steps += [lambda d, t=t: near_copy(d, d, t) for t in order]

    opposite = lax.rem(x + 2, xs)
    for h in range(2):
        far[h, piece:, :] = partial_of(opposite, h, piece, rows - piece).astype(bf)
    pl.semaphore_wait(barrier, len(everyone))
    tail_copy.start()
    for i in range(WINDOW):
        for h in range(2):
            steps[i](h).start()
    tail_copy.wait_recv()
    earlier = tail_in[0].astype(f32) * tail_in[1].astype(f32)
    earlier = jnp.where(me == 0, jnp.zeros_like(earlier), earlier)
    products[0:pad, :] = earlier[last - pad :, :]
    convolve(0, last)
    for h in range(2):
        far[h, :piece, :] = partial_of(opposite, h, 0, piece).astype(bf)
    for d in range(2):
        near[d, 1 - d] = partial_of(ways[d], 1 - d).astype(bf)
    for d in range(2):
        own[:, d * half : (d + 1) * half] = partial_of(ways[d], d)

    def step(i):
        for d in range(2):
            steps[i](d).wait_recv()
            if i < parts:
                at = slice(order[i] * piece, (order[i] + 1) * piece)
                near[d, d, at, :] = (own[at, d * half : (d + 1) * half] + far_in[d, at, :].astype(f32)).astype(bf)
            if i + WINDOW < len(steps):
                steps[i + WINDOW](d).start()

    step(0)
    tokens = ids_v.shape[1]
    for load in loads[5:8]:
        load.wait()
    table[...] = jnp.zeros_like(table)
    table[0:2, 0:tokens] = ids_v[...].astype(f32)
    table[2:4, 0:tokens] = scores_v[...]
    table[4:5, 0:tokens] = share_v[...]
    given = jnp.transpose(table[...])[0:tokens, :]
    expert = [given[:, k : k + 1] for k in range(2)]
    z_of = [jnp.floor((e + 0.5) / groups) for e in expert]
    lane = lax.broadcasted_iota(jnp.int32, (tokens, 128), 1).astype(f32)
    before = jnp.where(
        lax.broadcasted_iota(jnp.int32, (tokens, tokens), 1) < lax.broadcasted_iota(jnp.int32, (tokens, tokens), 0),
        jnp.ones((), f32), jnp.zeros((), f32),
    ).astype(bf)

    def ranks(labels):
        marks = [jnp.where(label == lane, jnp.ones((), f32), jnp.zeros((), f32)) for label in labels]
        firsts = jnp.sum(marks[0], axis=0, keepdims=True)
        seen = [dot32(before, marks[0].astype(bf)), dot32(before, marks[1].astype(bf)) + firsts]
        found = [jnp.sum(mark * s, axis=1, keepdims=True) for mark, s in zip(marks, seen)]
        return found, jnp.max(firsts + jnp.sum(marks[1], axis=0, keepdims=True), axis=1, keepdims=True)

    rank, _ = ranks(expert)
    lower = [jnp.floor(r * 0.5) for r in rank]
    parity = [r + e - 2.0 * jnp.floor((r + e) * 0.5) for r, e in zip(rank, expert)]
    block = [h * zs + zz for h, zz in zip(parity, z_of)]
    place, most = ranks(block)
    most = jnp.broadcast_to(most, (8, 128))
    mine[...] = most

    def flag_copy(src, dst, send, recv, i, peer):
        return pltpu.make_async_remote_copy(
            src_ref=src, dst_ref=dst.at[i], send_sem=send.at[i], recv_sem=recv.at[i],
            device_id=peer, device_id_type=MESH,
        )

    x_flags = [flag_copy(mine, x_in, mx_send, mx_recv, i, p) for i, p in enumerate(x_peers)]
    g_flags = [flag_copy(sent_x, g_in, mg_send, mg_recv, i, p) for i, p in enumerate(g_peers)]
    z_flags = [flag_copy(sent_g, z_in, mz_send, mz_recv, i, p) for i, p in enumerate(z_peers)]
    for flag in x_flags:
        flag.start()

    info = []
    step(1)
    scores = [given[:, 2 + k : 3 + k] for k in range(2)]
    top = jnp.maximum(scores[0], scores[1])
    powers = [jnp.exp(v - top) for v in scores]
    for k in range(2):
        slot = (expert[k] - groups * z_of[k]) * (zs * limit / 2) + (z * limit).astype(f32) * 0.5 + lower[k]
        info.append((block[k], place[k], slot, given[:, 4:5] * (powers[k] / (powers[0] + powers[1]))))
    column = jnp.zeros((tokens, 128), f32)
    for i in range(4):
        for k in range(2):
            column = column + jnp.where(lane == 2 * i + k, info[k][i], 0.0)
    columns_ref[...] = column
    spare = jnp.zeros((table.shape[1] - tokens, 128), f32)
    lanes_ref[...] = jnp.transpose(jnp.concatenate([column, spare], axis=0))[0:8, :]
    step(2)

    for flag in x_flags:
        flag.wait_recv()
    for i in range(xs - 1):
        most = jnp.maximum(most, x_in[i])
    sent_x[...] = most
    for flag in g_flags:
        flag.start()

    for i in range(3, parts):
        step(i)
    for h in range(2):
        own[:, h * half : (h + 1) * half] = partial_of(x, h)

    for flag in g_flags:
        flag.wait_recv()
    for i in range(groups - 1):
        most = jnp.maximum(most, g_in[i])
    sent_g[...] = most
    for flag in z_flags:
        flag.start()

    for load in loads[8:]:
        load.wait()
    for i in range(parts, 2 * parts):
        step(i)
    for i, t in enumerate(order):
        at = slice(t * piece, (t + 1) * piece)
        step(2 * parts + i)
        sums = []
        for h in range(2):
            part = own[at, h * half : (h + 1) * half]
            sums.append(part + near_in[0, h, at, :].astype(f32) + near_in[1, h, at, :].astype(f32))
        projected = jnp.concatenate(sums, axis=1)
        value = jax.nn.sigmoid(gate_v[at, :].astype(f32)) * projected
        hidden = (residual_v[at, :].astype(f32) + rms_scale(value, mix_gain_ref[...])).astype(bf)
        hidden_ref[at, :] = hidden
        normed_ref[at, :] = rms_scale(hidden.astype(f32), expert_gain_ref[...]).astype(bf)

    for flag in z_flags:
        flag.wait_recv()
    for i in range(zs - 1):
        most = jnp.maximum(most, z_in[i])
    level = jnp.max(most)
    tier = jnp.int32(0)
    for cap in caps:
        tier = tier + jnp.where(level > cap, 1, 0).astype(jnp.int32)
    tier_ref[0, 0] = tier

    tail_copy.wait_send()
    for h in range(2):
        for t in range(parts):
            far_copy(h, t).wait_send()
            for d in range(2):
                near_copy(d, h, t).wait_send()
    for flag in x_flags + g_flags + z_flags:
        flag.wait_send()


def mixer(outer, inner, values, taps, weight, gate, residual, mix_gain, expert_gain, ids, share, scores, limit, caps):
    sizes = tuple(lax.axis_size(a) for a in SP_TP)
    zs, ys, cs, xs = sizes
    groups = ys * cs
    length, lanes = inner.shape
    rows, model = residual.shape
    half, parts, last = model // 2, 4, 16
    bf, f32 = jnp.bfloat16, jnp.float32
    vmem, anywhere = pl.BlockSpec(memory_space=pltpu.VMEM), pl.BlockSpec(memory_space=pltpu.HBM)
    dma = pltpu.SemaphoreType.DMA
    flag = (8, 128)
    return pl.pallas_call(
        functools.partial(mixer_kernel, sizes, limit, caps, parts),
        out_shape=(
            jax.ShapeDtypeStruct((rows, model), bf),
            jax.ShapeDtypeStruct((rows, model), bf),
            jax.ShapeDtypeStruct((rows, 128), f32),
            jax.ShapeDtypeStruct((8, 256), f32),
            jax.ShapeDtypeStruct((1, 1), jnp.int32),
        ),
        in_specs=[anywhere] * 12,
        out_specs=(vmem,) * 4 + (pl.BlockSpec(memory_space=pltpu.SMEM),),
        scratch_shapes=[
            pltpu.VMEM(taps.shape, f32), pltpu.VMEM((1, model), f32), pltpu.VMEM((1, model), f32),
            pltpu.VMEM((2, rows), jnp.int32), pltpu.VMEM((1, rows), f32), pltpu.VMEM((2, rows), f32),
            pltpu.VMEM(outer.shape, bf), pltpu.VMEM(inner.shape, bf), pltpu.VMEM(values.shape, bf),
            pltpu.VMEM(weight.shape, bf), pltpu.VMEM(gate.shape, bf), pltpu.VMEM(residual.shape, bf),
            pltpu.VMEM((length + 8, lanes), f32),
            pltpu.VMEM((length, lanes), bf),
            pltpu.VMEM((rows, model), f32),
            pltpu.VMEM((2, rows, half), bf), pltpu.VMEM((2, rows, half), bf),
            pltpu.VMEM((2, 2, rows, half), bf), pltpu.VMEM((2, 2, rows, half), bf),
            pltpu.VMEM((2, last, lanes), bf), pltpu.VMEM((2, last, lanes), bf),
            pltpu.VMEM((128, 256), f32),
            pltpu.VMEM(flag, f32), pltpu.VMEM((xs - 1, *flag), f32),
            pltpu.VMEM((groups - 1, *flag), f32), pltpu.VMEM((zs - 1, *flag), f32),
            pltpu.VMEM(flag, f32), pltpu.VMEM(flag, f32),
            dma((12,)), dma, dma,
            dma((2, parts)), dma((2, parts)), dma((2, 2, parts)), dma((2, 2, parts)),
            dma((xs - 1,)), dma((xs - 1,)), dma((groups - 1,)), dma((groups - 1,)), dma((zs - 1,)), dma((zs - 1,)),
        ],
        compiler_params=pltpu.CompilerParams(
            collective_id=1, has_side_effects=True, vmem_limit_bytes=VMEM_LIMIT - MIXER_ROOM
        ),
        name="mixer",
    )(
        taps, mix_gain[None, :], expert_gain[None, :], ids.T, share[None, :], scores.T,
        outer, inner, values, weight, gate, residual,
    )


def expert_kernel(
    zs, ys, cs, cap, slots,
    normed_ref, hidden_ref, columns_ref, lanes_ref, gate_hbm, up_hbm, down_hbm,
    out_ref,
    pick, weigh, meta, s1, r1, s2, r2, o2, b2, o1, b1, metar, onehot_t, onehot, acc, act, partial,
    gate_v, up_v, down_v,
    z_send, z_recv, g_send, g_recv, bg_send, bg_recv, bz_send, bz_recv, m_send, m_recv, w_sem,
):
    z, y, c = lax.axis_index(Z), lax.axis_index(Y), lax.axis_index(CORE)
    groups = ys * cs
    g_me = y * cs + c
    chunks = s1.shape[0]
    each = chunks // 2
    high = -(-cap // 8) * 8
    width = s2.shape[3]
    odd = cap % 8
    folds = 8 // odd if odd else 1
    side, whole = width // folds, cap - odd
    tokens = normed_ref.shape[0]
    rows = zs * high
    padded = onehot_t.shape[1]
    total = groups * slots
    bf, f32 = jnp.bfloat16, jnp.float32
    one, zero = jnp.ones((), f32), jnp.zeros((), f32)

    weights = [
        pltpu.make_async_copy(src, dst, w_sem.at[i])
        for i, (src, dst) in enumerate(((gate_hbm, gate_v), (up_hbm, up_v), (down_hbm, down_v)))
    ]
    for copy in weights:
        copy.start()

    def z_peer(o):
        return lax.rem(z + o, zs)

    def g_peer(o):
        return lax.rem(g_me + o, groups)

    def g_device(g):
        return {Y: lax.div(g, cs), CORE: lax.rem(g, cs)}

    barrier = pltpu.get_barrier_semaphore()
    for o in range(1, zs):
        pl.semaphore_signal(barrier, inc=1, device_id={Z: z_peer(o)}, device_id_type=MESH)
    for o in range(1, groups):
        pl.semaphore_signal(barrier, inc=1, device_id=g_device(g_peer(o)), device_id_type=MESH)

    def z_copy(src, dst, send, recv, k, o):
        return pltpu.make_async_remote_copy(
            src_ref=src.at[k, z_peer(o)], dst_ref=dst.at[k, z],
            send_sem=send.at[k, o - 1], recv_sem=recv.at[k, o - 1],
            device_id={Z: z_peer(o)}, device_id_type=MESH,
        )

    def g_copy(src, dst, send, recv, k, o):
        return pltpu.make_async_remote_copy(
            src_ref=src.at[k, g_peer(o)], dst_ref=dst.at[k, g_me],
            send_sem=send.at[k, o - 1], recv_sem=recv.at[k, o - 1],
            device_id=g_device(g_peer(o)), device_id_type=MESH,
        )

    def m_copy(o):
        return pltpu.make_async_remote_copy(
            src_ref=meta.at[z_peer(o)], dst_ref=metar.at[z],
            send_sem=m_send.at[o - 1], recv_sem=m_recv.at[o - 1],
            device_id={Z: z_peer(o)}, device_id_type=MESH,
        )

    z_sends = functools.partial(z_copy, s1, r1, z_send, z_recv)
    g_sends = functools.partial(g_copy, s2, r2, g_send, g_recv)
    g_backs = functools.partial(g_copy, o2, b2, bg_send, bg_recv)
    z_backs = functools.partial(z_copy, o1, b1, bz_send, bz_recv)

    def start_all(copies, k, count):
        for o in range(1, count):
            copies(k, o).start()

    def wait_recv_all(copies, k, count):
        for o in range(1, count):
            copies(k, o).wait_recv()

    def half_of(k):
        return lax.div(k, each)

    def columns(k):
        return pl.ds(pl.multiple_of(lax.rem(k, each) * width, width), width)

    def fold(value):
        value = value.reshape(zs, high, width)
        if folds == 1:
            return value.astype(bf)
        blocks = []
        for j in range(zs):
            sides = [value[j, :, i * side : (i + 1) * side] for i in range(folds)]
            ends = sides[0][whole:]
            for i in range(1, folds):
                ends = ends + pltpu.roll(sides[i][whole:], i * odd, 0)
            blocks.append(jnp.concatenate([v[:whole] for v in sides] + [ends], axis=0)[None])
        return jnp.concatenate(blocks, axis=0).astype(bf)

    def unfold(ref, k):
        value = ref[k].astype(f32)
        if folds == 1:
            blocks = [value.reshape(rows, width)]
        else:
            blocks = []
            for j in range(zs):
                ends = value[j, folds * whole :]
                sides = []
                for i in range(folds):
                    end = pltpu.roll(ends, 8 - i * odd, 0) if i else ends
                    sides.append(jnp.concatenate([value[j, i * whole : (i + 1) * whole], end], axis=0))
                blocks.append(jnp.concatenate(sides, axis=1))
        if padded > rows:
            blocks.append(jnp.zeros((padded - rows, width), f32))
        return jnp.concatenate(blocks, axis=0).astype(bf)

    def row_of(block, place, h):
        inside = (block >= float(h * zs)) & (block < float((h + 1) * zs))
        return jnp.where(inside, (block - float(h * zs)) * high + place, -1.0)

    lane_rows = [
        [row_of(lanes_ref[k : k + 1, 0:tokens], lanes_ref[2 + k : 3 + k, 0:tokens], h) for k in range(2)]
        for h in range(2)
    ]
    slot_of = [lanes_ref[4 + k : 5 + k, 0:tokens] + 1.0 for k in range(2)]
    numbers = lax.broadcasted_iota(jnp.int32, (padded, tokens), 0).astype(f32)
    for h in range(2):
        hit = [numbers == r for r in lane_rows[h]]
        pick[h] = jnp.where(hit[0] | hit[1], one, zero).astype(bf)

    def pick_rows(k):
        value = dot32(pick[half_of(k)], normed_ref[:, columns(k)])
        s1[k] = fold(value[:rows])
        r1[k, z] = s1[k, z]

    pl.semaphore_wait(barrier, zs + groups - 2)
    for k in range(DEPTH):
        pick_rows(k)
        start_all(z_sends, k, zs)

    place = lax.broadcasted_iota(jnp.int32, (high, tokens), 0).astype(f32)
    blank = jnp.full((128 - high, 128), -1.0, f32)
    spot = lax.broadcasted_iota(jnp.int32, (128, 128), 1).astype(f32)
    for j in range(zs):
        both = jnp.zeros((128, 128), f32)
        for h in range(2):
            hit = [place + float(j * high) == r for r in lane_rows[h]]
            found = jnp.where(hit[0], slot_of[0], 0.0) + jnp.where(hit[1], slot_of[1], 0.0)
            found = jnp.broadcast_to(jnp.sum(found, axis=1, keepdims=True) - 1.0, (high, 128))
            both = jnp.where(spot == float(h), jnp.concatenate([found, blank], axis=0), both)
        meta[j] = jnp.transpose(both)[0:8, :]
    for o in range(1, zs):
        m_copy(o).start()
    row_lane = lax.broadcasted_iota(jnp.int32, (tokens, padded), 1).astype(f32)
    for h in range(2):
        weight = jnp.zeros((tokens, padded), f32)
        for k in range(2):
            row = row_of(columns_ref[:, k : k + 1], columns_ref[:, 2 + k : 3 + k], h)
            weight = weight + jnp.where(row == row_lane, columns_ref[:, 6 + k : 7 + k], 0.0)
        rounded = weight.astype(bf)
        weigh[h, 0] = rounded
        weigh[h, 1] = (weight - rounded.astype(f32)).astype(bf)
    metar[z] = meta[z]

    @pl.loop(DEPTH, chunks)
    def _(k):
        pick_rows(k)

    for o in range(1, zs):
        m_copy(o).wait_recv()
    places = lax.broadcasted_iota(jnp.int32, (high, total), 1).astype(f32)
    for h in range(2):
        blocks = []
        for j in range(zs):
            where = jnp.transpose(metar[j])[:high, h : h + 1]
            blocks.append(jnp.where(where == places, one, zero))
        if padded > rows:
            blocks.append(jnp.zeros((padded - rows, total), f32))
        table = jnp.concatenate(blocks, axis=0)
        onehot_t[h] = table.astype(bf)
        onehot[h] = jnp.transpose(table).astype(bf)

    weights[0].wait()
    weights[1].wait()
    weights[2].wait()
    acc[...] = jnp.zeros_like(acc)
    units = gate_v.shape[1]

    @pl.loop(0, 2 * chunks)
    def _(t):
        @pl.when(t < chunks)
        def _():
            wait_recv_all(z_sends, t, zs)

        @pl.when(t >= chunks)
        def _():
            wait_recv_all(z_backs, t - chunks, zs)

        @pl.when(t + DEPTH < chunks)
        def _():
            start_all(z_sends, t + DEPTH, zs)

        @pl.when((t > each) & (t <= each + chunks))
        def _():
            k = t - each - 1
            wait_recv_all(g_backs, k, groups)

            @pl.when(lax.rem(k, each) + DEPTH < each)
            def _():
                start_all(g_backs, k + DEPTH, groups)

            value = dot32(onehot_t[half_of(k)], b2[k].reshape(total, width))
            o1[k] = fold(value[:rows])
            b1[k, z] = o1[k, z]
            start_all(z_backs, k, zs)

        @pl.when(t < chunks)
        def _():
            value = dot32(onehot[half_of(t)], unfold(r1, t)).astype(bf)
            s2[t] = value.reshape(groups, slots, width)
            start_all(g_sends, t, groups)
            r2[t, g_me] = s2[t, g_me]

        @pl.when((t >= 1) & (t <= chunks))
        def _():
            k = t - 1
            wait_recv_all(g_sends, k, groups)
            values = r2[k].reshape(total, width)
            h = half_of(k)
            acc[h, :, :units] += dot32(values, gate_v[columns(k), :])
            acc[h, :, units:] += dot32(values, up_v[columns(k), :])

        @pl.when((t == each) | (t == chunks))
        def _():
            h = half_of(t - 1)
            first = acc[h, :, :units]
            act[...] = (first / (1.0 + jnp.exp(-first)) * acc[h, :, units:]).astype(bf)
            for i in range(each):
                k = h * each + i
                value = dot32(act[...], down_v[:, i * width : (i + 1) * width]).astype(bf)
                o2[k] = value.reshape(groups, slots, width)
                b2[k, g_me] = o2[k, g_me]
                if i < DEPTH:
                    start_all(g_backs, k, groups)

        @pl.when(t >= chunks)
        def _():
            k = t - chunks
            h = half_of(k)
            values = unfold(b1, k)
            at = columns(k)
            value = dot32(weigh[h, 0], values) + dot32(weigh[h, 1], values)

            @pl.when(h == 0)
            def _():
                partial[:, at] = hidden_ref[:, at].astype(f32) + value

            @pl.when(h == 1)
            def _():
                out_ref[:, at] = (partial[:, at] + value).astype(bf)

    for o in range(1, zs):
        m_copy(o).wait_send()

    @pl.loop(0, chunks)
    def _(k):
        for o in range(1, zs):
            z_sends(k, o).wait_send()
            z_backs(k, o).wait_send()
        for o in range(1, groups):
            g_sends(k, o).wait_send()
            g_backs(k, o).wait_send()


def routed_experts(cap, limit, collective, normed, hidden, columns, lanes, gate, up, down):
    zs, ys, cs = lax.axis_size(Z), lax.axis_size(Y), lax.axis_size(CORE)
    groups = ys * cs
    tokens, model = normed.shape
    slots = zs * limit // 2
    high = -(-cap // 8) * 8
    padded = -(-zs * high // 128) * 128
    chunks = 2 * model // WIDTH
    units = gate.shape[1]
    bf, f32 = jnp.bfloat16, jnp.float32
    vmem, anywhere = pl.BlockSpec(memory_space=pltpu.VMEM), pl.BlockSpec(memory_space=pltpu.HBM)
    folds = 8 // (cap % 8) if cap % 8 else 1
    z_block = (chunks, zs, folds * cap, WIDTH // folds)
    g_block = (chunks, groups, slots, WIDTH)
    dma = pltpu.SemaphoreType.DMA
    z_sem, g_sem, m_sem = dma((chunks, zs - 1)), dma((chunks, groups - 1)), dma((zs - 1,))
    total = groups * slots
    return pl.pallas_call(
        functools.partial(expert_kernel, zs, ys, cs, cap, slots),
        out_shape=jax.ShapeDtypeStruct((tokens, model), bf),
        in_specs=[vmem] * 4 + [anywhere] * 3,
        out_specs=vmem,
        scratch_shapes=[
            pltpu.VMEM((2, padded, tokens), bf), pltpu.VMEM((2, 2, tokens, padded), bf),
            pltpu.VMEM((zs, 8, 128), f32),
            pltpu.VMEM(z_block, bf), pltpu.VMEM(z_block, bf),
            pltpu.VMEM(g_block, bf), pltpu.VMEM(g_block, bf),
            pltpu.VMEM(g_block, bf), pltpu.VMEM(g_block, bf),
            pltpu.VMEM(z_block, bf), pltpu.VMEM(z_block, bf),
            pltpu.VMEM((zs, 8, 128), f32),
            pltpu.VMEM((2, padded, total), bf),
            pltpu.VMEM((2, total, padded), bf),
            pltpu.VMEM((2, total, 2 * units), f32),
            pltpu.VMEM((total, units), bf),
            pltpu.VMEM((tokens, model), f32),
            pltpu.VMEM(gate.shape, bf), pltpu.VMEM(up.shape, bf), pltpu.VMEM(down.shape, bf),
            z_sem, z_sem, g_sem, g_sem, g_sem, g_sem, z_sem, z_sem, m_sem, m_sem,
            dma((3,)),
        ],
        compiler_params=pltpu.CompilerParams(
            collective_id=collective, has_side_effects=True, vmem_limit_bytes=VMEM_LIMIT - EXPERT_ROOM
        ),
        name="routed_experts",
    )(normed, hidden, columns, lanes, gate, up, down)


def per_device(
    conv_outer,
    conv_inner,
    conv_input,
    conv_taps,
    out_weight,
    mix_gate,
    residual,
    mix_gain,
    expert_gain,
    expert_ids,
    group_share,
    pair_scores,
    gate_experts,
    up_experts,
    down_experts,
):
    limit = 2 * expert_ids.shape[1] * residual.shape[0] // (lax.axis_size(SP) * gate_experts.shape[0])
    worst = limit * lax.axis_size(Y) * lax.axis_size(CORE) // 2
    caps = [cap for cap in USUAL if cap < worst]
    hidden, normed, columns, lanes, tier = mixer(
        conv_outer, conv_inner, conv_input, conv_taps, out_weight, mix_gate, residual, mix_gain, expert_gain,
        expert_ids, group_share, pair_scores, limit, caps,
    )
    arguments = (normed, hidden, columns, lanes, gate_experts[0], up_experts[0], down_experts[0])
    return lax.switch(
        tier[0, 0],
        [functools.partial(routed_experts, cap, limit, 2 + i) for i, cap in enumerate(caps + [worst])],
        *arguments,
    )


def solution(mesh):
    torus = Mesh(mesh.devices.reshape(8, 4, 2, mesh.shape["tp"]), SP_TP)
    return jax.shard_map(
        per_device,
        mesh=torus,
        in_specs=(
            P(SP, X),
            P(SP, X),
            P(SP, X),
            P(None, X),
            P(X, None),
            P(SP_TP, None),
            P(SP_TP, None),
            P(),
            P(),
            P(SP_TP, None),
            P(SP_TP),
            P(SP_TP, None),
            P(SP, None, None),
            P(SP, None, None),
            P(SP, None, None),
        ),
        out_specs=P(SP_TP, None),
        check_vma=False,
    )
```

```python
import functools

import jax
import jax.numpy as jnp
from jax import lax
from jax.experimental import pallas as pl
from jax.experimental.pallas import tpu as pltpu
from jax.sharding import Mesh
from jax.sharding import PartitionSpec as P

Z, Y, CORE, X = "sp_0", "sp_1", "sp_2", "tp"
SP = (Z, Y, CORE)
SP_TP = (Z, Y, CORE, X)
MESH = pl.DeviceIdType.MESH

epsilon = 1e-06
WIDTH = 512
VMEM_LIMIT = 67043328
MIXER_ROOM = 1835008
EXPERT_ROOM = 2726297
DEPTH = 2
WINDOW = 4
USUAL = (36, 40)


def rms_scale(values, gain):
    return values * lax.rsqrt(jnp.mean(values * values, axis=-1, keepdims=True) + epsilon) * gain


def dot32(a, b):
    return jnp.dot(a, b, preferred_element_type=jnp.float32)


def mixer_kernel(
    sizes, limit, caps, parts,
    taps_hbm, mix_gain_hbm, expert_gain_hbm, ids_hbm, share_hbm, scores_hbm,
    outer_hbm, inner_hbm, input_hbm, weight_hbm, gate_hbm, residual_hbm,
    hidden_ref, normed_ref, columns_ref, lanes_ref, tier_ref,
    taps_ref, mix_gain_ref, expert_gain_ref, ids_v, share_v, scores_v,
    outer_v, inner_v, input_v, weight_v, gate_v, residual_v,
    products, mixed, own, far, far_in, near, near_in, tails, tail_in, table,
    mine, x_in, g_in, z_in, sent_x, sent_g,
    l_sem, t_send, t_recv, f_send, f_recv, n_send, n_recv, mx_send, mx_recv, mg_send, mg_recv, mz_send, mz_recv,
):
    zs, ys, cs, xs = sizes
    z, y, c, x = (lax.axis_index(a) for a in SP_TP)
    groups = ys * cs
    g_me = y * cs + c
    devices = zs * groups
    me = z * groups + g_me
    bf, f32 = jnp.bfloat16, jnp.float32
    length, lanes = inner_v.shape
    rows = length // xs
    half = own.shape[1] // 2
    piece = rows // parts

    loads = [
        pltpu.make_async_copy(src, dst, l_sem.at[i])
        for i, (src, dst) in enumerate(
            (
                (inner_hbm, inner_v), (input_hbm, input_v), (outer_hbm, outer_v),
                (taps_hbm, taps_ref), (weight_hbm, weight_v), (ids_hbm, ids_v), (share_hbm, share_v),
                (scores_hbm, scores_v), (gate_hbm, gate_v), (residual_hbm, residual_v),
                (mix_gain_hbm, mix_gain_ref), (expert_gain_hbm, expert_gain_ref),
            )
        )
    ]
    for load in loads[:8]:
        load.start()

    def sp_device(index):
        return {Z: lax.div(index, groups), Y: lax.div(lax.rem(index, groups), cs), CORE: lax.rem(index, cs)}

    following, preceding = lax.rem(me + 1, devices), lax.rem(me + devices - 1, devices)
    x_peers = [{X: lax.rem(x + o, xs)} for o in range(1, xs)]
    z_peers = [{Z: lax.rem(z + o, zs)} for o in range(1, zs)]
    g_peers = []
    for o in range(1, groups):
        g = lax.rem(g_me + o, groups)
        g_peers.append({Y: lax.div(g, cs), CORE: lax.rem(g, cs)})
    everyone = x_peers + z_peers + g_peers + [sp_device(following), sp_device(preceding)]
    barrier = pltpu.get_barrier_semaphore()
    for peer in everyone:
        pl.semaphore_signal(barrier, inc=1, device_id=peer, device_id_type=MESH)

    loads[0].wait()
    loads[1].wait()
    last = tails.shape[1]
    tails[0] = inner_v[length - last :, :]
    tails[1] = input_v[length - last :, :]
    tail_copy = pltpu.make_async_remote_copy(
        src_ref=tails, dst_ref=tail_in, send_sem=t_send, recv_sem=t_recv,
        device_id=sp_device(following), device_id_type=MESH,
    )

    pad = 8
    products[0:pad, :] = jnp.zeros((pad, lanes), f32)
    for b in range(xs):
        at = slice(b * rows, (b + 1) * rows)
        products[pad + b * rows : pad + (b + 1) * rows, :] = inner_v[at, :].astype(f32) * input_v[at, :].astype(f32)
    loads[2].wait()
    loads[3].wait()

    def convolve(start, count):
        base = products[pl.ds(start, count + pad), :]
        conv = taps_ref[0:1, :] * base[pad - 2 : pad - 2 + count]
        conv = conv + taps_ref[1:2, :] * base[pad - 1 : pad - 1 + count]
        conv = conv + taps_ref[2:3, :] * base[pad : pad + count]
        mixed[pl.ds(start, count), :] = (outer_v[pl.ds(start, count), :].astype(f32) * conv).astype(bf)

    def convolve_block(owner):
        convolve(pl.multiple_of(owner * rows, 16), rows)

    convolve_block(lax.rem(x + 2, xs))
    loads[4].wait()

    right, left = lax.rem(x + 1, xs), lax.rem(x + xs - 1, xs)
    ways = (right, left)

    def partial_of(owner, h, start=0, count=rows):
        block = mixed[pl.ds(pl.multiple_of(owner * rows + start, 16), count), :]
        return dot32(block, weight_v[:, h * half : (h + 1) * half])

    def far_copy(h, t):
        at = pl.ds(t * piece, piece)
        return pltpu.make_async_remote_copy(
            src_ref=far.at[h, at], dst_ref=far_in.at[h, at],
            send_sem=f_send.at[h, t], recv_sem=f_recv.at[h, t],
            device_id={X: ways[h]}, device_id_type=MESH,
        )

    def near_copy(d, h, t):
        at = pl.ds(t * piece, piece)
        return pltpu.make_async_remote_copy(
            src_ref=near.at[d, h, at], dst_ref=near_in.at[d, h, at],
            send_sem=n_send.at[d, h, t], recv_sem=n_recv.at[d, h, t],
            device_id={X: ways[d]}, device_id_type=MESH,
        )

    order = [*range(1, parts), 0]
    steps = [functools.partial(far_copy, t=t) for t in order]
    steps += [lambda d, t=t: near_copy(d, 1 - d, t) for t in order]
    steps += [lambda d, t=t: near_copy(d, d, t) for t in order]

    opposite = lax.rem(x + 2, xs)
    for h in range(2):
        far[h, piece:, :] = partial_of(opposite, h, piece, rows - piece).astype(bf)
    pl.semaphore_wait(barrier, len(everyone))
    tail_copy.start()
    for i in range(WINDOW):
        for h in range(2):
            steps[i](h).start()
    for load in loads[8:]:
        load.start()
    for owner in (right, left, x):
        convolve_block(owner)
    tail_copy.wait_recv()
    earlier = tail_in[0].astype(f32) * tail_in[1].astype(f32)
    earlier = jnp.where(me == 0, jnp.zeros_like(earlier), earlier)
    products[0:pad, :] = earlier[last - pad :, :]
    convolve(0, last)
    for h in range(2):
        far[h, :piece, :] = partial_of(opposite, h, 0, piece).astype(bf)
    for d in range(2):
        near[d, 1 - d] = partial_of(ways[d], 1 - d).astype(bf)
    for d in range(2):
        own[:, d * half : (d + 1) * half] = partial_of(ways[d], d)

    def step(i):
        for d in range(2):
            steps[i](d).wait_recv()
            if i < parts:
                at = slice(order[i] * piece, (order[i] + 1) * piece)
                near[d, d, at, :] = (own[at, d * half : (d + 1) * half] + far_in[d, at, :].astype(f32)).astype(bf)
            if i + WINDOW < len(steps):
                steps[i + WINDOW](d).start()

    step(0)
    tokens = ids_v.shape[1]
    for load in loads[5:8]:
        load.wait()
    table[...] = jnp.zeros_like(table)
    table[0:2, 0:tokens] = ids_v[...].astype(f32)
    table[2:4, 0:tokens] = scores_v[...]
    table[4:5, 0:tokens] = share_v[...]
    given = jnp.transpose(table[...])[0:tokens, :]
    expert = [given[:, k : k + 1] for k in range(2)]
    z_of = [jnp.floor((e + 0.5) / groups) for e in expert]
    lane = lax.broadcasted_iota(jnp.int32, (tokens, 128), 1).astype(f32)
    before = jnp.where(
        lax.broadcasted_iota(jnp.int32, (tokens, tokens), 1) < lax.broadcasted_iota(jnp.int32, (tokens, tokens), 0),
        jnp.ones((), f32), jnp.zeros((), f32),
    ).astype(bf)

    def ranks(labels):
        marks = [jnp.where(label == lane, jnp.ones((), f32), jnp.zeros((), f32)) for label in labels]
        firsts = jnp.sum(marks[0], axis=0, keepdims=True)
        seen = [dot32(before, marks[0].astype(bf)), dot32(before, marks[1].astype(bf)) + firsts]
        found = [jnp.sum(mark * s, axis=1, keepdims=True) for mark, s in zip(marks, seen)]
        return found, jnp.max(firsts + jnp.sum(marks[1], axis=0, keepdims=True), axis=1, keepdims=True)

    rank, _ = ranks(expert)
    lower = [jnp.floor(r * 0.5) for r in rank]
    parity = [r + e - 2.0 * jnp.floor((r + e) * 0.5) for r, e in zip(rank, expert)]
    block = [h * zs + zz for h, zz in zip(parity, z_of)]
    place, most = ranks(block)
    most = jnp.broadcast_to(most, (8, 128))
    mine[...] = most

    def flag_copy(src, dst, send, recv, i, peer):
        return pltpu.make_async_remote_copy(
            src_ref=src, dst_ref=dst.at[i], send_sem=send.at[i], recv_sem=recv.at[i],
            device_id=peer, device_id_type=MESH,
        )

    x_flags = [flag_copy(mine, x_in, mx_send, mx_recv, i, p) for i, p in enumerate(x_peers)]
    g_flags = [flag_copy(sent_x, g_in, mg_send, mg_recv, i, p) for i, p in enumerate(g_peers)]
    z_flags = [flag_copy(sent_g, z_in, mz_send, mz_recv, i, p) for i, p in enumerate(z_peers)]
    for flag in x_flags:
        flag.start()

    info = []
    step(1)
    scores = [given[:, 2 + k : 3 + k] for k in range(2)]
    top = jnp.maximum(scores[0], scores[1])
    powers = [jnp.exp(v - top) for v in scores]
    for k in range(2):
        slot = (expert[k] - groups * z_of[k]) * (zs * limit / 2) + (z * limit).astype(f32) * 0.5 + lower[k]
        info.append((block[k], place[k], slot, given[:, 4:5] * (powers[k] / (powers[0] + powers[1]))))
    column = jnp.zeros((tokens, 128), f32)
    for i in range(4):
        for k in range(2):
            column = column + jnp.where(lane == 2 * i + k, info[k][i], 0.0)
    columns_ref[...] = column
    spare = jnp.zeros((table.shape[1] - tokens, 128), f32)
    lanes_ref[...] = jnp.transpose(jnp.concatenate([column, spare], axis=0))[0:8, :]
    step(2)

    for flag in x_flags:
        flag.wait_recv()
    for i in range(xs - 1):
        most = jnp.maximum(most, x_in[i])
    sent_x[...] = most
    for flag in g_flags:
        flag.start()

    for i in range(3, parts):
        step(i)
    for h in range(2):
        own[:, h * half : (h + 1) * half] = partial_of(x, h)

    for flag in g_flags:
        flag.wait_recv()
    for i in range(groups - 1):
        most = jnp.maximum(most, g_in[i])
    sent_g[...] = most
    for flag in z_flags:
        flag.start()

    for load in loads[8:]:
        load.wait()
    for i in range(parts, 2 * parts):
        step(i)
    for i, t in enumerate(order):
        at = slice(t * piece, (t + 1) * piece)
        step(2 * parts + i)
        sums = []
        for h in range(2):
            part = own[at, h * half : (h + 1) * half]
            sums.append(part + near_in[0, h, at, :].astype(f32) + near_in[1, h, at, :].astype(f32))
        projected = jnp.concatenate(sums, axis=1)
        value = jax.nn.sigmoid(gate_v[at, :].astype(f32)) * projected
        hidden = (residual_v[at, :].astype(f32) + rms_scale(value, mix_gain_ref[...])).astype(bf)
        hidden_ref[at, :] = hidden
        normed_ref[at, :] = rms_scale(hidden.astype(f32), expert_gain_ref[...]).astype(bf)

    for flag in z_flags:
        flag.wait_recv()
    for i in range(zs - 1):
        most = jnp.maximum(most, z_in[i])
    level = jnp.max(most)
    tier = jnp.int32(0)
    for cap in caps:
        tier = tier + jnp.where(level > cap, 1, 0).astype(jnp.int32)
    tier_ref[0, 0] = tier

    tail_copy.wait_send()
    for h in range(2):
        for t in range(parts):
            far_copy(h, t).wait_send()
            for d in range(2):
                near_copy(d, h, t).wait_send()
    for flag in x_flags + g_flags + z_flags:
        flag.wait_send()


def mixer(outer, inner, values, taps, weight, gate, residual, mix_gain, expert_gain, ids, share, scores, limit, caps):
    sizes = tuple(lax.axis_size(a) for a in SP_TP)
    zs, ys, cs, xs = sizes
    groups = ys * cs
    length, lanes = inner.shape
    rows, model = residual.shape
    half, parts, last = model // 2, 6, 16
    bf, f32 = jnp.bfloat16, jnp.float32
    vmem, anywhere = pl.BlockSpec(memory_space=pltpu.VMEM), pl.BlockSpec(memory_space=pltpu.HBM)
    dma = pltpu.SemaphoreType.DMA
    flag = (8, 128)
    return pl.pallas_call(
        functools.partial(mixer_kernel, sizes, limit, caps, parts),
        out_shape=(
            jax.ShapeDtypeStruct((rows, model), bf),
            jax.ShapeDtypeStruct((rows, model), bf),
            jax.ShapeDtypeStruct((rows, 128), f32),
            jax.ShapeDtypeStruct((8, 256), f32),
            jax.ShapeDtypeStruct((1, 1), jnp.int32),
        ),
        in_specs=[anywhere] * 12,
        out_specs=(vmem,) * 4 + (pl.BlockSpec(memory_space=pltpu.SMEM),),
        scratch_shapes=[
            pltpu.VMEM(taps.shape, f32), pltpu.VMEM((1, model), f32), pltpu.VMEM((1, model), f32),
            pltpu.VMEM((2, rows), jnp.int32), pltpu.VMEM((1, rows), f32), pltpu.VMEM((2, rows), f32),
            pltpu.VMEM(outer.shape, bf), pltpu.VMEM(inner.shape, bf), pltpu.VMEM(values.shape, bf),
            pltpu.VMEM(weight.shape, bf), pltpu.VMEM(gate.shape, bf), pltpu.VMEM(residual.shape, bf),
            pltpu.VMEM((length + 8, lanes), f32),
            pltpu.VMEM((length, lanes), bf),
            pltpu.VMEM((rows, model), f32),
            pltpu.VMEM((2, rows, half), bf), pltpu.VMEM((2, rows, half), bf),
            pltpu.VMEM((2, 2, rows, half), bf), pltpu.VMEM((2, 2, rows, half), bf),
            pltpu.VMEM((2, last, lanes), bf), pltpu.VMEM((2, last, lanes), bf),
            pltpu.VMEM((128, 256), f32),
            pltpu.VMEM(flag, f32), pltpu.VMEM((xs - 1, *flag), f32),
            pltpu.VMEM((groups - 1, *flag), f32), pltpu.VMEM((zs - 1, *flag), f32),
            pltpu.VMEM(flag, f32), pltpu.VMEM(flag, f32),
            dma((12,)), dma, dma,
            dma((2, parts)), dma((2, parts)), dma((2, 2, parts)), dma((2, 2, parts)),
            dma((xs - 1,)), dma((xs - 1,)), dma((groups - 1,)), dma((groups - 1,)), dma((zs - 1,)), dma((zs - 1,)),
        ],
        compiler_params=pltpu.CompilerParams(
            collective_id=1, has_side_effects=True, vmem_limit_bytes=VMEM_LIMIT - MIXER_ROOM
        ),
        name="mixer",
    )(
        taps, mix_gain[None, :], expert_gain[None, :], ids.T, share[None, :], scores.T,
        outer, inner, values, weight, gate, residual,
    )


def expert_kernel(
    zs, ys, cs, cap, slots,
    normed_ref, hidden_ref, columns_ref, lanes_ref, gate_hbm, up_hbm, down_hbm,
    out_ref,
    pick, weigh, meta, s1, r1, s2, r2, o2, b2, o1, b1, metar, onehot_t, onehot, acc, act, partial,
    gate_v, up_v, down_v,
    z_send, z_recv, g_send, g_recv, bg_send, bg_recv, bz_send, bz_recv, m_send, m_recv, w_sem,
):
    z, y, c = lax.axis_index(Z), lax.axis_index(Y), lax.axis_index(CORE)
    groups = ys * cs
    g_me = y * cs + c
    chunks = s1.shape[0]
    each = chunks // 2
    high = -(-cap // 8) * 8
    width = s2.shape[3]
    odd = cap % 8
    folds = 8 // odd if odd else 1
    side, whole = width // folds, cap - odd
    tokens = normed_ref.shape[0]
    rows = zs * high
    padded = onehot_t.shape[1]
    total = groups * slots
    bf, f32 = jnp.bfloat16, jnp.float32
    one, zero = jnp.ones((), f32), jnp.zeros((), f32)

    weights = [
        pltpu.make_async_copy(src, dst, w_sem.at[i])
        for i, (src, dst) in enumerate(((gate_hbm, gate_v), (up_hbm, up_v), (down_hbm, down_v)))
    ]
    for copy in weights:
        copy.start()

    def z_peer(o):
        return lax.rem(z + o, zs)

    def g_peer(o):
        return lax.rem(g_me + o, groups)

    def g_device(g):
        return {Y: lax.div(g, cs), CORE: lax.rem(g, cs)}

    barrier = pltpu.get_barrier_semaphore()
    for o in range(1, zs):
        pl.semaphore_signal(barrier, inc=1, device_id={Z: z_peer(o)}, device_id_type=MESH)
    for o in range(1, groups):
        pl.semaphore_signal(barrier, inc=1, device_id=g_device(g_peer(o)), device_id_type=MESH)

    def z_copy(src, dst, send, recv, k, o):
        return pltpu.make_async_remote_copy(
            src_ref=src.at[k, z_peer(o)], dst_ref=dst.at[k, z],
            send_sem=send.at[k, o - 1], recv_sem=recv.at[k, o - 1],
            device_id={Z: z_peer(o)}, device_id_type=MESH,
        )

    def g_copy(src, dst, send, recv, k, o):
        return pltpu.make_async_remote_copy(
            src_ref=src.at[k, g_peer(o)], dst_ref=dst.at[k, g_me],
            send_sem=send.at[k, o - 1], recv_sem=recv.at[k, o - 1],
            device_id=g_device(g_peer(o)), device_id_type=MESH,
        )

    def m_copy(o):
        return pltpu.make_async_remote_copy(
            src_ref=meta.at[z_peer(o)], dst_ref=metar.at[z],
            send_sem=m_send.at[o - 1], recv_sem=m_recv.at[o - 1],
            device_id={Z: z_peer(o)}, device_id_type=MESH,
        )

    z_sends = functools.partial(z_copy, s1, r1, z_send, z_recv)
    g_sends = functools.partial(g_copy, s2, r2, g_send, g_recv)
    g_backs = functools.partial(g_copy, o2, b2, bg_send, bg_recv)
    z_backs = functools.partial(z_copy, o1, b1, bz_send, bz_recv)

    def start_all(copies, k, count):
        for o in range(1, count):
            copies(k, o).start()

    def wait_recv_all(copies, k, count):
        for o in range(1, count):
            copies(k, o).wait_recv()

    def half_of(k):
        return lax.div(k, each)

    def columns(k):
        return pl.ds(pl.multiple_of(lax.rem(k, each) * width, width), width)

    def fold(value):
        value = value.reshape(zs, high, width)
        if folds == 1:
            return value.astype(bf)
        blocks = []
        for j in range(zs):
            sides = [value[j, :, i * side : (i + 1) * side] for i in range(folds)]
            ends = sides[0][whole:]
            for i in range(1, folds):
                ends = ends + pltpu.roll(sides[i][whole:], i * odd, 0)
            blocks.append(jnp.concatenate([v[:whole] for v in sides] + [ends], axis=0)[None])
        return jnp.concatenate(blocks, axis=0).astype(bf)

    def unfold(ref, k):
        value = ref[k].astype(f32)
        if folds == 1:
            blocks = [value.reshape(rows, width)]
        else:
            blocks = []
            for j in range(zs):
                ends = value[j, folds * whole :]
                sides = []
                for i in range(folds):
                    end = pltpu.roll(ends, 8 - i * odd, 0) if i else ends
                    sides.append(jnp.concatenate([value[j, i * whole : (i + 1) * whole], end], axis=0))
                blocks.append(jnp.concatenate(sides, axis=1))
        if padded > rows:
            blocks.append(jnp.zeros((padded - rows, width), f32))
        return jnp.concatenate(blocks, axis=0).astype(bf)

    def row_of(block, place, h):
        inside = (block >= float(h * zs)) & (block < float((h + 1) * zs))
        return jnp.where(inside, (block - float(h * zs)) * high + place, -1.0)

    lane_rows = [
        [row_of(lanes_ref[k : k + 1, 0:tokens], lanes_ref[2 + k : 3 + k, 0:tokens], h) for k in range(2)]
        for h in range(2)
    ]
    slot_of = [lanes_ref[4 + k : 5 + k, 0:tokens] + 1.0 for k in range(2)]
    numbers = lax.broadcasted_iota(jnp.int32, (padded, tokens), 0).astype(f32)

    def fill_pick(h):
        hit = [numbers == r for r in lane_rows[h]]
        pick[h] = jnp.where(hit[0] | hit[1], one, zero).astype(bf)

    fill_pick(0)

    def pick_rows(k):
        value = dot32(pick[half_of(k)], normed_ref[:, columns(k)])
        s1[k] = fold(value[:rows])
        r1[k, z] = s1[k, z]

    pl.semaphore_wait(barrier, zs + groups - 2)
    for k in range(DEPTH):
        pick_rows(k)
        start_all(z_sends, k, zs)

    fill_pick(1)
    place = lax.broadcasted_iota(jnp.int32, (high, tokens), 0).astype(f32)
    blank = jnp.full((128 - high, 128), -1.0, f32)
    spot = lax.broadcasted_iota(jnp.int32, (128, 128), 1).astype(f32)
    for j in range(zs):
        both = jnp.zeros((128, 128), f32)
        for h in range(2):
            hit = [place + float(j * high) == r for r in lane_rows[h]]
            found = jnp.where(hit[0], slot_of[0], 0.0) + jnp.where(hit[1], slot_of[1], 0.0)
            found = jnp.broadcast_to(jnp.sum(found, axis=1, keepdims=True) - 1.0, (high, 128))
            both = jnp.where(spot == float(h), jnp.concatenate([found, blank], axis=0), both)
        meta[j] = jnp.transpose(both)[0:8, :]
    for o in range(1, zs):
        m_copy(o).start()
    row_lane = lax.broadcasted_iota(jnp.int32, (tokens, padded), 1).astype(f32)
    for h in range(2):
        weight = jnp.zeros((tokens, padded), f32)
        for k in range(2):
            row = row_of(columns_ref[:, k : k + 1], columns_ref[:, 2 + k : 3 + k], h)
            weight = weight + jnp.where(row == row_lane, columns_ref[:, 6 + k : 7 + k], 0.0)
        rounded = weight.astype(bf)
        weigh[h, 0] = rounded
        weigh[h, 1] = (weight - rounded.astype(f32)).astype(bf)
    metar[z] = meta[z]

    @pl.loop(DEPTH, chunks)
    def _(k):
        pick_rows(k)

    for o in range(1, zs):
        m_copy(o).wait_recv()
    places = lax.broadcasted_iota(jnp.int32, (high, total), 1).astype(f32)
    for h in range(2):
        blocks = []
        for j in range(zs):
            where = jnp.transpose(metar[j])[:high, h : h + 1]
            blocks.append(jnp.where(where == places, one, zero))
        if padded > rows:
            blocks.append(jnp.zeros((padded - rows, total), f32))
        table = jnp.concatenate(blocks, axis=0)
        onehot_t[h] = table.astype(bf)
        onehot[h] = jnp.transpose(table).astype(bf)

    weights[0].wait()
    weights[1].wait()
    weights[2].wait()
    acc[...] = jnp.zeros_like(acc)
    units = gate_v.shape[1]

    @pl.loop(0, 2 * chunks)
    def _(t):
        @pl.when(t < chunks)
        def _():
            wait_recv_all(z_sends, t, zs)

        @pl.when(t >= chunks)
        def _():
            wait_recv_all(z_backs, t - chunks, zs)

        @pl.when(t + DEPTH < chunks)
        def _():
            start_all(z_sends, t + DEPTH, zs)

        @pl.when((t > each) & (t <= each + chunks))
        def _():
            k = t - each - 1
            wait_recv_all(g_backs, k, groups)

            @pl.when(lax.rem(k, each) + DEPTH < each)
            def _():
                start_all(g_backs, k + DEPTH, groups)

            value = dot32(onehot_t[half_of(k)], b2[k].reshape(total, width))
            o1[k] = fold(value[:rows])
            b1[k, z] = o1[k, z]
            start_all(z_backs, k, zs)

        @pl.when(t < chunks)
        def _():
            value = dot32(onehot[half_of(t)], unfold(r1, t)).astype(bf)
            s2[t] = value.reshape(groups, slots, width)
            start_all(g_sends, t, groups)
            r2[t, g_me] = s2[t, g_me]

        @pl.when((t >= 1) & (t <= chunks))
        def _():
            k = t - 1
            wait_recv_all(g_sends, k, groups)
            values = r2[k].reshape(total, width)
            h = half_of(k)
            acc[h, :, :units] += dot32(values, gate_v[columns(k), :])
            acc[h, :, units:] += dot32(values, up_v[columns(k), :])

        @pl.when((t == each) | (t == chunks))
        def _():
            h = half_of(t - 1)
            first = acc[h, :, :units]
            act[...] = (first / (1.0 + jnp.exp(-first)) * acc[h, :, units:]).astype(bf)
            for i in range(each):
                k = h * each + i
                value = dot32(act[...], down_v[:, i * width : (i + 1) * width]).astype(bf)
                o2[k] = value.reshape(groups, slots, width)
                b2[k, g_me] = o2[k, g_me]
                if i < DEPTH:
                    start_all(g_backs, k, groups)

        @pl.when(t >= chunks)
        def _():
            k = t - chunks
            h = half_of(k)
            values = unfold(b1, k)
            at = columns(k)
            value = dot32(weigh[h, 0], values) + dot32(weigh[h, 1], values)

            @pl.when(h == 0)
            def _():
                partial[:, at] = hidden_ref[:, at].astype(f32) + value

            @pl.when(h == 1)
            def _():
                out_ref[:, at] = (partial[:, at] + value).astype(bf)

    for o in range(1, zs):
        m_copy(o).wait_send()

    @pl.loop(0, chunks)
    def _(k):
        for o in range(1, zs):
            z_sends(k, o).wait_send()
            z_backs(k, o).wait_send()
        for o in range(1, groups):
            g_sends(k, o).wait_send()
            g_backs(k, o).wait_send()


def routed_experts(cap, limit, collective, normed, hidden, columns, lanes, gate, up, down):
    zs, ys, cs = lax.axis_size(Z), lax.axis_size(Y), lax.axis_size(CORE)
    groups = ys * cs
    tokens, model = normed.shape
    slots = zs * limit // 2
    high = -(-cap // 8) * 8
    padded = -(-zs * high // 128) * 128
    chunks = 2 * model // WIDTH
    units = gate.shape[1]
    bf, f32 = jnp.bfloat16, jnp.float32
    vmem, anywhere = pl.BlockSpec(memory_space=pltpu.VMEM), pl.BlockSpec(memory_space=pltpu.HBM)
    folds = 8 // (cap % 8) if cap % 8 else 1
    z_block = (chunks, zs, folds * cap, WIDTH // folds)
    g_block = (chunks, groups, slots, WIDTH)
    dma = pltpu.SemaphoreType.DMA
    z_sem, g_sem, m_sem = dma((chunks, zs - 1)), dma((chunks, groups - 1)), dma((zs - 1,))
    total = groups * slots
    return pl.pallas_call(
        functools.partial(expert_kernel, zs, ys, cs, cap, slots),
        out_shape=jax.ShapeDtypeStruct((tokens, model), bf),
        in_specs=[vmem] * 4 + [anywhere] * 3,
        out_specs=vmem,
        scratch_shapes=[
            pltpu.VMEM((2, padded, tokens), bf), pltpu.VMEM((2, 2, tokens, padded), bf),
            pltpu.VMEM((zs, 8, 128), f32),
            pltpu.VMEM(z_block, bf), pltpu.VMEM(z_block, bf),
            pltpu.VMEM(g_block, bf), pltpu.VMEM(g_block, bf),
            pltpu.VMEM(g_block, bf), pltpu.VMEM(g_block, bf),
            pltpu.VMEM(z_block, bf), pltpu.VMEM(z_block, bf),
            pltpu.VMEM((zs, 8, 128), f32),
            pltpu.VMEM((2, padded, total), bf),
            pltpu.VMEM((2, total, padded), bf),
            pltpu.VMEM((2, total, 2 * units), f32),
            pltpu.VMEM((total, units), bf),
            pltpu.VMEM((tokens, model), f32),
            pltpu.VMEM(gate.shape, bf), pltpu.VMEM(up.shape, bf), pltpu.VMEM(down.shape, bf),
            z_sem, z_sem, g_sem, g_sem, g_sem, g_sem, z_sem, z_sem, m_sem, m_sem,
            dma((3,)),
        ],
        compiler_params=pltpu.CompilerParams(
            collective_id=collective, has_side_effects=True, vmem_limit_bytes=VMEM_LIMIT - EXPERT_ROOM
        ),
        name="routed_experts",
    )(normed, hidden, columns, lanes, gate, up, down)


def per_device(
    conv_outer,
    conv_inner,
    conv_input,
    conv_taps,
    out_weight,
    mix_gate,
    residual,
    mix_gain,
    expert_gain,
    expert_ids,
    group_share,
    pair_scores,
    gate_experts,
    up_experts,
    down_experts,
):
    limit = 2 * expert_ids.shape[1] * residual.shape[0] // (lax.axis_size(SP) * gate_experts.shape[0])
    worst = limit * lax.axis_size(Y) * lax.axis_size(CORE) // 2
    caps = [cap for cap in USUAL if cap < worst]
    hidden, normed, columns, lanes, tier = mixer(
        conv_outer, conv_inner, conv_input, conv_taps, out_weight, mix_gate, residual, mix_gain, expert_gain,
        expert_ids, group_share, pair_scores, limit, caps,
    )
    arguments = (normed, hidden, columns, lanes, gate_experts[0], up_experts[0], down_experts[0])
    return lax.switch(
        tier[0, 0],
        [functools.partial(routed_experts, cap, limit, 2 + i) for i, cap in enumerate(caps + [worst])],
        *arguments,
    )


def solution(mesh):
    torus = Mesh(mesh.devices.reshape(8, 4, 2, mesh.shape["tp"]), SP_TP)
    return jax.shard_map(
        per_device,
        mesh=torus,
        in_specs=(
            P(SP, X),
            P(SP, X),
            P(SP, X),
            P(None, X),
            P(X, None),
            P(SP_TP, None),
            P(SP_TP, None),
            P(),
            P(),
            P(SP_TP, None),
            P(SP_TP),
            P(SP_TP, None),
            P(SP, None, None),
            P(SP, None, None),
            P(SP, None, None),
        ),
        out_specs=P(SP_TP, None),
        check_vma=False,
    )
```
